512 devices in a mesh: sp: 32 (over z, x), tp: 16 (over y, core).
Axes of the slice: x: 4, y: 8, z: 8, core: 2. Of those that a mesh axis runs over, the one named last changes fastest.
Arguments:
- residual_layer_input: bfloat16 [8192, 2048], P(('sp', 'tp')), may hold values from -6 to 6
- value_projected: bfloat16 [8192, 4096], P('sp', 'tp'), may hold values from -6 to 6
- key_projected: bfloat16 [8192, 2048], P('sp', 'tp'), may hold values from -6 to 6
- query_projected: bfloat16 [8192, 2048], P('sp', 'tp'), may hold values from -6 to 6
- output_gate_projected: bfloat16 [8192, 4096], P('sp', 'tp'), may hold values from -6 to 6
- step_projected_raw: bfloat16 [2, 8192, 64], P(None, 'sp', 'tp'), may hold values from -5.5 to 5
- head_decay_logarithm: float32 [2, 64], P(None, 'tp'), may hold values from -15 to -2.9
- position_extra_decay: float32 [8192, 64], P('sp', 'tp'), may hold values from -2.1 to 0
- value_filter_weight: bfloat16 [5, 4096], P(None, 'tp'), may hold values from -2.5 to 2.5
- key_filter_weight: bfloat16 [5, 2048], P(None, 'tp'), may hold values from -2.5 to 2.5
- query_filter_weight: bfloat16 [5, 2048], P(None, 'tp'), may hold values from -2.5 to 2.5
- head_norm_gain: float32 [4096], P('tp'), may hold values from 0.1 to 1.9
- mixer_output_matrix: bfloat16 [4096, 2048], P(None, 'tp'), may hold values from -0.09375 to 0.09375
- expert_norm_gain: float32 [2048], replicated, may hold values from 0.1 to 1.9
- routes: int32 [8192, 2], P('sp'), may hold values from 0 to 31, all different within a row; in each aligned block of 16 rows (0 to 15, 16 to 31, ...) at most 2 rows name the same one
- chosen_expert_weight: float32 [8192, 2], P(('sp', 'tp')), may hold values from 0.1 to 1
- expert_gate_matrix: bfloat16 [32, 2048, 4096], P('sp', None, 'tp'), may hold values from -0.125 to 0.125
- expert_up_matrix: bfloat16 [32, 2048, 4096], P('sp', None, 'tp'), may hold values from -0.125 to 0.125
- expert_down_matrix: bfloat16 [32, 4096, 2048], P('sp', 'tp'), may hold values from -0.09375 to 0.09375
Outputs:
- layer_output: bfloat16 [8192, 2048], P(('sp', 'tp'))
The draws below stay inside these ranges and needn't reach their ends.
Inputs may be any that keep to these rules, and one draw needn't show every extreme that they name: `routes`: each row names 2 different experts; the rows of one device (aligned blocks of 16 rows) name one expert 2 times at most, and that most is reached.
All inputs are finite; a program needn't handle non-finite values.
Results may differ from the reference program's by a relative error of at most 0.015.
Values may be sent and summed in bfloat16 or wider, within the bound.
A program may use at most 64 MiB of HBM per device.

```python
import math
import jax
import jax.numpy as jnp
import numpy as np
from jax import lax

D = 2048
HEAD_DIM = 64
HEADS = 64
INNER = 4096
GROUPS = 16
STATE = 128
BLOCK = 128
TAPS = 5
EXPERT_FF = 4096
TOP = 2
TOK_DEV = 256
TOKENS = 8192
ROWS_DEV = 16
EXPERTS = 32
CAPACITY = 2
FF_SHARE = 256
N_TP = 16


def draw_step_projected_raw(key, part):
    noise_key, level_key = jax.random.split(key)
    noise_part = jnp.clip(jax.random.normal(noise_key, (2, TOKENS, HEADS), jnp.float32), -4.0, 4.0)
    segments = TOKENS // TOK_DEV
    first_key, second_key = jax.random.split(level_key)
    ranks = jnp.stack([jax.random.permutation(first_key, segments), jax.random.permutation(second_key, segments)]).astype(jnp.float32)
    shift = -1.5 + 2.5 * ranks / max(segments - 1, 1)
    shift_rows = jnp.repeat(shift, TOK_DEV, axis=1)
    return (noise_part + shift_rows[:, :, None]).astype(jnp.bfloat16)


def draw_head_decay_logarithm(key, part):
    pick_key, fast_key, slow_key = jax.random.split(key, 3)
    fast_share = 0.5
    fast_heads = jax.random.uniform(pick_key, (2, HEADS), jnp.float32) < fast_share
    fast_rate = jnp.exp(jax.random.uniform(fast_key, (2, HEADS), jnp.float32, math.log(1.0 / 60.0), math.log(1.0 / 20.0)))
    slow_rate = jax.random.uniform(slow_key, (2, HEADS), jnp.float32, 0.05, 0.6) / TOKENS
    return jnp.log(jnp.where(fast_heads, fast_rate, slow_rate)).astype(jnp.float32)


def draw_position_extra_decay(key, part):
    place_key, depth_key = jax.random.split(key)
    spots = jax.random.randint(place_key, (3,), 0, TOKENS)
    depth = jnp.log(jax.random.uniform(depth_key, (3, HEADS), jnp.float32, 0.5, 0.8))
    matches = (lax.broadcasted_iota(jnp.int32, (TOKENS, 3), 0) == spots[None, :]).astype(jnp.float32)
    return jnp.dot(matches, depth, precision=lax.Precision.HIGHEST).astype(jnp.float32)


def steps_of(rng, shape, cuts, smallest, high):
    loudness = 1.0
    for dim, parts in cuts:
        draws = jax.random.uniform(jax.random.fold_in(jax.random.fold_in(rng, 6), dim), (parts,), jnp.float32, smallest / len(cuts), high / len(cuts))
        loudness = loudness * jnp.repeat(jnp.exp(draws), shape[dim] // parts).reshape((-1,) + (1,) * (len(shape) - 1 - dim))
    return loudness


def routed_block(stream_key, own, number, rows, number_of, top, bound, skew):
    sequence = jax.random.permutation(stream_key, number_of)
    crowded, common = shares(number_of, rows * top, bound, skew, True), shares(number_of, rows * top, bound, skew, False)
    places = jnp.arange(number_of)

    def named(tallies, rotation):
        used = int((tallies > 0).sum())
        fixed = max(1, used // 4)
        moved = fixed + (places - fixed + rotation * (used - fixed)) % max(1, number_of - fixed)
        return jnp.zeros((number_of,), jnp.int32).at[sequence[jnp.where(places < fixed, places, moved)]].set(jnp.asarray(tallies, jnp.int32))

    tallies = jnp.where(number % 4 == 0, named(crowded, number // 4), named(common, number - number // 4 - 1))
    mixed = jax.random.permutation(jax.random.fold_in(own, 3), number_of)
    giver, taker = mixed[0:number_of // 2 * 2:2], mixed[1:number_of // 2 * 2:2]
    room = jnp.minimum(tallies[giver] - 1, bound - tallies[taker]) // 2
    room = jnp.where((giver == sequence[0]) | (taker == sequence[0]) | (tallies[taker] == 0), 0, jnp.maximum(room, 0))
    moved = jax.random.randint(jax.random.fold_in(own, 4), (number_of // 2,), 0, 1 << 20) % (room + 1)
    tallies = tallies.at[giver].add(-moved).at[taker].add(moved)
    labels = jnp.searchsorted(jnp.cumsum(tallies), jnp.arange(rows * top), side="right").astype(jnp.int32)
    grid = labels.reshape(top, rows).T
    grid = grid[jax.random.permutation(jax.random.fold_in(own, 1), rows)]
    rotation = jax.random.randint(jax.random.fold_in(own, 2), (rows, 1), 0, top)
    return jnp.take_along_axis(grid, (jnp.arange(top)[None, :] + rotation) % top, axis=1)


def shares(count, total, reach, lean, full):
    loads = [(1 << 20) // math.isqrt(rank ** lean) + 1 for rank in range(1, count + 1)]
    largest = reach if full else min(reach, max(-(-total // count), total * loads[0] // sum(loads)))
    least = 1 if total - largest >= count - 1 else 0
    counts, surplus = [largest] + [least] * (count - 1), total - largest - least * (count - 1)
    while surplus > 0:
        candidates = [i for i in range(1, count) if counts[i] < largest] or [i for i in range(1, count) if counts[i] < reach]
        whole, remaining = sum([loads[i] for i in candidates]), surplus
        for i in candidates:
            extra = min(reach - counts[i], max(1, remaining * loads[i] // whole), surplus)
            counts[i] = counts[i] + extra
            surplus = surplus - extra
    return np.array(counts)


def gaussian(stream_key, dims, scale, reach, shards=(), held_as=jnp.bfloat16):
    values = scale * jax.random.normal(stream_key, dims, jnp.float32)
    if shards:
        values = values * steps_of(stream_key, dims, shards, -0.22, 0.18)
    return jnp.clip(values, -reach, reach).astype(held_as)


def setup_inputs(seed: int = 0) -> dict:
    arg_keys = jax.random.split(jax.random.key(seed), 20)
    residual_layer_input = gaussian(arg_keys[0], (TOKENS, D), 1.0, 6.0, ((0, 512),))
    value_projected = gaussian(arg_keys[1], (TOKENS, INNER), 1.0, 6.0, ((0, 32), (1, 16)))
    key_projected = gaussian(arg_keys[2], (TOKENS, GROUPS * STATE), 1.0, 6.0, ((0, 32), (1, 16)))
    query_projected = gaussian(arg_keys[3], (TOKENS, GROUPS * STATE), 1.0, 6.0, ((0, 32), (1, 16)))
    output_gate_projected = gaussian(arg_keys[4], (TOKENS, INNER), 1.0, 6.0, ((0, 32), (1, 16)))
    step_projected_raw = draw_step_projected_raw(jax.random.fold_in(arg_keys[19], 71), 0)
    head_decay_logarithm = draw_head_decay_logarithm(jax.random.fold_in(arg_keys[19], 71), 0)
    position_extra_decay = draw_position_extra_decay(jax.random.fold_in(arg_keys[19], 71), 0)
    value_filter_weight = gaussian(arg_keys[8], (TAPS, INNER), TAPS ** -0.5, 2.5, ((1, 16),))
    key_filter_weight = gaussian(arg_keys[9], (TAPS, GROUPS * STATE), TAPS ** -0.5, 2.5, ((1, 16),))
    query_filter_weight = gaussian(arg_keys[10], (TAPS, GROUPS * STATE), TAPS ** -0.5, 2.5, ((1, 16),))
    head_norm_gain = jnp.clip(1.0 + 0.18 * jax.random.normal(arg_keys[11], (INNER,), jnp.float32), 0.1, 1.9)
    mixer_output_matrix = gaussian(arg_keys[12], (INNER, D), INNER ** -0.5, 0.09375, ((1, 16),))
    expert_norm_gain = jnp.clip(1.0 + 0.18 * jax.random.normal(arg_keys[13], (D,), jnp.float32), 0.1, 1.9)
    routes_keys = jax.random.split(jax.random.fold_in(arg_keys[14], 1), TOKENS // ROWS_DEV)
    routes_turns = jax.random.permutation(jax.random.fold_in(arg_keys[14], 3), TOKENS // ROWS_DEV)
    routes = jax.vmap(lambda own, number: routed_block(jax.random.fold_in(arg_keys[14], 2), own, number, ROWS_DEV, EXPERTS, TOP, CAPACITY, 1))(routes_keys, routes_turns).reshape((TOKENS, TOP))
    chosen_expert_weight = jnp.clip(0.1 + 0.9 * jax.random.uniform(arg_keys[15], (TOKENS, TOP), jnp.float32) ** steps_of(arg_keys[15], (TOKENS, TOP), ((0, 512),), -0.2, 0.2), 0.1, 1.0)
    expert_gate_matrix = gaussian(arg_keys[16], (EXPERTS, D, EXPERT_FF), D ** -0.5, 0.125, ((0, 32), (2, 16)))
    expert_up_matrix = gaussian(arg_keys[17], (EXPERTS, D, EXPERT_FF), D ** -0.5, 0.125, ((0, 32), (2, 16)))
    expert_down_matrix = gaussian(arg_keys[18], (EXPERTS, EXPERT_FF, D), EXPERT_FF ** -0.5, 0.09375, ((0, 32), (1, 16)))
    return {"residual_layer_input": residual_layer_input, "value_projected": value_projected, "key_projected": key_projected, "query_projected": query_projected, "output_gate_projected": output_gate_projected, "step_projected_raw": step_projected_raw, "head_decay_logarithm": head_decay_logarithm, "position_extra_decay": position_extra_decay, "value_filter_weight": value_filter_weight, "key_filter_weight": key_filter_weight, "query_filter_weight": query_filter_weight, "head_norm_gain": head_norm_gain, "mixer_output_matrix": mixer_output_matrix, "expert_norm_gain": expert_norm_gain, "routes": routes, "chosen_expert_weight": chosen_expert_weight, "expert_gate_matrix": expert_gate_matrix, "expert_up_matrix": expert_up_matrix, "expert_down_matrix": expert_down_matrix}


epsilon = 1e-06

def centred_taps(inputs, taps):
    length = inputs.shape[0]
    half_width = (taps.shape[0] - 1) // 2
    padded = jnp.pad(inputs.astype(jnp.float32), ((half_width, half_width), (0, 0)))
    weights = taps.astype(jnp.float32)
    result = weights[0] * padded[0:length]
    for offset in range(1, taps.shape[0]):
        result = result + weights[offset] * padded[offset:offset + length]
    return result

def block_terms(operands):
    forward_cum, backward_excl, forward_part, backward_part, key_rows, query_rows = operands
    scores = jnp.einsum('lgn,sgn->lsg', query_rows.astype(jnp.float32), key_rows.astype(jnp.float32))
    position = jnp.arange(scores.shape[0], dtype=jnp.int32)
    lower_mask = (position[None, :] <= position[:, None])[:, :, None, None]
    upper_mask = (position[None, :] >= position[:, None])[:, :, None, None]
    forward_gap = jnp.where(lower_mask, forward_cum[:, None] - forward_cum[None, :], -jnp.inf)
    backward_gap = jnp.where(upper_mask, backward_excl[None, :] - backward_excl[:, None], -jnp.inf)
    forward_weight = (scores[..., None] * jnp.exp(forward_gap)).astype(jnp.bfloat16)
    backward_weight = (scores[..., None] * jnp.exp(backward_gap)).astype(jnp.bfloat16)
    inner = jnp.einsum('lsgh,sghp->lghp', forward_weight.astype(jnp.float32), forward_part.astype(jnp.float32))
    inner = inner + jnp.einsum('lsgh,sghp->lghp', backward_weight.astype(jnp.float32), backward_part.astype(jnp.float32))
    key_wide = key_rows.astype(jnp.float32)[:, :, None, :]
    forward_keys = (jnp.exp(forward_cum[-1][None] - forward_cum)[..., None] * key_wide).astype(jnp.bfloat16)
    backward_keys = (jnp.exp(backward_excl)[..., None] * key_wide).astype(jnp.bfloat16)
    forward_state = jnp.einsum('sghn,sghp->ghpn', forward_keys.astype(jnp.float32), forward_part.astype(jnp.float32))
    backward_state = jnp.einsum('sghn,sghp->ghpn', backward_keys.astype(jnp.float32), backward_part.astype(jnp.float32))
    return (inner, forward_state, backward_state)

def advance(carried, operands):
    block_state, block_total = operands
    return (jnp.exp(block_total)[..., None, None] * carried + block_state, carried)

def apply_expert(operands):
    slot_block, gate_part, up_part, down_part = operands
    gate_value = jnp.dot(slot_block, gate_part, preferred_element_type=jnp.float32)
    up_value = jnp.dot(slot_block, up_part, preferred_element_type=jnp.float32)
    hidden = (jax.nn.silu(gate_value) * up_value).astype(jnp.bfloat16)
    pieces = jnp.einsum('rjf,jfd->jrd', hidden.reshape(slot_block.shape[0], N_TP, FF_SHARE).astype(jnp.float32), down_part.reshape(N_TP, FF_SHARE, D).astype(jnp.float32)).astype(jnp.bfloat16)
    return lax.optimization_barrier(jnp.sum(pieces.astype(jnp.float32), axis=0)).astype(jnp.bfloat16)

def reference(residual_layer_input, value_projected, key_projected, query_projected, output_gate_projected, step_projected_raw, head_decay_logarithm, position_extra_decay, value_filter_weight, key_filter_weight, query_filter_weight, head_norm_gain, mixer_output_matrix, expert_norm_gain, routes, chosen_expert_weight, expert_gate_matrix, expert_up_matrix, expert_down_matrix):
    tokens = value_projected.shape[0]
    per_group = HEADS // GROUPS
    blocks = tokens // BLOCK
    values = centred_taps(value_projected, value_filter_weight).astype(jnp.bfloat16)
    key_rows = jax.nn.silu(centred_taps(key_projected, key_filter_weight)).astype(jnp.bfloat16).reshape(blocks, BLOCK, GROUPS, STATE)
    query_rows = jax.nn.silu(centred_taps(query_projected, query_filter_weight)).astype(jnp.bfloat16).reshape(blocks, BLOCK, GROUPS, STATE)
    positive_step_sizes = jax.nn.softplus(step_projected_raw.astype(jnp.float32))
    decay_logarithm = -jnp.exp(head_decay_logarithm)[:, None, :] * positive_step_sizes + position_extra_decay[None]
    scaled = (values.astype(jnp.float32).reshape(tokens, HEADS, HEAD_DIM)[None] * positive_step_sizes[..., None]).astype(jnp.bfloat16)
    scaled = scaled.reshape(2, blocks, BLOCK, GROUPS, per_group, HEAD_DIM)
    log_blocks = decay_logarithm.reshape(2, blocks, BLOCK, GROUPS, per_group)
    running = jnp.cumsum(log_blocks, axis=2)
    forward_cum = running[0]
    backward_excl = running[1] - log_blocks[1]
    forward_total = running[0][:, -1]
    backward_total = running[1][:, -1]
    inner, forward_state, backward_state = lax.map(block_terms, (forward_cum, backward_excl, scaled[0], scaled[1], key_rows, query_rows))
    zero_state = jnp.zeros((GROUPS, per_group, HEAD_DIM, STATE), jnp.float32)
    entering = lax.scan(advance, zero_state, (forward_state, forward_total))[1]
    leaving = lax.scan(advance, zero_state, (backward_state, backward_total), reverse=True)[1]
    query_wide = query_rows.astype(jnp.float32)
    forward_read = jnp.exp(forward_cum)[..., None] * jnp.einsum('blgn,bghpn->blghp', query_wide, entering.astype(jnp.bfloat16).astype(jnp.float32))
    backward_read = jnp.exp(backward_total[:, None] - backward_excl)[..., None] * jnp.einsum('blgn,bghpn->blghp', query_wide, leaving.astype(jnp.bfloat16).astype(jnp.float32))
    mixer_raw = (inner + forward_read + backward_read).reshape(tokens, HEADS, HEAD_DIM)
    gated = mixer_raw * jax.nn.silu(output_gate_projected.astype(jnp.float32)).reshape(tokens, HEADS, HEAD_DIM)
    inverse_rms = lax.rsqrt(lax.optimization_barrier(jnp.mean(gated * gated, axis=-1, keepdims=True)) + epsilon)
    head_normed = (gated * inverse_rms * head_norm_gain.reshape(HEADS, HEAD_DIM)).astype(jnp.bfloat16)
    head_normed = head_normed.reshape(tokens, HEADS * HEAD_DIM)
    mixer_out = jnp.dot(head_normed, mixer_output_matrix, preferred_element_type=jnp.float32).astype(jnp.bfloat16)
    middle = (residual_layer_input.astype(jnp.float32) + mixer_out.astype(jnp.float32)).astype(jnp.bfloat16)
    residual = middle.astype(jnp.float32)
    normed = (residual * lax.rsqrt(lax.optimization_barrier(jnp.mean(residual * residual, axis=-1, keepdims=True)) + epsilon) * expert_norm_gain).astype(jnp.bfloat16)
    device_blocks = tokens // ROWS_DEV
    slots_each = device_blocks * CAPACITY
    flat_routes = routes.reshape(device_blocks, ROWS_DEV * TOP).astype(jnp.int32)
    matches = (flat_routes[:, :, None] == jnp.arange(EXPERTS, dtype=jnp.int32)[None, None, :]).astype(jnp.int32)
    earlier = (jnp.cumsum(matches, axis=1) - matches).astype(jnp.int32)
    rank_in = lax.optimization_barrier(jnp.sum(matches * earlier, axis=2)).astype(jnp.int32)
    block_index = jnp.arange(device_blocks, dtype=jnp.int32)[:, None]
    slot_ids = (flat_routes * slots_each + block_index * CAPACITY + rank_in).reshape(-1).astype(jnp.int32)
    copies = jnp.repeat(normed, TOP, axis=0)
    slot_rows = jnp.zeros((EXPERTS * slots_each, D), jnp.bfloat16).at[slot_ids].set(copies)
    expert_out = lax.map(apply_expert, (slot_rows.reshape(EXPERTS, slots_each, D), expert_gate_matrix, expert_up_matrix, expert_down_matrix))
    picked = expert_out.reshape(EXPERTS * slots_each, D)[slot_ids].astype(jnp.float32).reshape(tokens, TOP, D)
    expert_mix = lax.optimization_barrier(jnp.sum(picked * chosen_expert_weight[:, :, None], axis=1))
    return (residual + expert_mix).astype(jnp.bfloat16)
```

```python
import functools

import jax
import jax.numpy as jnp
from jax import lax
from jax.experimental import pallas as pl
from jax.experimental.pallas import tpu as pltpu
from jax.sharding import PartitionSpec as P

MESH = pl.DeviceIdType.MESH
HIGH = lax.Precision.HIGHEST
F32 = jnp.float32
BF16 = jnp.bfloat16
EPS = 1e-06
BLOCK = 128
NCH = 4


def dot(a, b, contract=((1,), (0,)), precision=None):
    return lax.dot_general(
        a, b, (contract, ((), ())), preferred_element_type=F32, precision=precision
    )


def silu(v):
    return v / (1.0 + jnp.exp(-v))


def rcopy(src, dst, send, recv, dev):
    return pltpu.make_async_remote_copy(
        src_ref=src, dst_ref=dst, send_sem=send, recv_sem=recv, device_id=dev, device_id_type=MESH
    )


def wait_bytes(ref, sem):
    pltpu.make_async_copy(ref, ref, sem).wait()


def iota(shape, dim):
    return lax.broadcasted_iota(jnp.int32, shape, dim)


def body(
    nsp,
    ntp,
    resid,
    v_in,
    k_in,
    q_in,
    og_in,
    raw_in,
    extra_in,
    rate_in,
    vf_in,
    kf_in,
    qf_in,
    gain_in,
    wout,
    ngain_in,
    routes_in,
    cw_in,
    wg,
    wu,
    wd,
    out,
    hl,
    hr,
    pad,
    tot_s,
    tot_r,
    st_s,
    st_r,
    sc_f,
    sc_s,
    sc_r,
    heads,
    wc,
    po,
    mo,
    dm,
    dr,
    rowsf,
    xs,
    wgu,
    wdn,
    acc,
    zs,
    sp_b,
    sn_b,
    rp_b,
    rn_b,
    bm,
    br,
    lsem,
    hsem,
    tsem,
    ssem,
    osem,
    hdsem,
    wsem,
    swsem,
    psem,
    dsem,
    ag_send,
    ag_recv,
    rs_send,
    rs_recv,
    bsem,
):
    me = lax.axis_index("sp")
    tp = lax.axis_index("tp")
    ny = ntp // 2
    y = tp // 2
    c = tp % 2
    partner = y * 2 + (1 - c)
    right_y = ((y + 1) % ny) * 2 + c
    left_y = ((y + ny - 1) % ny) * 2 + c
    others = nsp - 1

    bar = pltpu.get_barrier_semaphore()

    @pl.loop(1, nsp)
    def _(i):
        pl.semaphore_signal(bar, inc=1, device_id={"sp": (me + i) % nsp}, device_id_type=MESH)

    @pl.loop(1, ntp)
    def _(i):
        pl.semaphore_signal(bar, inc=1, device_id={"tp": (tp + i) % ntp}, device_id_type=MESH)

    ff = wg.shape[1]
    chan = wout.shape[0] // ny
    ycol = pl.ds(pl.multiple_of(y * 128, 128), 128)
    loads = [
        pltpu.make_async_copy(wout.at[pl.ds(pl.multiple_of(y * chan, chan), chan)], wc.at[:, ycol], lsem.at[0]),
        pltpu.make_async_copy(wg, wgu.at[:, pl.ds(0, ff)], lsem.at[1]),
        pltpu.make_async_copy(wu, wgu.at[:, pl.ds(2 * ff, ff)], lsem.at[2]),
        pltpu.make_async_copy(wd, wdn.at[pl.ds(0, ff)], lsem.at[3]),
    ]
    for load in loads:
        load.start()

    lane = iota((1, 128), 1)
    step8 = raw_in[...]
    step8 = jnp.maximum(step8, 0.0) + jnp.log1p(jnp.exp(-jnp.abs(step8)))
    log8 = rate_in[...] * step8 + extra_in[...]
    row = iota((BLOCK, BLOCK), 0)
    col = iota((BLOCK, BLOCK), 1)
    lower = (col <= row).astype(F32)
    ones = jnp.ones((BLOCK, BLOCK), F32)
    spread = ((iota((128, 512), 1) // 64) == iota((128, 512), 0)).astype(F32)
    cum, cum_t, tot_c, sw8, rd8 = [], [], [], [], []
    for b in range(2):
        logs = log8[b * BLOCK : (b + 1) * BLOCK]
        run = dot(lower, logs, precision=HIGH)
        total = run[BLOCK - 1 : BLOCK]
        both = run - jnp.where(lane >= 4, logs, 0.0)
        cum.append(both)
        cum_t.append(both.T)
        tot_c.append(dot(logs, ones, ((0,), (0,)), HIGH)[0:8])
        sw8.append(jnp.exp(jnp.where(lane < 4, total - both, both)))
        rd8.append(jnp.exp(jnp.where(lane < 4, both, total - both)))
    tot_dev = jnp.exp(tot_c[0] + tot_c[1])
    tot_s[...] = tot_dev
    tot_r[me] = tot_dev
    step_x = dot(step8, spread, precision=HIGH)
    sw_x = [dot(sw8[b], spread, precision=HIGH) for b in range(2)]
    rd_x = [dot(rd8[b], spread, precision=HIGH) for b in range(2)]

    def head_rows(b, first):
        e = jnp.exp(tot_c[b][first : first + 4])
        return jnp.concatenate([jnp.broadcast_to(e[h : h + 1], (64, 128)) for h in range(4)], axis=0)

    pl.semaphore_wait(bar, nsp - 1 + ntp - 1)

    right = {"sp": (me + 1) % nsp}
    left = {"sp": (me + nsp - 1) % nsp}
    tokens = v_in.shape[0]
    for ref, lo, width in ((v_in, 0, 256), (k_in, 256, 128), (q_in, 384, 128)):
        cols = pl.ds(lo, width)
        rcopy(ref.at[pl.ds(tokens - 16, 16)], hl.at[:, cols], hsem.at[0], hsem.at[1], right).start()
        rcopy(ref.at[pl.ds(0, 16)], hr.at[:, cols], hsem.at[2], hsem.at[3], left).start()

    @pl.loop(1, nsp)
    def _(i):
        rcopy(tot_s, tot_r.at[me], tsem.at[0], tsem.at[1], {"sp": (me + i) % nsp}).start()

    @pl.loop(1, ny)
    def _(i):
        dst = (y + i) % ny
        rcopy(
            wout.at[pl.ds(pl.multiple_of(dst * chan, chan), chan)],
            wc.at[:, ycol],
            wsem.at[0],
            wsem.at[1],
            {"tp": dst * 2 + c},
        ).start()

    swaps = [
        rcopy(wg, wgu.at[:, pl.ds(ff, ff)], swsem.at[0], swsem.at[1], {"tp": partner}),
        rcopy(wu, wgu.at[:, pl.ds(3 * ff, ff)], swsem.at[2], swsem.at[3], {"tp": partner}),
        rcopy(wd, wdn.at[pl.ds(ff, ff)], swsem.at[4], swsem.at[5], {"tp": partner}),
    ]
    for swap in swaps:
        swap.start()

    pad[16 : 16 + tokens, 0:256] = v_in[...].astype(F32)
    pad[16 : 16 + tokens, 256:384] = k_in[...].astype(F32)
    pad[16 : 16 + tokens, 384:512] = q_in[...].astype(F32)
    wait_bytes(hl, hsem.at[1])
    wait_bytes(hr, hsem.at[3])
    pad[0:16] = jnp.where(me > 0, hl[...].astype(F32), 0.0)
    pad[16 + tokens : 32 + tokens] = jnp.where(me < nsp - 1, hr[...].astype(F32), 0.0)
    filt = jnp.concatenate([vf_in[...], kf_in[...], qf_in[...]], axis=1).astype(F32)
    conv = filt[0:1] * pad[14 : 14 + tokens]
    for o in range(1, 5):
        conv = conv + filt[o : o + 1] * pad[14 + o : 14 + o + tokens]
    values = conv[:, 0:256].astype(BF16).astype(F32)
    keys = silu(conv[:, 256:384]).astype(BF16)
    queries = silu(conv[:, 384:512]).astype(BF16)
    scaled = (jnp.concatenate([values, values], axis=1) * step_x).astype(BF16)

    part = []
    for b in range(2):
        rows = slice(b * BLOCK, (b + 1) * BLOCK)
        weighted = (scaled[rows].astype(F32) * sw_x[b]).astype(BF16)
        part.append(dot(weighted, keys[rows], ((0,), (0,))))
    final_f = head_rows(1, 0) * part[0][0:256] + part[1][0:256]
    final_b = head_rows(0, 4) * part[1][256:512] + part[0][256:512]
    piece = 256 // nsp
    mine = jnp.concatenate(
        [final_f.reshape(nsp, piece, 128), final_b.reshape(nsp, piece, 128)], axis=1
    ).astype(BF16)
    st_s[...] = mine

    @pl.loop(1, nsp)
    def _(i):
        dst = (me + i) % nsp
        rcopy(st_s.at[dst], st_r.at[me], ssem.at[0], ssem.at[1], {"sp": dst}).start()

    st_r[me] = st_s[me]

    inner = []
    lo_half = lane < 64
    for b in range(2):
        rows = slice(b * BLOCK, (b + 1) * BLOCK)
        score = dot(queries[rows], keys[rows], ((1,), (1,)))
        pairs = []
        for pair in range(2):
            halves = []
            for h in (2 * pair, 2 * pair + 1):
                f_gap = cum[b][:, h : h + 1] - cum_t[b][h : h + 1, :]
                b_gap = cum_t[b][4 + h : 5 + h, :] - cum[b][:, 4 + h : 5 + h]
                w = score * jnp.exp(jnp.where(col <= row, f_gap, b_gap))
                w_f = jnp.where(col <= row, w, 0.0)
                w_b = jnp.where(col >= row, w, 0.0)
                both = jnp.concatenate([w_f, w_b], axis=1).astype(BF16)
                lanes = slice(128 * pair, 128 * pair + 128)
                rhs = jnp.concatenate(
                    [scaled[rows, lanes], scaled[rows, 256 + 128 * pair : 384 + 128 * pair]], axis=0
                )
                halves.append(dot(both, rhs))
            pairs.append(jnp.where(lo_half, halves[0], halves[1]))
        inner.append(jnp.concatenate(pairs, axis=1))
    gate_act = silu(og_in[...].astype(F32))

    own = routes_in.shape[0] // ntp
    my_routes = routes_in[pl.ds(pl.multiple_of(tp * own, own), own), :]
    e_lane = iota((own, 128), 1)
    hot0 = (my_routes[:, 0:1] == e_lane).astype(F32)
    hot1 = (my_routes[:, 1:2] == e_lane).astype(F32)
    strict = (iota((own, own), 1) < iota((own, own), 0)).astype(F32)
    before = dot(strict, hot0 + hot1, precision=HIGH)
    ids = e_lane.astype(F32) * 2.0 + before
    slot0 = jnp.sum(hot0 * ids, axis=1, keepdims=True)
    slot1 = jnp.sum(hot1 * ids, axis=1, keepdims=True)
    r_id = iota((NCH * own, nsp * 8), 1)
    r_slot = ((r_id // 8) * 2 + r_id % 2).astype(F32)
    same = ((r_id // 2) % 4) == (iota((NCH * own, nsp * 8), 0) // own)
    hit0 = same & (r_slot == jnp.concatenate([slot0] * NCH, axis=0))
    hit1 = same & (r_slot == jnp.concatenate([slot1] * NCH, axis=0))
    place = jnp.where(hit0 | hit1, 1.0, 0.0).astype(BF16)
    w0 = jnp.concatenate([cw_in[:, 0:1]] * NCH, axis=0)
    w1 = jnp.concatenate([cw_in[:, 1:2]] * NCH, axis=0)
    mixing = jnp.where(hit0, w0, 0.0) + jnp.where(hit1, w1, 0.0)
    mix_hi = mixing.astype(BF16)
    mix_lo = (mixing - mix_hi.astype(F32)).astype(BF16)

    wait_bytes(tot_r.at[pl.ds(0, others)], tsem.at[1])
    wait_bytes(st_r.at[pl.ds(0, others)], ssem.at[1])
    head = me // (64 // piece)

    def forward(d, carry):
        sc_f[d, 0:piece] = carry
        decay = tot_r[d, pl.ds(head, 1), :]
        return decay * carry + st_r[d].astype(F32)[0:piece]

    def backward(i, carry):
        d = nsp - 1 - i
        sc_f[d, piece : 2 * piece] = carry
        decay = tot_r[d, pl.ds(head + 4, 1), :]
        return decay * carry + st_r[d].astype(F32)[piece : 2 * piece]

    zero = jnp.zeros((piece, 128), F32)
    lax.fori_loop(0, nsp, forward, zero)
    lax.fori_loop(0, nsp, backward, zero)
    sc_s[...] = sc_f[...].astype(BF16)

    @pl.loop(1, nsp)
    def _(i):
        dst = (me + i) % nsp
        rcopy(sc_s.at[dst], sc_r.at[me], osem.at[0], osem.at[1], {"sp": dst}).start()

    sc_r[me] = sc_s[me]
    wait_bytes(sc_r.at[pl.ds(0, others)], osem.at[1])

    around = sc_r[...].astype(F32)
    enter = around[:, 0:piece].reshape(256, 128)
    leave = around[:, piece : 2 * piece].reshape(256, 128)
    enters = [enter, head_rows(0, 0) * enter + part[0][0:256]]
    leaves = [head_rows(1, 4) * leave + part[1][256:512], leave]
    group = (iota((256, 256), 0) // 64 == iota((256, 256), 1) // 64).astype(F32) * (1.0 / 64.0)
    for b in range(2):
        rows = slice(b * BLOCK, (b + 1) * BLOCK)
        state = jnp.concatenate([enters[b], leaves[b]], axis=0).astype(BF16)
        read = dot(queries[rows], state, ((1,), (1,))) * rd_x[b]
        gated = (inner[b] + read[:, 0:256] + read[:, 256:512]) * gate_act[rows]
        mean = dot(gated * gated, group, precision=HIGH)
        normed = gated * lax.rsqrt(mean + EPS) * gain_in[...]
        heads[c, rows, :] = normed.astype(BF16)

    swap_h = rcopy(heads.at[c], heads.at[c], hdsem.at[0], hdsem.at[1], {"tp": partner})
    swap_h.start()

    loads[0].wait()
    wait_bytes(wc.at[:, pl.ds(0, 128 * (ny - 1))], wsem.at[1])
    inner_c = chan // 2
    own_part = dot(heads[c], wc[pl.ds(pl.multiple_of(c * inner_c, inner_c), inner_c), :])
    swap_h.wait()
    o_c = 1 - c
    full = own_part + dot(heads[o_c], wc[pl.ds(pl.multiple_of(o_c * inner_c, inner_c), inner_c), :])
    po[...] = full.reshape(ntp, own, full.shape[1]).astype(BF16)

    @pl.loop(1, ntp)
    def _(i):
        dst = (tp + i) % ntp
        rcopy(po.at[dst], mo.at[tp], psem.at[0], psem.at[1], {"tp": dst}).start()

    mo[tp] = po[tp]
    wait_bytes(mo.at[pl.ds(0, ntp - 1)], psem.at[1])
    halves = []
    for core in range(2):
        total = mo[core].astype(F32)
        for other in range(1, ny):
            total = total + mo[2 * other + core].astype(F32)
        halves.append(total)
    pieces = []
    for j in range(ny):
        pieces += [halves[0][:, 128 * j : 128 * j + 128], halves[1][:, 128 * j : 128 * j + 128]]
    mixer_out = jnp.concatenate(pieces, axis=1).astype(BF16).astype(F32)
    middle = (resid[...].astype(F32) + mixer_out).astype(BF16).astype(F32)
    square = jnp.mean(middle * middle, axis=-1, keepdims=True)
    normed = (middle * lax.rsqrt(square + EPS) * ngain_in[...]).astype(BF16)
    width = normed.shape[1] // NCH
    stacked = jnp.concatenate([normed[:, j * width : (j + 1) * width] for j in range(NCH)], axis=0)
    sent = dot(place, stacked, ((0,), (0,)))
    dm[...] = sent.reshape(nsp, 8, width).astype(BF16)

    @pl.loop(1, nsp)
    def _(i):
        dst = (me + i) % nsp
        rcopy(dm.at[dst], dr.at[me], dsem.at[0], dsem.at[1], {"sp": dst}).start()

    dr[me] = dm[me]
    wait_bytes(dr.at[pl.ds(0, others)], dsem.at[1])
    arrived = dr[...].astype(F32).reshape(nsp * 8, width)
    for n in range(width // 128):
        rowsf[n] = arrived[:, n * 128 : (n + 1) * 128]
    r_dev = {"tp": right_y}
    l_dev = {"tp": left_y}
    for j in range(NCH):
        for s in range(2):
            for n in range(width // 128):
                picked = rowsf[n, pl.ds(2 * j + s, nsp, stride=8), :]
                xs[0, j, s * nsp : (s + 1) * nsp, n * 128 : (n + 1) * 128] = picked.astype(BF16)
        rcopy(xs.at[0, j], xs.at[1, j], ag_send.at[0, 0], ag_recv.at[0, 1, j], r_dev).start()
        rcopy(xs.at[0, j], xs.at[5, j], ag_send.at[1, 0], ag_recv.at[1, 1, j], l_dev).start()

    for load in loads[1:]:
        load.wait()
    for swap in swaps:
        swap.wait()

    rows1 = 2 * nsp

    def add_chunk(x, j, first):
        n = x.shape[0]
        w = wgu[pl.ds(pl.multiple_of(j * width, width), width), :]
        g = dot(x, w)

        @pl.when(first)
        def _():
            acc[0:n] = g

        @pl.when(jnp.logical_not(first))
        def _():
            acc[0:n] += g

    def finish(n, store):
        g = acc[0:n, 0 : 2 * ff]
        u = acc[0:n, 2 * ff : 4 * ff]
        hidden = (silu(g) * u).astype(BF16)
        for j in range(NCH):
            store(j, dot(hidden, wdn[:, j * width : (j + 1) * width]))

    def store_own(j, z):
        zs[0, j] = z

    @pl.loop(0, NCH)
    def _(j):
        add_chunk(xs[0, j], j, j == 0)

    finish(rows1, store_own)

    @pl.loop(0, 3 * NCH)
    def _(t):
        k = 1 + t // NCH
        j = t % NCH
        wait_bytes(xs.at[k, j], ag_recv.at[0, k, j])
        wait_bytes(xs.at[4 + k, j], ag_recv.at[1, k, j])

        @pl.when(k < 3)
        def _():
            rcopy(xs.at[k, j], xs.at[k + 1, j], ag_send.at[0, k], ag_recv.at[0, k + 1, j], r_dev).start()
            rcopy(xs.at[4 + k, j], xs.at[5 + k, j], ag_send.at[1, k], ag_recv.at[1, k + 1, j], l_dev).start()

        @pl.when((k == 3) & (j < 2))
        def _():
            rcopy(xs.at[3, j], xs.at[4, j], ag_send.at[0, 3], ag_recv.at[0, 4, j], r_dev).start()

        @pl.when((k == 3) & (j >= 2))
        def _():
            rcopy(xs.at[7, j], xs.at[4, j], ag_send.at[1, 3], ag_recv.at[1, 4, j], l_dev).start()

        add_chunk(jnp.concatenate([xs[k, j], xs[4 + k, j]], axis=0), j, j == 0)

        @pl.when(j == NCH - 1)
        def _():
            def store(i, z):
                zs[k, i] = z[0:rows1]
                zs[4 + k, i] = z[rows1 : 2 * rows1]

            finish(2 * rows1, store)

    for j in (0, 2, 1, 3):
        wait_bytes(xs.at[4, j], ag_recv.at[0 if j < 2 else 1, 4, j])
        add_chunk(xs[4, j], j, j == 0)

    def store_far(j, z):
        zs[4, j] = z
        if j < 2:
            sp_b[3, j] = z.astype(BF16)
            rcopy(sp_b.at[3, j], rp_b.at[3, j], rs_send.at[0, 3], rs_recv.at[0, 3, j], r_dev).start()
        else:
            sn_b[3, j] = z.astype(BF16)
            rcopy(sn_b.at[3, j], rn_b.at[3, j], rs_send.at[1, 3], rs_recv.at[1, 3, j], l_dev).start()

    finish(rows1, store_far)

    @pl.loop(0, 3 * NCH)
    def _(t):
        k = 3 - t // NCH
        i = t % NCH
        jp = (i + 2) % NCH
        jn = i
        ready = (k < 3) | (i >= 2)

        @pl.when(ready)
        def _():
            wait_bytes(rp_b.at[k, jp], rs_recv.at[0, k, jp])
            wait_bytes(rn_b.at[k, jn], rs_recv.at[1, k, jn])
            sp_b[k - 1, jp] = (zs[4 + k, jp] + rp_b[k, jp].astype(F32)).astype(BF16)
            sn_b[k - 1, jn] = (zs[k, jn] + rn_b[k, jn].astype(F32)).astype(BF16)

        @pl.when(jnp.logical_not(ready))
        def _():
            sp_b[k - 1, jp] = zs[4 + k, jp].astype(BF16)
            sn_b[k - 1, jn] = zs[k, jn].astype(BF16)

        rcopy(
            sp_b.at[k - 1, jp], rp_b.at[k - 1, jp], rs_send.at[0, k - 1], rs_recv.at[0, k - 1, jp], r_dev
        ).start()
        rcopy(
            sn_b.at[k - 1, jn], rn_b.at[k - 1, jn], rs_send.at[1, k - 1], rs_recv.at[1, k - 1, jn], l_dev
        ).start()

    for j in range(NCH):
        wait_bytes(rp_b.at[0, j], rs_recv.at[0, 0, j])
        wait_bytes(rn_b.at[0, j], rs_recv.at[1, 0, j])
        total = zs[0, j] + rp_b[0, j].astype(F32) + rn_b[0, j].astype(F32)
        for s in range(2):
            for n in range(width // 128):
                lanes = slice(n * 128, (n + 1) * 128)
                rowsf[n, pl.ds(2 * j + s, nsp, stride=8), :] = total[s * nsp : (s + 1) * nsp, lanes]
    done = jnp.concatenate([rowsf[n] for n in range(width // 128)], axis=1)
    bm[...] = done.reshape(nsp, 8, width).astype(BF16)

    @pl.loop(1, nsp)
    def _(i):
        dst = (me + i) % nsp
        rcopy(bm.at[dst], br.at[me], bsem.at[0], bsem.at[1], {"sp": dst}).start()

    br[me] = bm[me]
    wait_bytes(br.at[pl.ds(0, others)], bsem.at[1])
    back = br[...].astype(F32).reshape(nsp * 8, width).astype(BF16)
    mixed = dot(mix_hi, back) + dot(mix_lo, back)
    for j in range(NCH):
        cols = slice(j * width, (j + 1) * width)
        out[:, cols] = (middle[:, cols] + mixed[j * own : (j + 1) * own]).astype(BF16)

    wait_bytes(hl, hsem.at[0])
    wait_bytes(hr, hsem.at[2])
    wait_bytes(tot_r.at[pl.ds(0, others)], tsem.at[0])
    wait_bytes(st_r.at[pl.ds(0, others)], ssem.at[0])
    wait_bytes(sc_r.at[pl.ds(0, others)], osem.at[0])
    wait_bytes(wc.at[:, pl.ds(0, 128 * (ny - 1))], wsem.at[0])
    wait_bytes(mo.at[pl.ds(0, ntp - 1)], psem.at[0])
    wait_bytes(dr.at[pl.ds(0, others)], dsem.at[0])
    wait_bytes(br.at[pl.ds(0, others)], bsem.at[0])
    for way in range(2):
        for k in range(3):
            wait_bytes(xs.at[0], ag_send.at[way, k])
            wait_bytes(xs.at[0], rs_send.at[way, k])
        wait_bytes(xs.at[0, pl.ds(0, 2)], ag_send.at[way, 3])
        wait_bytes(xs.at[0, pl.ds(0, 2)], rs_send.at[way, 3])


def layer(nsp, ntp, resid, v, k, q, og, raw, hdl, extra, vf, kf, qf, gain, wout, ngain, routes, cw, wg, wu, wd):
    ny = ntp // 2
    tokens = v.shape[0]
    own = tokens // ntp
    width = resid.shape[1] // NCH
    ff = wg.shape[2]
    chan = wout.shape[0] // ny
    rows1 = 2 * nsp

    def lanes(x):
        return jnp.pad(x, ((0, 0), (0, 128 - x.shape[1])))

    raw8 = lanes(jnp.concatenate([raw[0], raw[1]], axis=1).astype(F32))
    extra8 = lanes(jnp.concatenate([extra, extra], axis=1))
    rate8 = lanes(-jnp.exp(hdl).reshape(1, 8))
    dma = pltpu.SemaphoreType.DMA
    vmem = pl.BlockSpec(memory_space=pltpu.VMEM)
    hbm = pl.BlockSpec(memory_space=pl.ANY)
    pair = (nsp, 16, 128)
    msg = (nsp, 8, width)
    ring = (4, NCH, rows1, width)
    scratch = [
        pltpu.VMEM((16, 512), BF16),
        pltpu.VMEM((16, 512), BF16),
        pltpu.VMEM((tokens + 32, 512), F32),
        pltpu.VMEM((8, 128), F32),
        pltpu.VMEM((nsp, 8, 128), F32),
        pltpu.VMEM(pair, BF16),
        pltpu.VMEM(pair, BF16),
        pltpu.VMEM(pair, F32),
        pltpu.VMEM(pair, BF16),
        pltpu.VMEM(pair, BF16),
        pltpu.VMEM((2, tokens, 256), BF16),
        pltpu.VMEM((chan, 128 * ny), BF16),
        pltpu.VMEM((ntp, own, 128 * ny), BF16),
        pltpu.VMEM((ntp, own, 128 * ny), BF16),
        pltpu.VMEM(msg, BF16),
        pltpu.VMEM(msg, BF16),
        pltpu.VMEM((width // 128, nsp * 8, 128), F32),
        pltpu.VMEM((8, NCH, rows1, width), BF16),
        pltpu.VMEM((wg.shape[1], 4 * ff), BF16),
        pltpu.VMEM((2 * ff, wd.shape[2]), BF16),
        pltpu.VMEM((2 * rows1, 4 * ff), F32),
        pltpu.VMEM((8, NCH, rows1, width), F32),
        pltpu.VMEM(ring, BF16),
        pltpu.VMEM(ring, BF16),
        pltpu.VMEM(ring, BF16),
        pltpu.VMEM(ring, BF16),
        pltpu.VMEM(msg, BF16),
        pltpu.VMEM(msg, BF16),
        dma((4,)),
        dma((4,)),
        dma((2,)),
        dma((2,)),
        dma((2,)),
        dma((2,)),
        dma((2,)),
        dma((6,)),
        dma((2,)),
        dma((2,)),
        dma((2, 4)),
        dma((2, 5, NCH)),
        dma((2, 4)),
        dma((2, 4, NCH)),
        dma((2,)),
    ]
    return pl.pallas_call(
        functools.partial(body, nsp, ntp),
        out_shape=jax.ShapeDtypeStruct(resid.shape, BF16),
        in_specs=[vmem] * 12 + [hbm] + [vmem] * 3 + [hbm] * 3,
        out_specs=vmem,
        scratch_shapes=scratch,
        compiler_params=pltpu.CompilerParams(
            collective_id=0, has_side_effects=True, vmem_limit_bytes=56 * 1024 * 1024
        ),
        name="layer",
    )(
        resid,
        v,
        k,
        q,
        og,
        raw8,
        extra8,
        rate8,
        vf,
        kf,
        qf,
        gain.reshape(1, -1),
        wout,
        ngain.reshape(1, -1),
        routes,
        cw,
        wg[0],
        wu[0],
        wd[0],
    )


def solution(mesh):
    both = ("sp", "tp")
    return jax.shard_map(
        functools.partial(layer, mesh.shape["sp"], mesh.shape["tp"]),
        mesh=mesh,
        in_specs=(
            P(both, None),
            P("sp", "tp"),
            P("sp", "tp"),
            P("sp", "tp"),
            P("sp", "tp"),
            P(None, "sp", "tp"),
            P(None, "tp"),
            P("sp", "tp"),
            P(None, "tp"),
            P(None, "tp"),
            P(None, "tp"),
            P("tp"),
            P(None, "tp"),
            P(),
            P("sp", None),
            P(both, None),
            P("sp", None, "tp"),
            P("sp", None, "tp"),
            P("sp", "tp", None),
        ),
        out_specs=P(both, None),
        check_vma=False,
    )
```

```python
import functools

import jax
import jax.numpy as jnp
from jax import lax
from jax.experimental import pallas as pl
from jax.experimental.pallas import tpu as pltpu
from jax.sharding import PartitionSpec as P

MESH = pl.DeviceIdType.MESH
HIGH = lax.Precision.HIGHEST
F32 = jnp.float32
BF16 = jnp.bfloat16
EPS = 1e-06
BLOCK = 128
NCH = 4
WIDE = 1024
NSMALL = 15


def dot(a, b, contract=((1,), (0,)), precision=None):
    return lax.dot_general(
        a, b, (contract, ((), ())), preferred_element_type=F32, precision=precision
    )


def silu(v):
    return v / (1.0 + jnp.exp(-v))


def rcopy(src, dst, send, recv, dev):
    return pltpu.make_async_remote_copy(
        src_ref=src, dst_ref=dst, send_sem=send, recv_sem=recv, device_id=dev, device_id_type=MESH
    )


def wait_bytes(ref, sem):
    pltpu.make_async_copy(ref, ref, sem).wait()


def peer(i, me, n):
    step = n - 2 - i
    return (me + jnp.where(step % 2 == 0, step // 2 + 1, n - 1 - step // 2)) % n


def iota(shape, dim):
    return lax.broadcasted_iota(jnp.int32, shape, dim)


def body(
    nsp,
    ntp,
    *refs,
):
    small_hbm, (wout, wg, wu, wd), out = refs[:NSMALL], refs[NSMALL : NSMALL + 4], refs[NSMALL + 4]
    small = refs[NSMALL + 5 : 2 * NSMALL + 5]
    resid, v_in, k_in, q_in, og_in, raw_in, hdl_in, extra_in = small[:8]
    vf_in, kf_in, qf_in, gain_in, ngain_in, routes_in, cw_in = small[8:]
    (
    raw8,
    hl,
    hr,
    pad,
    tot_s,
    tot_r,
    st_s,
    st_r,
    sc_f,
    sc_s,
    sc_r,
    heads,
    wc,
    po,
    mo,
    dm,
    dr,
    rowsf,
    xs,
    wgu,
    wdn,
    acc,
    zs,
    sp_b,
    sn_b,
    rp_b,
    rn_b,
    bm,
    br,
    lsem,
    hsem,
    tsem,
    ssem,
    osem,
    hdsem,
    wsem,
    swsem,
    psem,
    dsem,
    ag_send,
    ag_recv,
    rs_send,
    rs_recv,
    bsem,
    isem,
    ) = refs[2 * NSMALL + 5 :]
    me = lax.axis_index("sp")
    tp = lax.axis_index("tp")
    ny = ntp // 2
    y = tp // 2
    c = tp % 2
    partner = y * 2 + (1 - c)
    right_y = ((y + 1) % ny) * 2 + c
    left_y = ((y + ny - 1) % ny) * 2 + c
    others = nsp - 1
    inputs = [
        pltpu.make_async_copy(src, dst, isem.at[n]) for n, (src, dst) in enumerate(zip(small_hbm, small))
    ]
    for n in (5, 6, 7, 1, 2, 3, 8, 9, 10, 4, 13, 14, 0, 11, 12):
        inputs[n].start()

    bar = pltpu.get_barrier_semaphore()

    @pl.loop(1, nsp)
    def _(i):
        pl.semaphore_signal(bar, inc=1, device_id={"sp": (me + i) % nsp}, device_id_type=MESH)

    @pl.loop(1, ntp)
    def _(i):
        pl.semaphore_signal(bar, inc=1, device_id={"tp": (tp + i) % ntp}, device_id_type=MESH)

    ff = wg.shape[1]
    chan = wout.shape[0] // ny
    ycol = pl.ds(pl.multiple_of(y * 128, 128), 128)
    loads = [
        pltpu.make_async_copy(wout.at[pl.ds(pl.multiple_of(y * chan, chan), chan)], wc.at[:, ycol], lsem.at[0]),
        pltpu.make_async_copy(wg, wgu.at[:, pl.ds(0, ff)], lsem.at[1]),
        pltpu.make_async_copy(wu, wgu.at[:, pl.ds(2 * ff, ff)], lsem.at[2]),
        pltpu.make_async_copy(wd, wdn.at[pl.ds(0, ff)], lsem.at[3]),
    ]
    for load in loads:
        load.start()

    for n in (5, 6, 7):
        inputs[n].wait()
    raw8[0, 0:4] = raw_in[0].astype(F32)
    raw8[0, 4:8] = raw_in[1].astype(F32)
    raw8[1, 0:4] = extra_in[...]
    raw8[1, 4:8] = extra_in[...]
    sub = iota((8, 1), 0)
    rates = jnp.where(
        sub < 4, jnp.broadcast_to(hdl_in[0:1], (8, 4)), jnp.broadcast_to(hdl_in[1:2], (8, 4))
    )
    rates = jnp.sum(jnp.where(iota((8, 4), 0) % 4 == iota((8, 4), 1), rates, 0.0), axis=1, keepdims=True)
    step8 = raw8[0]
    step8 = jnp.maximum(step8, 0.0) + jnp.log1p(jnp.exp(-jnp.abs(step8)))
    log8 = raw8[1] - jnp.exp(rates) * step8
    lane = iota((1, 128), 1)
    row = iota((BLOCK, BLOCK), 0)
    col = iota((BLOCK, BLOCK), 1)
    upper = (row <= col).astype(F32)
    spread = ((iota((8, 512), 1) // 64) == iota((8, 512), 0)).astype(F32)
    cum, cum_t, tot_c, sw8, rd8 = [], [], [], [], []
    for b in range(2):
        logs = log8[:, b * BLOCK : (b + 1) * BLOCK]
        run = dot(logs, upper, precision=HIGH)
        total = run[:, BLOCK - 1 : BLOCK]
        both = jnp.where(sub < 4, run, run - logs)
        cum_t.append(both)
        cum.append(jnp.concatenate([both, jnp.zeros((120, BLOCK), F32)], axis=0).T)
        tot_c.append(jnp.broadcast_to(total, (8, 128)))
        sw8.append(jnp.exp(jnp.where(sub < 4, total - both, both)))
        rd8.append(jnp.exp(jnp.where(sub < 4, both, total - both)))
    tot_dev = jnp.exp(tot_c[0] + tot_c[1])
    tot_s[...] = tot_dev
    tot_r[me] = tot_dev
    first = ((0,), (0,))
    step_x = dot(step8, spread, first, HIGH)
    sw_x = [dot(sw8[b], spread, first, HIGH) for b in range(2)]
    rd_x = [dot(rd8[b], spread, first, HIGH) for b in range(2)]

    def head_rows(b, first):
        e = jnp.exp(tot_c[b][first : first + 4])
        return jnp.concatenate([jnp.broadcast_to(e[h : h + 1], (64, 128)) for h in range(4)], axis=0)

    tokens = v_in.shape[0]
    for n in (1, 2, 3):
        inputs[n].wait()
    pad[16 : 16 + tokens, 0:256] = v_in[...].astype(F32)
    pad[16 : 16 + tokens, 256:384] = k_in[...].astype(F32)
    pad[16 : 16 + tokens, 384:512] = q_in[...].astype(F32)
    for n in (0, 4, *range(8, NSMALL)):
        inputs[n].wait()

    pl.semaphore_wait(bar, nsp - 1 + ntp - 1)

    right = {"sp": (me + 1) % nsp}
    left = {"sp": (me + nsp - 1) % nsp}
    for ref, lo, width in ((v_in, 0, 256), (k_in, 256, 128), (q_in, 384, 128)):
        cols = pl.ds(lo, width)
        rcopy(ref.at[pl.ds(tokens - 16, 16)], hl.at[:, cols], hsem.at[0], hsem.at[1], right).start()
        rcopy(ref.at[pl.ds(0, 16)], hr.at[:, cols], hsem.at[2], hsem.at[3], left).start()

    @pl.loop(1, ny)
    def _(i):
        dst = (y + i) % ny
        rcopy(
            wout.at[pl.ds(pl.multiple_of(dst * chan, chan), chan)],
            wc.at[:, ycol],
            wsem.at[0],
            wsem.at[1],
            {"tp": dst * 2 + c},
        ).start()

    @pl.loop(0, nsp - 1)
    def _(i):
        rcopy(tot_s, tot_r.at[me], tsem.at[0], tsem.at[1], {"sp": peer(i, me, nsp)}).start()

    swaps = [
        rcopy(wg, wgu.at[:, pl.ds(ff, ff)], swsem.at[0], swsem.at[1], {"tp": partner}),
        rcopy(wu, wgu.at[:, pl.ds(3 * ff, ff)], swsem.at[2], swsem.at[3], {"tp": partner}),
        rcopy(wd, wdn.at[pl.ds(ff, ff)], swsem.at[4], swsem.at[5], {"tp": partner}),
    ]
    for swap in swaps:
        swap.start()

    wait_bytes(hl, hsem.at[1])
    wait_bytes(hr, hsem.at[3])
    pad[0:16] = jnp.where(me > 0, hl[...].astype(F32), 0.0)
    pad[16 + tokens : 32 + tokens] = jnp.where(me < nsp - 1, hr[...].astype(F32), 0.0)
    filt = jnp.concatenate([vf_in[...], kf_in[...], qf_in[...]], axis=1).astype(F32)
    conv = filt[0:1] * pad[14 : 14 + tokens]
    for o in range(1, 5):
        conv = conv + filt[o : o + 1] * pad[14 + o : 14 + o + tokens]
    values = conv[:, 0:256].astype(BF16).astype(F32)
    keys = silu(conv[:, 256:384]).astype(BF16)
    queries = silu(conv[:, 384:512]).astype(BF16)
    scaled = (jnp.concatenate([values, values], axis=1) * step_x).astype(BF16)

    part = []
    for b in range(2):
        rows = slice(b * BLOCK, (b + 1) * BLOCK)
        weighted = (scaled[rows].astype(F32) * sw_x[b]).astype(BF16)
        part.append(dot(weighted, keys[rows], ((0,), (0,))))
    final_f = head_rows(1, 0) * part[0][0:256] + part[1][0:256]
    final_b = head_rows(0, 4) * part[1][256:512] + part[0][256:512]
    piece = 256 // nsp
    mine = jnp.concatenate(
        [final_f.reshape(nsp, piece, 128), final_b.reshape(nsp, piece, 128)], axis=1
    ).astype(BF16)
    st_s[...] = mine

    @pl.loop(0, nsp - 1)
    def _(i):
        dst = peer(i, me, nsp)
        rcopy(st_s.at[dst], st_r.at[me], ssem.at[0], ssem.at[1], {"sp": dst}).start()

    st_r[me] = st_s[me]

    inner = []
    lo_half = lane < 64
    for b in range(2):
        rows = slice(b * BLOCK, (b + 1) * BLOCK)
        score = dot(queries[rows], keys[rows], ((1,), (1,)))
        pairs = []
        for pair in range(2):
            halves = []
            for h in (2 * pair, 2 * pair + 1):
                f_gap = cum[b][:, h : h + 1] - cum_t[b][h : h + 1, :]
                b_gap = cum_t[b][4 + h : 5 + h, :] - cum[b][:, 4 + h : 5 + h]
                w = score * jnp.exp(jnp.where(col <= row, f_gap, b_gap))
                w_f = jnp.where(col <= row, w, 0.0)
                w_b = jnp.where(col >= row, w, 0.0)
                both = jnp.concatenate([w_f, w_b], axis=1).astype(BF16)
                lanes = slice(128 * pair, 128 * pair + 128)
                rhs = jnp.concatenate(
                    [scaled[rows, lanes], scaled[rows, 256 + 128 * pair : 384 + 128 * pair]], axis=0
                )
                halves.append(dot(both, rhs))
            pairs.append(jnp.where(lo_half, halves[0], halves[1]))
        inner.append(jnp.concatenate(pairs, axis=1))
    gate_act = silu(og_in[...].astype(F32))

    own = tokens // ntp
    mine_lane = iota((own, tokens), 1) == iota((own, tokens), 0) + tp * own
    e_lane = iota((own, 128), 1).astype(F32)
    hots = []
    for n in range(2):
        ids = jnp.where(mine_lane, routes_in[n : n + 1].astype(F32), 0.0)
        hots.append((jnp.sum(ids, axis=1, keepdims=True) == e_lane).astype(F32))
    strict = (iota((own, own), 1) < iota((own, own), 0)).astype(F32)
    ids = e_lane * 2.0 + dot(strict, hots[0] + hots[1], precision=HIGH)
    tiles = WIDE // 128
    r_id = iota((tiles * own, nsp * 2 * tiles), 1)
    t_id = iota((tiles * own, nsp * 2 * tiles), 0)
    r_slot = ((r_id // (2 * tiles)) * 2 + r_id % 2).astype(F32)
    same = ((r_id // 2) % tiles) == (t_id // own)
    w_lane = iota((tiles * own, own), 0) % own == iota((tiles * own, own), 1)
    mixing = jnp.zeros(r_id.shape, F32)
    place = jnp.zeros(r_id.shape, F32)
    for n in range(2):
        slot = jnp.sum(hots[n] * ids, axis=1, keepdims=True)
        hit = same & (r_slot == jnp.concatenate([slot] * tiles, axis=0))
        weight = jnp.sum(jnp.where(w_lane, cw_in[n : n + 1], 0.0), axis=1, keepdims=True)
        place = jnp.where(hit, 1.0, place)
        mixing = jnp.where(hit, weight, mixing)
    place = place.astype(BF16)
    mix_hi = mixing.astype(BF16)
    mix_lo = (mixing - mix_hi.astype(F32)).astype(BF16)

    wait_bytes(tot_r.at[pl.ds(0, others)], tsem.at[1])
    wait_bytes(st_r.at[pl.ds(0, others)], ssem.at[1])
    head = me // (64 // piece)

    def forward(d, carry):
        sc_f[d, 0:piece] = carry
        decay = tot_r[d, pl.ds(head, 1), :]
        return decay * carry + st_r[d].astype(F32)[0:piece]

    def backward(i, carry):
        d = nsp - 1 - i
        sc_f[d, piece : 2 * piece] = carry
        decay = tot_r[d, pl.ds(head + 4, 1), :]
        return decay * carry + st_r[d].astype(F32)[piece : 2 * piece]

    zero = jnp.zeros((piece, 128), F32)
    lax.fori_loop(0, nsp, forward, zero)
    lax.fori_loop(0, nsp, backward, zero)
    sc_s[...] = sc_f[...].astype(BF16)

    @pl.loop(0, nsp - 1)
    def _(i):
        dst = peer(i, me, nsp)
        rcopy(sc_s.at[dst], sc_r.at[me], osem.at[0], osem.at[1], {"sp": dst}).start()

    sc_r[me] = sc_s[me]
    wait_bytes(sc_r.at[pl.ds(0, others)], osem.at[1])

    around = sc_r[...].astype(F32)
    enter = around[:, 0:piece].reshape(256, 128)
    leave = around[:, piece : 2 * piece].reshape(256, 128)
    enters = [enter, head_rows(0, 0) * enter + part[0][0:256]]
    leaves = [head_rows(1, 4) * leave + part[1][256:512], leave]
    group = (iota((256, 256), 0) // 64 == iota((256, 256), 1) // 64).astype(F32) * (1.0 / 64.0)
    for b in range(2):
        rows = slice(b * BLOCK, (b + 1) * BLOCK)
        state = jnp.concatenate([enters[b], leaves[b]], axis=0).astype(BF16)
        read = dot(queries[rows], state, ((1,), (1,))) * rd_x[b]
        gated = (inner[b] + read[:, 0:256] + read[:, 256:512]) * gate_act[rows]
        mean = dot(gated * gated, group, precision=HIGH)
        normed = gated * lax.rsqrt(mean + EPS) * gain_in[...]
        heads[c, rows, :] = normed.astype(BF16)

    swap_h = rcopy(heads.at[c], heads.at[c], hdsem.at[0], hdsem.at[1], {"tp": partner})
    swap_h.start()

    loads[0].wait()
    wait_bytes(wc.at[:, pl.ds(0, 128 * (ny - 1))], wsem.at[1])
    inner_c = chan // 2
    own_part = dot(heads[c], wc[pl.ds(pl.multiple_of(c * inner_c, inner_c), inner_c), :])
    swap_h.wait()
    o_c = 1 - c
    full = own_part + dot(heads[o_c], wc[pl.ds(pl.multiple_of(o_c * inner_c, inner_c), inner_c), :])
    po[...] = full.reshape(ntp, own, full.shape[1]).astype(BF16)

    @pl.loop(1, ntp)
    def _(i):
        dst = (tp + i) % ntp
        rcopy(po.at[dst], mo.at[tp], psem.at[0], psem.at[1], {"tp": dst}).start()

    mo[tp] = po[tp]
    wait_bytes(mo.at[pl.ds(0, ntp - 1)], psem.at[1])
    halves = []
    for core in range(2):
        total = mo[core].astype(F32)
        for other in range(1, ny):
            total = total + mo[2 * other + core].astype(F32)
        halves.append(total)
    pieces = []
    for j in range(ny):
        pieces += [halves[0][:, 128 * j : 128 * j + 128], halves[1][:, 128 * j : 128 * j + 128]]
    mixer_out = jnp.concatenate(pieces, axis=1).astype(BF16).astype(F32)
    middle = (resid[...].astype(F32) + mixer_out).astype(BF16).astype(F32)
    square = jnp.mean(middle * middle, axis=-1, keepdims=True)
    normed = (middle * lax.rsqrt(square + EPS) * ngain_in[...]).astype(BF16)
    parts = normed.shape[1] // WIDE
    width = normed.shape[1] // NCH
    per = NCH // parts
    stacked = jnp.concatenate(
        [
            jnp.concatenate(
                [normed[:, p * WIDE + n * 128 : p * WIDE + (n + 1) * 128] for n in range(tiles)], axis=0
            )
            for p in range(parts)
        ],
        axis=1,
    )
    sent = dot(place, stacked, first)
    for p in range(parts):
        dm[p] = sent[:, p * 128 : (p + 1) * 128].reshape(nsp, 2 * tiles, 128).astype(BF16)

        @pl.loop(0, nsp - 1)
        def _(i):
            dst = peer(i, me, nsp)
            rcopy(dm.at[p, dst], dr.at[p, me], dsem.at[0, p], dsem.at[1, p], {"sp": dst}).start()

        dr[p, me] = dm[p, me]

    r_dev = {"tp": right_y}
    l_dev = {"tp": left_y}
    for p in range(parts):
        wait_bytes(dr.at[p, pl.ds(0, others)], dsem.at[1, p])
        rowsf[...] = dr[p].astype(F32).reshape(nsp * 2 * tiles, 128)
        for q in range(per):
            j = p * per + q
            for n in range(width // 128):
                for s in range(2):
                    tile = q * (width // 128) + n
                    picked = rowsf[pl.ds(2 * tile + s, nsp, stride=2 * tiles), :]
                    xs[0, j, s * nsp : (s + 1) * nsp, n * 128 : (n + 1) * 128] = picked.astype(BF16)
            rcopy(xs.at[0, j], xs.at[1, j], ag_send.at[0, 0], ag_recv.at[0, 1, j], r_dev).start()
            rcopy(xs.at[0, j], xs.at[5, j], ag_send.at[1, 0], ag_recv.at[1, 1, j], l_dev).start()

    for load in loads[1:]:
        load.wait()
    for swap in swaps:
        swap.wait()

    rows1 = 2 * nsp
    top = pl.ds(0, nsp)
    low = pl.ds(nsp, nsp)

    def add_chunk(x, j, first):
        n = x.shape[0]
        w = wgu[pl.ds(pl.multiple_of(j * width, width), width), :]
        g = dot(x, w)

        @pl.when(first)
        def _():
            acc[0:n] = g

        @pl.when(jnp.logical_not(first))
        def _():
            acc[0:n] += g

    def finish(n, store):
        g = acc[0:n, 0 : 2 * ff]
        u = acc[0:n, 2 * ff : 4 * ff]
        hidden = (silu(g) * u).astype(BF16)
        for j in range(NCH):
            store(j, dot(hidden, wdn[:, j * width : (j + 1) * width]))

    def store_own(j, z):
        zs[0, j] = z

    @pl.loop(0, NCH)
    def _(j):
        add_chunk(xs[0, j], j, j == 0)

    finish(rows1, store_own)

    @pl.loop(0, 3 * NCH)
    def _(t):
        k = 1 + t // NCH
        j = t % NCH
        wait_bytes(xs.at[k, j], ag_recv.at[0, k, j])
        wait_bytes(xs.at[4 + k, j], ag_recv.at[1, k, j])

        @pl.when(k < 3)
        def _():
            rcopy(xs.at[k, j], xs.at[k + 1, j], ag_send.at[0, k], ag_recv.at[0, k + 1, j], r_dev).start()
            rcopy(xs.at[4 + k, j], xs.at[5 + k, j], ag_send.at[1, k], ag_recv.at[1, k + 1, j], l_dev).start()

        @pl.when(k == 3)
        def _():
            rcopy(
                xs.at[3, j, top], xs.at[4, j, top], ag_send.at[0, 3], ag_recv.at[0, 4, j], r_dev
            ).start()
            rcopy(
                xs.at[7, j, low], xs.at[4, j, low], ag_send.at[1, 3], ag_recv.at[1, 4, j], l_dev
            ).start()

        add_chunk(jnp.concatenate([xs[k, j], xs[4 + k, j]], axis=0), j, j == 0)

        @pl.when(j == NCH - 1)
        def _():
            def store(i, z):
                zs[k, i] = z[0:rows1]
                zs[4 + k, i] = z[rows1 : 2 * rows1]

            finish(2 * rows1, store)

    @pl.loop(0, NCH)
    def _(j):
        wait_bytes(xs.at[4, j, top], ag_recv.at[0, 4, j])
        wait_bytes(xs.at[4, j, low], ag_recv.at[1, 4, j])
        add_chunk(xs[4, j], j, j == 0)

    def store_far(j, z):
        sp_b[3, j, 0:nsp] = z[0:nsp].astype(BF16)
        sn_b[3, j, nsp:rows1] = z[nsp:rows1].astype(BF16)
        rcopy(
            sp_b.at[3, j, top], rp_b.at[3, j, top], rs_send.at[0, 3], rs_recv.at[0, 3, j], r_dev
        ).start()
        rcopy(
            sn_b.at[3, j, low], rn_b.at[3, j, low], rs_send.at[1, 3], rs_recv.at[1, 3, j], l_dev
        ).start()

    finish(rows1, store_far)

    @pl.loop(0, 3 * NCH)
    def _(t):
        k = 3 - t // NCH
        j = t % NCH

        @pl.when(k == 3)
        def _():
            wait_bytes(rp_b.at[3, j, top], rs_recv.at[0, 3, j])
            wait_bytes(rn_b.at[3, j, low], rs_recv.at[1, 3, j])
            sp_b[2, j, 0:nsp] = (zs[7, j, 0:nsp] + rp_b[3, j, 0:nsp].astype(F32)).astype(BF16)
            sp_b[2, j, nsp:rows1] = zs[7, j, nsp:rows1].astype(BF16)
            sn_b[2, j, 0:nsp] = zs[3, j, 0:nsp].astype(BF16)
            sn_b[2, j, nsp:rows1] = (
                zs[3, j, nsp:rows1] + rn_b[3, j, nsp:rows1].astype(F32)
            ).astype(BF16)

        @pl.when(k < 3)
        def _():
            wait_bytes(rp_b.at[k, j], rs_recv.at[0, k, j])
            wait_bytes(rn_b.at[k, j], rs_recv.at[1, k, j])
            sp_b[k - 1, j] = (zs[4 + k, j] + rp_b[k, j].astype(F32)).astype(BF16)
            sn_b[k - 1, j] = (zs[k, j] + rn_b[k, j].astype(F32)).astype(BF16)

        rcopy(
            sp_b.at[k - 1, j], rp_b.at[k - 1, j], rs_send.at[0, k - 1], rs_recv.at[0, k - 1, j], r_dev
        ).start()
        rcopy(
            sn_b.at[k - 1, j], rn_b.at[k - 1, j], rs_send.at[1, k - 1], rs_recv.at[1, k - 1, j], l_dev
        ).start()

    for p in range(parts):
        for q in range(per):
            j = p * per + q
            wait_bytes(rp_b.at[0, j], rs_recv.at[0, 0, j])
            wait_bytes(rn_b.at[0, j], rs_recv.at[1, 0, j])
            total = zs[0, j] + rp_b[0, j].astype(F32) + rn_b[0, j].astype(F32)
            for n in range(width // 128):
                for s in range(2):
                    tile = q * (width // 128) + n
                    rowsf[pl.ds(2 * tile + s, nsp, stride=2 * tiles), :] = total[
                        s * nsp : (s + 1) * nsp, n * 128 : (n + 1) * 128
                    ]
        bm[p] = rowsf[...].reshape(nsp, 2 * tiles, 128).astype(BF16)

        @pl.loop(0, nsp - 1)
        def _(i):
            dst = peer(i, me, nsp)
            rcopy(bm.at[p, dst], br.at[p, me], bsem.at[0, p], bsem.at[1, p], {"sp": dst}).start()

        br[p, me] = bm[p, me]

    for p in range(parts):
        wait_bytes(br.at[p, pl.ds(0, others)], bsem.at[1, p])
        back = br[p].astype(F32).reshape(nsp * 2 * tiles, 128).astype(BF16)
        mixed = dot(mix_hi, back) + dot(mix_lo, back)
        for n in range(tiles):
            cols = slice(p * WIDE + n * 128, p * WIDE + (n + 1) * 128)
            out[:, cols] = (middle[:, cols] + mixed[n * own : (n + 1) * own]).astype(BF16)

    wait_bytes(hl, hsem.at[0])
    wait_bytes(hr, hsem.at[2])
    wait_bytes(tot_r.at[pl.ds(0, others)], tsem.at[0])
    wait_bytes(st_r.at[pl.ds(0, others)], ssem.at[0])
    wait_bytes(sc_r.at[pl.ds(0, others)], osem.at[0])
    wait_bytes(wc.at[:, pl.ds(0, 128 * (ny - 1))], wsem.at[0])
    wait_bytes(mo.at[pl.ds(0, ntp - 1)], psem.at[0])
    for p in range(parts):
        wait_bytes(dr.at[p, pl.ds(0, others)], dsem.at[0, p])
        wait_bytes(br.at[p, pl.ds(0, others)], bsem.at[0, p])
    for way in range(2):
        for k in range(3):
            wait_bytes(xs.at[0], ag_send.at[way, k])
            wait_bytes(xs.at[0], rs_send.at[way, k])
        wait_bytes(xs.at[0, pl.ds(0, 2)], ag_send.at[way, 3])
        wait_bytes(xs.at[0, pl.ds(0, 2)], rs_send.at[way, 3])


def layer(nsp, ntp, resid, v, k, q, og, raw, hdl, extra, vf, kf, qf, gain, wout, ngain, routes, cw, wg, wu, wd):
    ny = ntp // 2
    tokens = v.shape[0]
    own = tokens // ntp
    width = resid.shape[1] // NCH
    ff = wg.shape[2]
    chan = wout.shape[0] // ny
    rows1 = 2 * nsp

    small = [
        resid,
        v,
        k,
        q,
        og,
        raw.transpose(0, 2, 1),
        hdl,
        extra.T,
        vf,
        kf,
        qf,
        gain.reshape(1, -1),
        ngain.reshape(1, -1),
        routes.T,
        cw.T,
    ]
    dma = pltpu.SemaphoreType.DMA
    hbm = pl.BlockSpec(memory_space=pl.ANY)
    pair = (nsp, 16, 128)
    parts = resid.shape[1] // WIDE
    msg = (parts, nsp, WIDE // 64, 128)
    ring = (4, NCH, rows1, width)
    scratch = [pltpu.VMEM(x.shape, x.dtype) for x in small] + [
        pltpu.VMEM((2, 8, tokens), F32),
        pltpu.VMEM((16, 512), BF16),
        pltpu.VMEM((16, 512), BF16),
        pltpu.VMEM((tokens + 32, 512), F32),
        pltpu.VMEM((8, 128), F32),
        pltpu.VMEM((nsp, 8, 128), F32),
        pltpu.VMEM(pair, BF16),
        pltpu.VMEM(pair, BF16),
        pltpu.VMEM(pair, F32),
        pltpu.VMEM(pair, BF16),
        pltpu.VMEM(pair, BF16),
        pltpu.VMEM((2, tokens, 256), BF16),
        pltpu.VMEM((chan, 128 * ny), BF16),
        pltpu.VMEM((ntp, own, 128 * ny), BF16),
        pltpu.VMEM((ntp, own, 128 * ny), BF16),
        pltpu.VMEM(msg, BF16),
        pltpu.VMEM(msg, BF16),
        pltpu.VMEM((nsp * WIDE // 64, 128), F32),
        pltpu.VMEM((8, NCH, rows1, width), BF16),
        pltpu.VMEM((wg.shape[1], 4 * ff), BF16),
        pltpu.VMEM((2 * ff, wd.shape[2]), BF16),
        pltpu.VMEM((2 * rows1, 4 * ff), F32),
        pltpu.VMEM((8, NCH, rows1, width), F32),
        pltpu.VMEM(ring, BF16),
        pltpu.VMEM(ring, BF16),
        pltpu.VMEM(ring, BF16),
        pltpu.VMEM(ring, BF16),
        pltpu.VMEM(msg, BF16),
        pltpu.VMEM(msg, BF16),
        dma((4,)),
        dma((4,)),
        dma((2,)),
        dma((2,)),
        dma((2,)),
        dma((2,)),
        dma((2,)),
        dma((6,)),
        dma((2,)),
        dma((2, parts)),
        dma((2, 4)),
        dma((2, 5, NCH)),
        dma((2, 4)),
        dma((2, 4, NCH)),
        dma((2, parts)),
        dma((NSMALL,)),
    ]
    return pl.pallas_call(
        functools.partial(body, nsp, ntp),
        out_shape=jax.ShapeDtypeStruct(resid.shape, BF16),
        in_specs=[hbm] * (NSMALL + 4),
        out_specs=pl.BlockSpec(memory_space=pltpu.VMEM),
        scratch_shapes=scratch,
        compiler_params=pltpu.CompilerParams(
            collective_id=0, has_side_effects=True, vmem_limit_bytes=56 * 1024 * 1024
        ),
        name="layer",
    )(*small, wout, wg[0], wu[0], wd[0])


def solution(mesh):
    both = ("sp", "tp")
    return jax.shard_map(
        functools.partial(layer, mesh.shape["sp"], mesh.shape["tp"]),
        mesh=mesh,
        in_specs=(
            P(both, None),
            P("sp", "tp"),
            P("sp", "tp"),
            P("sp", "tp"),
            P("sp", "tp"),
            P(None, "sp", "tp"),
            P(None, "tp"),
            P("sp", "tp"),
            P(None, "tp"),
            P(None, "tp"),
            P(None, "tp"),
            P("tp"),
            P(None, "tp"),
            P(),
            P("sp", None),
            P(both, None),
            P("sp", None, "tp"),
            P("sp", None, "tp"),
            P("sp", "tp", None),
        ),
        out_specs=P(both, None),
        check_vma=False,
    )
```

```python
import functools

import jax
import jax.numpy as jnp
from jax import lax
from jax.experimental import pallas as pl
from jax.experimental.pallas import tpu as pltpu
from jax.sharding import PartitionSpec as P

MESH = pl.DeviceIdType.MESH
HIGH = lax.Precision.HIGHEST
F32 = jnp.float32
BF16 = jnp.bfloat16
EPS = 1e-06
BLOCK = 128
NCH = 4
NX = 4
WIDE = 512
NSMALL = 15


def dot(a, b, contract=((1,), (0,)), precision=None):
    return lax.dot_general(
        a, b, (contract, ((), ())), preferred_element_type=F32, precision=precision
    )


def silu(v):
    return v / (1.0 + jnp.exp(-v))


def rcopy(src, dst, send, recv, dev):
    return pltpu.make_async_remote_copy(
        src_ref=src, dst_ref=dst, send_sem=send, recv_sem=recv, device_id=dev, device_id_type=MESH
    )


def wait_bytes(ref, sem):
    pltpu.make_async_copy(ref, ref, sem).wait()


def peer(i, me, n):
    step = n - 2 - i
    return (me + jnp.where(step % 2 == 0, step // 2 + 1, n - 1 - step // 2)) % n


def iota(shape, dim):
    return lax.broadcasted_iota(jnp.int32, shape, dim)


def body(
    nsp,
    ntp,
    *refs,
):
    small_hbm, (wout, wg, wu, wd), out = refs[:NSMALL], refs[NSMALL : NSMALL + 4], refs[NSMALL + 4]
    small = refs[NSMALL + 5 : 2 * NSMALL + 5]
    resid, v_in, k_in, q_in, og_in, raw_in, hdl_in, extra_in = small[:8]
    vf_in, kf_in, qf_in, gain_in, ngain_in, routes_in, cw_in = small[8:]
    (
    raw8,
    hl,
    hr,
    pad,
    tot_s,
    tot_r,
    decay,
    st_s,
    st_r,
    sc_f,
    sc_s,
    sc_r,
    heads,
    wc,
    po,
    mo,
    near,
    through,
    dm,
    dr,
    rowsf,
    xs,
    wgu,
    wdn,
    acc,
    hidden,
    zs,
    sp_b,
    sn_b,
    rp_b,
    rn_b,
    bm,
    br,
    lsem,
    hsem,
    tsem,
    ssem,
    osem,
    hdsem,
    wsem,
    wsend,
    wrecv,
    swsem,
    psem,
    nsem,
    dsem,
    ag_send,
    ag_recv,
    rs_send,
    rs_recv,
    bsem,
    isem,
    ) = refs[2 * NSMALL + 5 :]
    me = lax.axis_index("sp")
    tp = lax.axis_index("tp")
    ny = ntp // 2
    y = tp // 2
    c = tp % 2
    partner = y * 2 + (1 - c)
    right_y = ((y + 1) % ny) * 2 + c
    left_y = ((y + ny - 1) % ny) * 2 + c
    others = nsp - 1
    inputs = [
        pltpu.make_async_copy(src, dst, isem.at[n]) for n, (src, dst) in enumerate(zip(small_hbm, small))
    ]
    for n in (5, 6, 7, 1, 2, 3, 8, 9, 10, 4, 13, 14, 0, 11, 12):
        inputs[n].start()

    bar = pltpu.get_barrier_semaphore()

    @pl.loop(1, nsp)
    def _(i):
        pl.semaphore_signal(bar, inc=1, device_id={"sp": (me + i) % nsp}, device_id_type=MESH)

    @pl.loop(1, ntp)
    def _(i):
        pl.semaphore_signal(bar, inc=1, device_id={"tp": (tp + i) % ntp}, device_id_type=MESH)

    ff = wg.shape[1]
    chan = wout.shape[0] // ny
    nx = NX
    x = me % nx
    turns = ny // nx

    def w_rows(of):
        return wout.at[pl.ds(pl.multiple_of(of * chan, chan), chan)]

    def w_block(of):
        return wc.at[:, pl.ds(pl.multiple_of(of * 128, 128), 128)]

    @pl.when(x == 0)
    def _():
        pltpu.make_async_copy(w_rows(y), w_block(y), wrecv.at[0]).start()

    loads = [
        pltpu.make_async_copy(wg, wgu.at[:, pl.ds(0, ff)], lsem.at[0]),
        pltpu.make_async_copy(wu, wgu.at[:, pl.ds(2 * ff, ff)], lsem.at[1]),
        pltpu.make_async_copy(wd, wdn.at[pl.ds(0, ff)], lsem.at[2]),
    ]
    for load in loads:
        load.start()

    for n in (5, 6, 7):
        inputs[n].wait()
    raw8[0, 0:4] = raw_in[0].astype(F32)
    raw8[0, 4:8] = raw_in[1].astype(F32)
    raw8[1, 0:4] = extra_in[...]
    raw8[1, 4:8] = extra_in[...]
    sub = iota((8, 1), 0)
    rates = jnp.where(
        sub < 4, jnp.broadcast_to(hdl_in[0:1], (8, 4)), jnp.broadcast_to(hdl_in[1:2], (8, 4))
    )
    rates = jnp.sum(jnp.where(iota((8, 4), 0) % 4 == iota((8, 4), 1), rates, 0.0), axis=1, keepdims=True)
    step8 = raw8[0]
    step8 = jnp.maximum(step8, 0.0) + jnp.log1p(jnp.exp(-jnp.abs(step8)))
    log8 = raw8[1] - jnp.exp(rates) * step8
    lane = iota((1, 128), 1)
    row = iota((BLOCK, BLOCK), 0)
    col = iota((BLOCK, BLOCK), 1)
    upper = (row <= col).astype(F32)
    spread = ((iota((8, 512), 1) // 64) == iota((8, 512), 0)).astype(F32)
    cum, cum_t, tot_c, sw8, rd8 = [], [], [], [], []
    for b in range(2):
        logs = log8[:, b * BLOCK : (b + 1) * BLOCK]
        run = dot(logs, upper, precision=HIGH)
        total = run[:, BLOCK - 1 : BLOCK]
        both = jnp.where(sub < 4, run, run - logs)
        cum_t.append(both)
        cum.append(jnp.concatenate([both, jnp.zeros((120, BLOCK), F32)], axis=0).T)
        tot_c.append(jnp.broadcast_to(total, (8, 128)))
        sw8.append(jnp.exp(jnp.where(sub < 4, total - both, both)))
        rd8.append(jnp.exp(jnp.where(sub < 4, both, total - both)))
    tot_dev = jnp.exp(tot_c[0] + tot_c[1])
    tot_row = jnp.sum(jnp.where(sub == lane, tot_dev, 0.0), axis=0, keepdims=True)
    tot_s[...] = tot_row
    tot_r[me] = tot_row
    first = ((0,), (0,))
    step_x = dot(step8, spread, first, HIGH)
    sw_x = [dot(sw8[b], spread, first, HIGH) for b in range(2)]
    rd_x = [dot(rd8[b], spread, first, HIGH) for b in range(2)]

    def head_rows(b, first):
        e = jnp.exp(tot_c[b][first : first + 4])
        return jnp.concatenate([jnp.broadcast_to(e[h : h + 1], (64, 128)) for h in range(4)], axis=0)

    tokens = v_in.shape[0]
    for n in (1, 2, 3):
        inputs[n].wait()
    pad[16 : 16 + tokens, 0:256] = v_in[...].astype(F32)
    pad[16 : 16 + tokens, 256:384] = k_in[...].astype(F32)
    pad[16 : 16 + tokens, 384:512] = q_in[...].astype(F32)
    for n in (0, 4, *range(8, NSMALL)):
        inputs[n].wait()

    pl.semaphore_wait(bar, nsp - 1 + ntp - 1)

    right = {"sp": (me + 1) % nsp}
    left = {"sp": (me + nsp - 1) % nsp}
    for ref, lo, width in ((v_in, 0, 256), (k_in, 256, 128), (q_in, 384, 128)):
        cols = pl.ds(lo, width)
        rcopy(ref.at[pl.ds(tokens - 16, 16)], hl.at[:, cols], hsem.at[0], hsem.at[1], right).start()
        rcopy(ref.at[pl.ds(0, 16)], hr.at[:, cols], hsem.at[2], hsem.at[3], left).start()

    @pl.loop(0, nsp - 1)
    def _(i):
        rcopy(tot_s, tot_r.at[me], tsem.at[0], tsem.at[1], {"sp": peer(i, me, nsp)}).start()

    def w_send(m):
        dst = (y + ny - x - m * nx) % ny
        return rcopy(w_rows(dst), w_block(y), wsend.at[m], wrecv.at[m], {"tp": dst * 2 + c})

    @pl.when(x > 0)
    def _():
        w_send(0).start()

    for m in range(1, turns):
        w_send(m).start()

    def w_relay(m):
        block = w_block((y + x + m * nx) % ny)
        wait_bytes(block, wrecv.at[m])
        for i in range(1, nx):
            to = me - x + (x + i) % nx
            rcopy(block, block, wsem.at[0], wsem.at[1], {"sp": to}).start()

    wait_bytes(hl, hsem.at[1])
    wait_bytes(hr, hsem.at[3])
    pad[0:16] = jnp.where(me > 0, hl[...].astype(F32), 0.0)
    pad[16 + tokens : 32 + tokens] = jnp.where(me < nsp - 1, hr[...].astype(F32), 0.0)
    filt = jnp.concatenate([vf_in[...], kf_in[...], qf_in[...]], axis=1).astype(F32)
    conv = filt[0:1] * pad[14 : 14 + tokens]
    for o in range(1, 5):
        conv = conv + filt[o : o + 1] * pad[14 + o : 14 + o + tokens]
    values = conv[:, 0:256].astype(BF16).astype(F32)
    keys = silu(conv[:, 256:384]).astype(BF16)
    queries = silu(conv[:, 384:512]).astype(BF16)
    scaled = (jnp.concatenate([values, values], axis=1) * step_x).astype(BF16)

    part = []
    for b in range(2):
        rows = slice(b * BLOCK, (b + 1) * BLOCK)
        weighted = (scaled[rows].astype(F32) * sw_x[b]).astype(BF16)
        part.append(dot(weighted, keys[rows], ((0,), (0,))))
    final_f = head_rows(1, 0) * part[0][0:256] + part[1][0:256]
    final_b = head_rows(0, 4) * part[1][256:512] + part[0][256:512]
    piece = 256 // nsp
    mine = jnp.concatenate(
        [final_f.reshape(nsp, piece, 128), final_b.reshape(nsp, piece, 128)], axis=1
    ).astype(BF16)
    st_s[...] = mine

    @pl.loop(0, nsp - 1)
    def _(i):
        dst = peer(i, me, nsp)
        rcopy(st_s.at[dst], st_r.at[me], ssem.at[0], ssem.at[1], {"sp": dst}).start()

    st_r[me] = st_s[me]

    inner = []
    lo_half = lane < 64
    for b in range(2):
        rows = slice(b * BLOCK, (b + 1) * BLOCK)
        score = dot(queries[rows], keys[rows], ((1,), (1,)))
        pairs = []
        for pair in range(2):
            halves = []
            for h in (2 * pair, 2 * pair + 1):
                f_gap = cum[b][:, h : h + 1] - cum_t[b][h : h + 1, :]
                b_gap = cum_t[b][4 + h : 5 + h, :] - cum[b][:, 4 + h : 5 + h]
                w = score * jnp.exp(jnp.where(col <= row, f_gap, b_gap))
                w_f = jnp.where(col <= row, w, 0.0)
                w_b = jnp.where(col >= row, w, 0.0)
                both = jnp.concatenate([w_f, w_b], axis=1).astype(BF16)
                lanes = slice(128 * pair, 128 * pair + 128)
                rhs = jnp.concatenate(
                    [scaled[rows, lanes], scaled[rows, 256 + 128 * pair : 384 + 128 * pair]], axis=0
                )
                halves.append(dot(both, rhs))
            pairs.append(jnp.where(lo_half, halves[0], halves[1]))
        inner.append(jnp.concatenate(pairs, axis=1))
    gate_act = silu(og_in[...].astype(F32))

    own = tokens // ntp
    mine_lane = iota((own, tokens), 1) == iota((own, tokens), 0) + tp * own
    e_lane = iota((own, 128), 1).astype(F32)
    hots = []
    for n in range(2):
        ids = jnp.where(mine_lane, routes_in[n : n + 1].astype(F32), 0.0)
        hots.append((jnp.sum(ids, axis=1, keepdims=True) == e_lane).astype(F32))
    strict = (iota((own, own), 1) < iota((own, own), 0)).astype(F32)
    ids = e_lane * 2.0 + dot(strict, hots[0] + hots[1], precision=HIGH)
    tiles = WIDE // 128
    r_id = iota((tiles * own, nsp * 2 * tiles), 1)
    t_id = iota((tiles * own, nsp * 2 * tiles), 0)
    r_slot = ((r_id // (2 * tiles)) * 2 + r_id % 2).astype(F32)
    same = ((r_id // 2) % tiles) == (t_id // own)
    w_lane = iota((tiles * own, own), 0) % own == iota((tiles * own, own), 1)
    mixing = jnp.zeros(r_id.shape, F32)
    place = jnp.zeros(r_id.shape, F32)
    for n in range(2):
        slot = jnp.sum(hots[n] * ids, axis=1, keepdims=True)
        hit = same & (r_slot == jnp.concatenate([slot] * tiles, axis=0))
        weight = jnp.sum(jnp.where(w_lane, cw_in[n : n + 1], 0.0), axis=1, keepdims=True)
        place = jnp.where(hit, 1.0, place)
        mixing = jnp.where(hit, weight, mixing)
    place = place.astype(BF16)
    mix_hi = mixing.astype(BF16)
    mix_lo = (mixing - mix_hi.astype(F32)).astype(BF16)

    w_relay(0)

    wait_bytes(tot_r.at[pl.ds(0, others)], tsem.at[1])
    wait_bytes(st_r.at[pl.ds(0, others)], ssem.at[1])
    head = me // (64 // piece)
    totals = jnp.concatenate([tot_r[d] for d in range(nsp)], axis=0)
    for n in range(2):
        of_head = jnp.sum(jnp.where(lane == head + 4 * n, totals, 0.0), axis=1, keepdims=True)
        decay[n] = jnp.broadcast_to(of_head, (nsp, 128))

    def forward(d, carry):
        sc_f[d, 0:piece] = carry
        return decay[0, pl.ds(d, 1), :] * carry + st_r[d].astype(F32)[0:piece]

    def backward(i, carry):
        d = nsp - 1 - i
        sc_f[d, piece : 2 * piece] = carry
        return decay[1, pl.ds(d, 1), :] * carry + st_r[d].astype(F32)[piece : 2 * piece]

    zero = jnp.zeros((piece, 128), F32)
    lax.fori_loop(0, nsp, forward, zero)
    lax.fori_loop(0, nsp, backward, zero)
    sc_s[...] = sc_f[...].astype(BF16)

    @pl.loop(0, nsp - 1)
    def _(i):
        dst = peer(i, me, nsp)
        rcopy(sc_s.at[dst], sc_r.at[me], osem.at[0], osem.at[1], {"sp": dst}).start()

    sc_r[me] = sc_s[me]
    for m in range(1, turns):
        w_relay(m)

    wait_bytes(sc_r.at[pl.ds(0, others)], osem.at[1])

    around = sc_r[...].astype(F32)
    enter = around[:, 0:piece].reshape(256, 128)
    leave = around[:, piece : 2 * piece].reshape(256, 128)
    enters = [enter, head_rows(0, 0) * enter + part[0][0:256]]
    leaves = [head_rows(1, 4) * leave + part[1][256:512], leave]
    group = (iota((256, 256), 0) // 64 == iota((256, 256), 1) // 64).astype(F32) * (1.0 / 64.0)
    for b in range(2):
        rows = slice(b * BLOCK, (b + 1) * BLOCK)
        state = jnp.concatenate([enters[b], leaves[b]], axis=0).astype(BF16)
        read = dot(queries[rows], state, ((1,), (1,))) * rd_x[b]
        gated = (inner[b] + read[:, 0:256] + read[:, 256:512]) * gate_act[rows]
        mean = dot(gated * gated, group, precision=HIGH)
        normed = gated * lax.rsqrt(mean + EPS) * gain_in[...]
        heads[c, rows, :] = normed.astype(BF16)

    swap_h = rcopy(heads.at[c], heads.at[c], hdsem.at[0], hdsem.at[1], {"tp": partner})
    swap_h.start()

    far_w = wc.at[:, pl.ds(0, 128 * (ny - turns))]
    wait_bytes(far_w, wsem.at[1])
    inner_c = chan // 2
    own_part = dot(heads[c], wc[pl.ds(pl.multiple_of(c * inner_c, inner_c), inner_c), :])
    swap_h.wait()
    o_c = 1 - c
    full = own_part + dot(heads[o_c], wc[pl.ds(pl.multiple_of(o_c * inner_c, inner_c), inner_c), :])
    po[...] = full.reshape(ntp, own, full.shape[1]).astype(BF16)

    def chip(distance, core):
        return ((y + ny + distance) % ny) * 2 + core

    relays = []
    for way in range(2):
        sign = 1 - 2 * way
        for core in range(2):
            copy = rcopy(
                po.at[chip(3 * sign, core)],
                near.at[way, core],
                nsem.at[0, way, core],
                nsem.at[1, way, core],
                {"tp": chip(sign, c)},
            )
            copy.start()
            relays.append(copy)
    for distance in (4, 1, -1):
        for core in range(2):
            dst = chip(distance, core)
            rcopy(po.at[dst], mo.at[tp], psem.at[0], psem.at[1], {"tp": dst}).start()
    rcopy(po.at[partner], mo.at[tp], psem.at[0], psem.at[1], {"tp": partner}).start()
    mo[tp] = po[tp]
    for way in range(2):
        for core in range(2):
            dst = chip(2 - 4 * way, core)
            relays[2 * way + core].wait_recv()
            through[way, core] = (po[dst].astype(F32) + near[way, core].astype(F32)).astype(BF16)
            rcopy(through.at[way, core], mo.at[tp], psem.at[0], psem.at[1], {"tp": dst}).start()

    swaps = [
        rcopy(wg, wgu.at[:, pl.ds(ff, ff)], swsem.at[0], swsem.at[1], {"tp": partner}),
        rcopy(wu, wgu.at[:, pl.ds(3 * ff, ff)], swsem.at[2], swsem.at[3], {"tp": partner}),
        rcopy(wd, wdn.at[pl.ds(ff, ff)], swsem.at[4], swsem.at[5], {"tp": partner}),
    ]
    for swap in swaps:
        swap.start()

    wait_bytes(mo.at[pl.ds(0, ntp - 5)], psem.at[1])
    halves = []
    for core in range(2):
        total = mo[chip(0, core)].astype(F32)
        for distance in (1, -1, 2, -2, 4):
            total = total + mo[chip(distance, core)].astype(F32)
        halves.append(total)
    pieces = []
    for j in range(ny):
        pieces += [halves[0][:, 128 * j : 128 * j + 128], halves[1][:, 128 * j : 128 * j + 128]]
    mixer_out = jnp.concatenate(pieces, axis=1).astype(BF16).astype(F32)
    middle = (resid[...].astype(F32) + mixer_out).astype(BF16).astype(F32)
    square = jnp.mean(middle * middle, axis=-1, keepdims=True)
    normed = (middle * lax.rsqrt(square + EPS) * ngain_in[...]).astype(BF16)
    parts = normed.shape[1] // WIDE
    width = normed.shape[1] // NCH
    per = NCH // parts
    stacked = jnp.concatenate(
        [
            jnp.concatenate(
                [normed[:, p * WIDE + n * 128 : p * WIDE + (n + 1) * 128] for n in range(tiles)], axis=0
            )
            for p in range(parts)
        ],
        axis=1,
    )
    sent = dot(place, stacked, first)
    for p in range(parts):
        dm[p] = sent[:, p * 128 : (p + 1) * 128].reshape(nsp, 2 * tiles, 128).astype(BF16)

        @pl.loop(0, nsp - 1)
        def _(i):
            dst = peer(i, me, nsp)
            rcopy(dm.at[p, dst], dr.at[p, me], dsem.at[0, p], dsem.at[1, p], {"sp": dst}).start()

        dr[p, me] = dm[p, me]

    r_dev = {"tp": right_y}
    l_dev = {"tp": left_y}
    for p in range(parts):
        wait_bytes(dr.at[p, pl.ds(0, others)], dsem.at[1, p])
        rowsf[...] = dr[p].astype(F32).reshape(nsp * 2 * tiles, 128)
        for q in range(per):
            j = p * per + q
            for n in range(width // 128):
                for s in range(2):
                    tile = q * (width // 128) + n
                    picked = rowsf[pl.ds(2 * tile + s, nsp, stride=2 * tiles), :]
                    xs[0, j, s * nsp : (s + 1) * nsp, n * 128 : (n + 1) * 128] = picked.astype(BF16)
            rcopy(xs.at[0, j], xs.at[1, j], ag_send.at[0, 0], ag_recv.at[0, 1, j], r_dev).start()
            rcopy(xs.at[0, j], xs.at[5, j], ag_send.at[1, 0], ag_recv.at[1, 1, j], l_dev).start()

    for load in loads:
        load.wait()
    for swap in swaps:
        swap.wait()

    rows1 = 2 * nsp
    top = pl.ds(0, nsp)
    low = pl.ds(nsp, nsp)

    def add_chunk(rows, j):
        n = rows.shape[0]
        w = wgu[pl.ds(pl.multiple_of(j * width, width), width), :]
        acc[0:n] = jnp.where(j == 0, 0.0, acc[0:n]) + dot(rows, w)

    def activate(n):
        hidden[0:n] = (silu(acc[0:n, 0 : 2 * ff]) * acc[0:n, 2 * ff : 4 * ff]).astype(BF16)

    def down(n, j):
        return dot(hidden[0:n], wdn[:, pl.ds(pl.multiple_of(j * width, width), width)])

    def down_pair(k, j):
        z = down(2 * rows1, j)
        zs[k, j] = z[0:rows1]
        zs[4 + k, j] = z[rows1 : 2 * rows1]

    @pl.loop(0, NCH)
    def _(j):
        add_chunk(xs[0, j], j)

    activate(rows1)

    @pl.loop(0, NCH)
    def _(j):
        zs[0, j] = down(rows1, j)

    @pl.loop(0, 3 * NCH)
    def _(t):
        k = 1 + t // NCH
        j = t % NCH
        wait_bytes(xs.at[k, j], ag_recv.at[0, k, j])
        wait_bytes(xs.at[4 + k, j], ag_recv.at[1, k, j])

        @pl.when(k < 3)
        def _():
            rcopy(xs.at[k, j], xs.at[k + 1, j], ag_send.at[0, k], ag_recv.at[0, k + 1, j], r_dev).start()
            rcopy(xs.at[4 + k, j], xs.at[5 + k, j], ag_send.at[1, k], ag_recv.at[1, k + 1, j], l_dev).start()

        @pl.when(k == 3)
        def _():
            rcopy(
                xs.at[3, j, top], xs.at[4, j, top], ag_send.at[0, 3], ag_recv.at[0, 4, j], r_dev
            ).start()
            rcopy(
                xs.at[7, j, low], xs.at[4, j, low], ag_send.at[1, 3], ag_recv.at[1, 4, j], l_dev
            ).start()

        add_chunk(jnp.concatenate([xs[k, j], xs[4 + k, j]], axis=0), j)

        @pl.when(k > 1)
        def _():
            down_pair(k - 1, j)

        @pl.when(j == NCH - 1)
        def _():
            activate(2 * rows1)

    @pl.loop(0, NCH)
    def _(j):
        down_pair(3, j)
        sp_b[2, j, nsp:rows1] = zs[7, j, nsp:rows1].astype(BF16)
        sn_b[2, j, 0:nsp] = zs[3, j, 0:nsp].astype(BF16)
        rcopy(
            sp_b.at[2, j, low], rp_b.at[2, j, low], rs_send.at[0, 2], rs_recv.at[0, 2, j], r_dev
        ).start()
        rcopy(
            sn_b.at[2, j, top], rn_b.at[2, j, top], rs_send.at[1, 2], rs_recv.at[1, 2, j], l_dev
        ).start()
        wait_bytes(xs.at[4, j, top], ag_recv.at[0, 4, j])
        wait_bytes(xs.at[4, j, low], ag_recv.at[1, 4, j])
        add_chunk(xs[4, j], j)

    activate(rows1)

    @pl.loop(0, NCH)
    def _(j):
        z = down(rows1, j)
        sp_b[3, j, 0:nsp] = z[0:nsp].astype(BF16)
        sn_b[3, j, nsp:rows1] = z[nsp:rows1].astype(BF16)
        rcopy(
            sp_b.at[3, j, top], rp_b.at[3, j, top], rs_send.at[0, 3], rs_recv.at[0, 3, j], r_dev
        ).start()
        rcopy(
            sn_b.at[3, j, low], rn_b.at[3, j, low], rs_send.at[1, 3], rs_recv.at[1, 3, j], l_dev
        ).start()

    @pl.loop(0, NCH)
    def _(j):
        wait_bytes(rp_b.at[3, j, top], rs_recv.at[0, 3, j])
        wait_bytes(rn_b.at[3, j, low], rs_recv.at[1, 3, j])
        sp_b[2, j, 0:nsp] = (zs[7, j, 0:nsp] + rp_b[3, j, 0:nsp].astype(F32)).astype(BF16)
        sn_b[2, j, nsp:rows1] = (zs[3, j, nsp:rows1] + rn_b[3, j, nsp:rows1].astype(F32)).astype(BF16)
        rcopy(
            sp_b.at[2, j, top], rp_b.at[2, j, top], rs_send.at[0, 2], rs_recv.at[0, 2, j], r_dev
        ).start()
        rcopy(
            sn_b.at[2, j, low], rn_b.at[2, j, low], rs_send.at[1, 2], rs_recv.at[1, 2, j], l_dev
        ).start()

    @pl.loop(0, 2 * NCH)
    def _(t):
        k = 2 - t // NCH
        j = t % NCH
        wait_bytes(rp_b.at[k, j], rs_recv.at[0, k, j])
        wait_bytes(rn_b.at[k, j], rs_recv.at[1, k, j])
        sp_b[k - 1, j] = (zs[4 + k, j] + rp_b[k, j].astype(F32)).astype(BF16)
        sn_b[k - 1, j] = (zs[k, j] + rn_b[k, j].astype(F32)).astype(BF16)
        rcopy(
            sp_b.at[k - 1, j], rp_b.at[k - 1, j], rs_send.at[0, k - 1], rs_recv.at[0, k - 1, j], r_dev
        ).start()
        rcopy(
            sn_b.at[k - 1, j], rn_b.at[k - 1, j], rs_send.at[1, k - 1], rs_recv.at[1, k - 1, j], l_dev
        ).start()

    for p in range(parts):
        for q in range(per):
            j = p * per + q
            wait_bytes(rp_b.at[0, j], rs_recv.at[0, 0, j])
            wait_bytes(rn_b.at[0, j], rs_recv.at[1, 0, j])
            total = zs[0, j] + rp_b[0, j].astype(F32) + rn_b[0, j].astype(F32)
            for n in range(width // 128):
                for s in range(2):
                    tile = q * (width // 128) + n
                    rowsf[pl.ds(2 * tile + s, nsp, stride=2 * tiles), :] = total[
                        s * nsp : (s + 1) * nsp, n * 128 : (n + 1) * 128
                    ]
        bm[p] = rowsf[...].reshape(nsp, 2 * tiles, 128).astype(BF16)

        @pl.loop(0, nsp - 1)
        def _(i):
            dst = peer(i, me, nsp)
            rcopy(bm.at[p, dst], br.at[p, me], bsem.at[0, p], bsem.at[1, p], {"sp": dst}).start()

        br[p, me] = bm[p, me]

    for p in range(parts):
        wait_bytes(br.at[p, pl.ds(0, others)], bsem.at[1, p])
        back = br[p].astype(F32).reshape(nsp * 2 * tiles, 128).astype(BF16)
        mixed = dot(mix_hi, back) + dot(mix_lo, back)
        for n in range(tiles):
            cols = slice(p * WIDE + n * 128, p * WIDE + (n + 1) * 128)
            out[:, cols] = (middle[:, cols] + mixed[n * own : (n + 1) * own]).astype(BF16)

    wait_bytes(hl, hsem.at[0])
    wait_bytes(hr, hsem.at[2])
    wait_bytes(tot_r.at[pl.ds(0, others)], tsem.at[0])
    wait_bytes(st_r.at[pl.ds(0, others)], ssem.at[0])
    wait_bytes(sc_r.at[pl.ds(0, others)], osem.at[0])
    wait_bytes(far_w, wsem.at[0])

    @pl.when(x > 0)
    def _():
        wait_bytes(w_block(0), wsend.at[0])

    for m in range(1, turns):
        wait_bytes(w_block(0), wsend.at[m])
    wait_bytes(mo.at[pl.ds(0, ntp - 5)], psem.at[0])
    for copy in relays:
        copy.wait_send()
    for p in range(parts):
        wait_bytes(dr.at[p, pl.ds(0, others)], dsem.at[0, p])
        wait_bytes(br.at[p, pl.ds(0, others)], bsem.at[0, p])
    for way in range(2):
        for k in range(3):
            wait_bytes(xs.at[0], ag_send.at[way, k])
            wait_bytes(xs.at[0], rs_send.at[way, k])
        wait_bytes(xs.at[0, pl.ds(0, 2)], ag_send.at[way, 3])
        wait_bytes(xs.at[0, pl.ds(0, 2)], rs_send.at[way, 3])


def layer(nsp, ntp, resid, v, k, q, og, raw, hdl, extra, vf, kf, qf, gain, wout, ngain, routes, cw, wg, wu, wd):
    ny = ntp // 2
    tokens = v.shape[0]
    own = tokens // ntp
    width = resid.shape[1] // NCH
    ff = wg.shape[2]
    chan = wout.shape[0] // ny
    rows1 = 2 * nsp

    small = [
        resid,
        v,
        k,
        q,
        og,
        raw.transpose(0, 2, 1),
        hdl,
        extra.T,
        vf,
        kf,
        qf,
        gain.reshape(1, -1),
        ngain.reshape(1, -1),
        routes.T,
        cw.T,
    ]
    dma = pltpu.SemaphoreType.DMA
    hbm = pl.BlockSpec(memory_space=pl.ANY)
    pair = (nsp, 16, 128)
    parts = resid.shape[1] // WIDE
    msg = (parts, nsp, WIDE // 64, 128)
    ring = (4, NCH, rows1, width)
    scratch = [pltpu.VMEM(x.shape, x.dtype) for x in small] + [
        pltpu.VMEM((2, 8, tokens), F32),
        pltpu.VMEM((16, 512), BF16),
        pltpu.VMEM((16, 512), BF16),
        pltpu.VMEM((tokens + 32, 512), F32),
        pltpu.VMEM((1, 128), F32),
        pltpu.VMEM((nsp, 1, 128), F32),
        pltpu.VMEM((2, nsp, 128), F32),
        pltpu.VMEM(pair, BF16),
        pltpu.VMEM(pair, BF16),
        pltpu.VMEM(pair, F32),
        pltpu.VMEM(pair, BF16),
        pltpu.VMEM(pair, BF16),
        pltpu.VMEM((2, tokens, 256), BF16),
        pltpu.VMEM((chan, 128 * ny), BF16),
        pltpu.VMEM((ntp, own, 128 * ny), BF16),
        pltpu.VMEM((ntp, own, 128 * ny), BF16),
        pltpu.VMEM((2, 2, own, 128 * ny), BF16),
        pltpu.VMEM((2, 2, own, 128 * ny), BF16),
        pltpu.VMEM(msg, BF16),
        pltpu.VMEM(msg, BF16),
        pltpu.VMEM((nsp * WIDE // 64, 128), F32),
        pltpu.VMEM((8, NCH, rows1, width), BF16),
        pltpu.VMEM((wg.shape[1], 4 * ff), BF16),
        pltpu.VMEM((2 * ff, wd.shape[2]), BF16),
        pltpu.VMEM((2 * rows1, 4 * ff), F32),
        pltpu.VMEM((2 * rows1, 2 * ff), BF16),
        pltpu.VMEM((8, NCH, rows1, width), F32),
        pltpu.VMEM(ring, BF16),
        pltpu.VMEM(ring, BF16),
        pltpu.VMEM(ring, BF16),
        pltpu.VMEM(ring, BF16),
        pltpu.VMEM(msg, BF16),
        pltpu.VMEM(msg, BF16),
        dma((3,)),
        dma((4,)),
        dma((2,)),
        dma((2,)),
        dma((2,)),
        dma((2,)),
        dma((2,)),
        dma((ny // NX,)),
        dma((ny // NX,)),
        dma((6,)),
        dma((2,)),
        dma((2, 2, 2)),
        dma((2, parts)),
        dma((2, 4)),
        dma((2, 5, NCH)),
        dma((2, 4)),
        dma((2, 4, NCH)),
        dma((2, parts)),
        dma((NSMALL,)),
    ]
    return pl.pallas_call(
        functools.partial(body, nsp, ntp),
        out_shape=jax.ShapeDtypeStruct(resid.shape, BF16),
        in_specs=[hbm] * (NSMALL + 4),
        out_specs=pl.BlockSpec(memory_space=pltpu.VMEM),
        scratch_shapes=scratch,
        compiler_params=pltpu.CompilerParams(
            collective_id=0, has_side_effects=True, vmem_limit_bytes=56 * 1024 * 1024
        ),
        name="layer",
    )(*small, wout, wg[0], wu[0], wd[0])


def solution(mesh):
    both = ("sp", "tp")
    return jax.shard_map(
        functools.partial(layer, mesh.shape["sp"], mesh.shape["tp"]),
        mesh=mesh,
        in_specs=(
            P(both, None),
            P("sp", "tp"),
            P("sp", "tp"),
            P("sp", "tp"),
            P("sp", "tp"),
            P(None, "sp", "tp"),
            P(None, "tp"),
            P("sp", "tp"),
            P(None, "tp"),
            P(None, "tp"),
            P(None, "tp"),
            P("tp"),
            P(None, "tp"),
            P(),
            P("sp", None),
            P(both, None),
            P("sp", None, "tp"),
            P("sp", None, "tp"),
            P("sp", "tp", None),
        ),
        out_specs=P(both, None),
        check_vma=False,
    )
```

```python
import functools

import jax
import jax.numpy as jnp
from jax import lax
from jax.experimental import pallas as pl
from jax.experimental.pallas import tpu as pltpu
from jax.sharding import PartitionSpec as P

MESH = pl.DeviceIdType.MESH
HIGH = lax.Precision.HIGHEST
F32 = jnp.float32
BF16 = jnp.bfloat16
EPS = 1e-06
BLOCK = 128
NCH = 4
NX = 4
WIDE = 512
NSMALL = 15


def dot(a, b, contract=((1,), (0,)), precision=None):
    return lax.dot_general(
        a, b, (contract, ((), ())), preferred_element_type=F32, precision=precision
    )


def silu(v):
    return v / (1.0 + jnp.exp(-v))


def rcopy(src, dst, send, recv, dev):
    return pltpu.make_async_remote_copy(
        src_ref=src, dst_ref=dst, send_sem=send, recv_sem=recv, device_id=dev, device_id_type=MESH
    )


def wait_bytes(ref, sem):
    pltpu.make_async_copy(ref, ref, sem).wait()


def peer(i, me, n):
    step = n - 2 - i
    return (me + jnp.where(step % 2 == 0, step // 2 + 1, n - 1 - step // 2)) % n


def iota(shape, dim):
    return lax.broadcasted_iota(jnp.int32, shape, dim)


def body(
    nsp,
    ntp,
    *refs,
):
    small_hbm, (wout, wg, wu, wd), out = refs[:NSMALL], refs[NSMALL : NSMALL + 4], refs[NSMALL + 4]
    small = refs[NSMALL + 5 : 2 * NSMALL + 5]
    resid, v_in, k_in, q_in, og_in, raw_in, hdl_in, extra_in = small[:8]
    vf_in, kf_in, qf_in, gain_in, ngain_in, routes_in, cw_in = small[8:]
    (
    raw8,
    hl,
    hr,
    pad,
    tot_s,
    tot_r,
    decay,
    st_s,
    st_r,
    sc_f,
    sc_s,
    sc_r,
    heads,
    wc,
    po,
    mo,
    near,
    through,
    dm,
    dr,
    rowsf,
    xs,
    wgu,
    wdn,
    acc,
    hidden,
    zs,
    sp_b,
    sn_b,
    rp_b,
    rn_b,
    bm,
    br,
    lsem,
    hsem,
    tsem,
    ssem,
    osem,
    hdsem,
    wsem,
    wnear,
    wfar,
    swsem,
    psem,
    nsem,
    dsem,
    ag_send,
    ag_recv,
    rs_send,
    rs_recv,
    bsem,
    isem,
    ) = refs[2 * NSMALL + 5 :]
    me = lax.axis_index("sp")
    tp = lax.axis_index("tp")
    ny = ntp // 2
    y = tp // 2
    c = tp % 2
    partner = y * 2 + (1 - c)
    right_y = ((y + 1) % ny) * 2 + c
    left_y = ((y + ny - 1) % ny) * 2 + c
    others = nsp - 1
    inputs = [
        pltpu.make_async_copy(src, dst, isem.at[n]) for n, (src, dst) in enumerate(zip(small_hbm, small))
    ]
    for n in (5, 6, 7, 1, 2, 3, 8, 9, 10, 4, 13, 14, 0, 11, 12):
        inputs[n].start()

    bar = pltpu.get_barrier_semaphore()

    @pl.loop(1, nsp)
    def _(i):
        pl.semaphore_signal(bar, inc=1, device_id={"sp": (me + i) % nsp}, device_id_type=MESH)

    @pl.loop(1, ntp)
    def _(i):
        pl.semaphore_signal(bar, inc=1, device_id={"tp": (tp + i) % ntp}, device_id_type=MESH)

    ff = wg.shape[1]
    chan = wout.shape[0] // ny
    nx = NX
    x = me % nx

    def w_rows(of):
        return wout.at[pl.ds(pl.multiple_of(of * chan, chan), chan)]

    def w_block(of):
        return wc.at[:, pl.ds(pl.multiple_of(of * 128, 128), 128)]

    loads = [
        pltpu.make_async_copy(w_rows(y), w_block(y), lsem.at[3]),
        pltpu.make_async_copy(wg, wgu.at[:, pl.ds(0, ff)], lsem.at[0]),
        pltpu.make_async_copy(wu, wgu.at[:, pl.ds(2 * ff, ff)], lsem.at[1]),
        pltpu.make_async_copy(wd, wdn.at[pl.ds(0, ff)], lsem.at[2]),
    ]
    for load in loads:
        load.start()

    tokens = v_in.shape[0]
    for n in (1, 2, 3):
        inputs[n].wait()

    pl.semaphore_wait(bar, nsp - 1 + ntp - 1)

    right = {"sp": (me + 1) % nsp}
    left = {"sp": (me + nsp - 1) % nsp}
    for ref, lo, width in ((v_in, 0, 256), (k_in, 256, 128), (q_in, 384, 128)):
        cols = pl.ds(lo, width)
        rcopy(ref.at[pl.ds(tokens - 16, 16)], hl.at[:, cols], hsem.at[0], hsem.at[1], right).start()
        rcopy(ref.at[pl.ds(0, 16)], hr.at[:, cols], hsem.at[2], hsem.at[3], left).start()

    far = 2 + x

    def w_send(distance, send, recv):
        dst = (y + ny - distance) % ny
        return rcopy(w_rows(dst), w_block(y), send, recv, {"tp": dst * 2 + c})

    @pl.when(x > 0)
    def _():
        w_send(far, wfar.at[0], wfar.at[1]).start()

    for distance in (1, -1, 2, -2):
        w_send(distance, wnear.at[0], wnear.at[1]).start()

    def w_relay():
        block = w_block((y + far) % ny)
        wait_bytes(block, wfar.at[1])
        for i in range(1, nx):
            to = me - x + (x + i) % nx
            rcopy(block, block, wsem.at[0], wsem.at[1], {"sp": to}).start()

    for n in (5, 6, 7):
        inputs[n].wait()
    raw8[0, 0:4] = raw_in[0].astype(F32)
    raw8[0, 4:8] = raw_in[1].astype(F32)
    raw8[1, 0:4] = extra_in[...]
    raw8[1, 4:8] = extra_in[...]
    sub = iota((8, 1), 0)
    rates = jnp.where(
        sub < 4, jnp.broadcast_to(hdl_in[0:1], (8, 4)), jnp.broadcast_to(hdl_in[1:2], (8, 4))
    )
    rates = jnp.sum(jnp.where(iota((8, 4), 0) % 4 == iota((8, 4), 1), rates, 0.0), axis=1, keepdims=True)
    step8 = raw8[0]
    step8 = jnp.maximum(step8, 0.0) + jnp.log1p(jnp.exp(-jnp.abs(step8)))
    log8 = raw8[1] - jnp.exp(rates) * step8
    lane = iota((1, 128), 1)
    row = iota((BLOCK, BLOCK), 0)
    col = iota((BLOCK, BLOCK), 1)
    upper = (row <= col).astype(F32)
    spread = ((iota((8, 512), 1) // 64) == iota((8, 512), 0)).astype(F32)
    cum, cum_t, tot_c, sw8, rd8 = [], [], [], [], []
    for b in range(2):
        logs = log8[:, b * BLOCK : (b + 1) * BLOCK]
        run = dot(logs, upper, precision=HIGH)
        total = run[:, BLOCK - 1 : BLOCK]
        both = jnp.where(sub < 4, run, run - logs)
        cum_t.append(both)
        cum.append(jnp.concatenate([both, jnp.zeros((120, BLOCK), F32)], axis=0).T)
        tot_c.append(jnp.broadcast_to(total, (8, 128)))
        sw8.append(jnp.exp(jnp.where(sub < 4, total - both, both)))
        rd8.append(jnp.exp(jnp.where(sub < 4, both, total - both)))
    tot_dev = jnp.exp(tot_c[0] + tot_c[1])
    tot_row = jnp.sum(jnp.where(sub == lane, tot_dev, 0.0), axis=0, keepdims=True)
    tot_s[...] = tot_row
    tot_r[me] = tot_row
    first = ((0,), (0,))
    step_x = dot(step8, spread, first, HIGH)
    sw_x = [dot(sw8[b], spread, first, HIGH) for b in range(2)]
    rd_x = [dot(rd8[b], spread, first, HIGH) for b in range(2)]

    def head_rows(b, first):
        e = jnp.exp(tot_c[b][first : first + 4])
        return jnp.concatenate([jnp.broadcast_to(e[h : h + 1], (64, 128)) for h in range(4)], axis=0)

    @pl.loop(0, nsp - 1)
    def _(i):
        rcopy(tot_s, tot_r.at[me], tsem.at[0], tsem.at[1], {"sp": peer(i, me, nsp)}).start()

    pad[16 : 16 + tokens, 0:256] = v_in[...].astype(F32)
    pad[16 : 16 + tokens, 256:384] = k_in[...].astype(F32)
    pad[16 : 16 + tokens, 384:512] = q_in[...].astype(F32)
    for n in (0, 4, *range(8, NSMALL)):
        inputs[n].wait()
    wait_bytes(hl, hsem.at[1])
    wait_bytes(hr, hsem.at[3])
    pad[0:16] = jnp.where(me > 0, hl[...].astype(F32), 0.0)
    pad[16 + tokens : 32 + tokens] = jnp.where(me < nsp - 1, hr[...].astype(F32), 0.0)
    filt = jnp.concatenate([vf_in[...], kf_in[...], qf_in[...]], axis=1).astype(F32)
    conv = filt[0:1] * pad[14 : 14 + tokens]
    for o in range(1, 5):
        conv = conv + filt[o : o + 1] * pad[14 + o : 14 + o + tokens]
    values = conv[:, 0:256].astype(BF16).astype(F32)
    keys = silu(conv[:, 256:384]).astype(BF16)
    queries = silu(conv[:, 384:512]).astype(BF16)
    scaled = (jnp.concatenate([values, values], axis=1) * step_x).astype(BF16)

    part = []
    for b in range(2):
        rows = slice(b * BLOCK, (b + 1) * BLOCK)
        weighted = (scaled[rows].astype(F32) * sw_x[b]).astype(BF16)
        part.append(dot(weighted, keys[rows], ((0,), (0,))))
    final_f = head_rows(1, 0) * part[0][0:256] + part[1][0:256]
    final_b = head_rows(0, 4) * part[1][256:512] + part[0][256:512]
    piece = 256 // nsp
    mine = jnp.concatenate(
        [final_f.reshape(nsp, piece, 128), final_b.reshape(nsp, piece, 128)], axis=1
    ).astype(BF16)
    st_s[...] = mine

    @pl.loop(0, nsp - 1)
    def _(i):
        dst = peer(i, me, nsp)
        rcopy(st_s.at[dst], st_r.at[me], ssem.at[0], ssem.at[1], {"sp": dst}).start()

    st_r[me] = st_s[me]

    inner = []
    lo_half = lane < 64
    for b in range(2):
        rows = slice(b * BLOCK, (b + 1) * BLOCK)
        score = dot(queries[rows], keys[rows], ((1,), (1,)))
        pairs = []
        for pair in range(2):
            halves = []
            for h in (2 * pair, 2 * pair + 1):
                f_gap = cum[b][:, h : h + 1] - cum_t[b][h : h + 1, :]
                b_gap = cum_t[b][4 + h : 5 + h, :] - cum[b][:, 4 + h : 5 + h]
                w = score * jnp.exp(jnp.where(col <= row, f_gap, b_gap))
                w_f = jnp.where(col <= row, w, 0.0)
                w_b = jnp.where(col >= row, w, 0.0)
                both = jnp.concatenate([w_f, w_b], axis=1).astype(BF16)
                lanes = slice(128 * pair, 128 * pair + 128)
                rhs = jnp.concatenate(
                    [scaled[rows, lanes], scaled[rows, 256 + 128 * pair : 384 + 128 * pair]], axis=0
                )
                halves.append(dot(both, rhs))
            pairs.append(jnp.where(lo_half, halves[0], halves[1]))
        inner.append(jnp.concatenate(pairs, axis=1))
    gate_act = silu(og_in[...].astype(F32))

    own = tokens // ntp
    mine_lane = iota((own, tokens), 1) == iota((own, tokens), 0) + tp * own
    e_lane = iota((own, 128), 1).astype(F32)
    hots = []
    for n in range(2):
        ids = jnp.where(mine_lane, routes_in[n : n + 1].astype(F32), 0.0)
        hots.append((jnp.sum(ids, axis=1, keepdims=True) == e_lane).astype(F32))
    strict = (iota((own, own), 1) < iota((own, own), 0)).astype(F32)
    ids = e_lane * 2.0 + dot(strict, hots[0] + hots[1], precision=HIGH)
    tiles = WIDE // 128
    r_id = iota((tiles * own, nsp * 2 * tiles), 1)
    t_id = iota((tiles * own, nsp * 2 * tiles), 0)
    r_slot = ((r_id // (2 * tiles)) * 2 + r_id % 2).astype(F32)
    same = ((r_id // 2) % tiles) == (t_id // own)
    w_lane = iota((tiles * own, own), 0) % own == iota((tiles * own, own), 1)
    mixing = jnp.zeros(r_id.shape, F32)
    place = jnp.zeros(r_id.shape, F32)
    for n in range(2):
        slot = jnp.sum(hots[n] * ids, axis=1, keepdims=True)
        hit = same & (r_slot == jnp.concatenate([slot] * tiles, axis=0))
        weight = jnp.sum(jnp.where(w_lane, cw_in[n : n + 1], 0.0), axis=1, keepdims=True)
        place = jnp.where(hit, 1.0, place)
        mixing = jnp.where(hit, weight, mixing)
    place = place.astype(BF16)
    mix_hi = mixing.astype(BF16)
    mix_lo = (mixing - mix_hi.astype(F32)).astype(BF16)

    @pl.when(x > 0)
    def _():
        w_relay()

    wait_bytes(tot_r.at[pl.ds(0, others)], tsem.at[1])
    head = me // (64 // piece)
    totals = jnp.concatenate([tot_r[d] for d in range(nsp)], axis=0)
    for n in range(2):
        of_head = jnp.sum(jnp.where(lane == head + 4 * n, totals, 0.0), axis=1, keepdims=True)
        decay[n] = jnp.broadcast_to(of_head, (nsp, 128))

    def scan(i, carry):
        d = nsp - 1 - i
        sc_f[i, 0:piece] = carry[0]
        sc_f[d, piece : 2 * piece] = carry[1]
        return (
            decay[0, pl.ds(i, 1), :] * carry[0] + st_r[i].astype(F32)[0:piece],
            decay[1, pl.ds(d, 1), :] * carry[1] + st_r[d].astype(F32)[piece : 2 * piece],
        )

    wait_bytes(st_r.at[pl.ds(0, others)], ssem.at[1])
    zero = jnp.zeros((piece, 128), F32)
    lax.fori_loop(0, nsp, scan, (zero, zero), unroll=8)
    sc_s[...] = sc_f[...].astype(BF16)

    @pl.loop(0, nsp - 1)
    def _(i):
        dst = peer(i, me, nsp)
        rcopy(sc_s.at[dst], sc_r.at[me], osem.at[0], osem.at[1], {"sp": dst}).start()

    sc_r[me] = sc_s[me]
    wait_bytes(sc_r.at[pl.ds(0, others)], osem.at[1])

    around = sc_r[...].astype(F32)
    enter = around[:, 0:piece].reshape(256, 128)
    leave = around[:, piece : 2 * piece].reshape(256, 128)
    enters = [enter, head_rows(0, 0) * enter + part[0][0:256]]
    leaves = [head_rows(1, 4) * leave + part[1][256:512], leave]
    group = jnp.where(iota((256, 256), 0) // 64 == iota((256, 256), 1) // 64, 1.0 / 64.0, 0.0).astype(BF16)
    swap_h = []
    for b in range(2):
        rows = slice(b * BLOCK, (b + 1) * BLOCK)
        state = jnp.concatenate([enters[b], leaves[b]], axis=0).astype(BF16)
        read = dot(queries[rows], state, ((1,), (1,))) * rd_x[b]
        gated = (inner[b] + read[:, 0:256] + read[:, 256:512]) * gate_act[rows]
        square = gated * gated
        square_hi = square.astype(BF16)
        mean = dot(square_hi, group) + dot((square - square_hi.astype(F32)).astype(BF16), group)
        normed = gated * lax.rsqrt(mean + EPS) * gain_in[...]
        heads[c, rows, :] = normed.astype(BF16)
        half = heads.at[c, pl.ds(b * BLOCK, BLOCK)]
        copy = rcopy(half, half, hdsem.at[0, b], hdsem.at[1, b], {"tp": partner})
        copy.start()
        swap_h.append(copy)

    def blocks(n):
        return wc.at[:, pl.ds(0, 128 * n)]

    loads[0].wait()
    wait_bytes(blocks(4), wnear.at[1])

    @pl.when(x == 0)
    def _():
        wait_bytes(blocks(nx - 1), wsem.at[1])

    @pl.when(x > 0)
    def _():
        wait_bytes(blocks(nx - 2), wsem.at[1])

    inner_c = chan // 2
    own_part = dot(heads[c], wc[pl.ds(pl.multiple_of(c * inner_c, inner_c), inner_c), :])
    for copy in swap_h:
        copy.wait()
    o_c = 1 - c
    full = own_part + dot(heads[o_c], wc[pl.ds(pl.multiple_of(o_c * inner_c, inner_c), inner_c), :])
    po[...] = full.reshape(ntp, own, full.shape[1]).astype(BF16)

    def chip(distance, core):
        return ((y + ny + distance) % ny) * 2 + core

    relays = []
    for way in range(2):
        sign = 1 - 2 * way
        for core in range(2):
            copy = rcopy(
                po.at[chip(3 * sign, core)],
                near.at[way, core],
                nsem.at[0, way, core],
                nsem.at[1, way, core],
                {"tp": chip(sign, c)},
            )
            copy.start()
            relays.append(copy)
    for distance in (4, 1, -1):
        for core in range(2):
            dst = chip(distance, core)
            rcopy(po.at[dst], mo.at[tp], psem.at[0], psem.at[1], {"tp": dst}).start()
    rcopy(po.at[partner], mo.at[tp], psem.at[0], psem.at[1], {"tp": partner}).start()
    mo[tp] = po[tp]
    for way in range(2):
        for core in range(2):
            dst = chip(2 - 4 * way, core)
            relays[2 * way + core].wait_recv()
            through[way, core] = (po[dst].astype(F32) + near[way, core].astype(F32)).astype(BF16)
            rcopy(through.at[way, core], mo.at[tp], psem.at[0], psem.at[1], {"tp": dst}).start()

    swaps = [
        rcopy(wg, wgu.at[:, pl.ds(ff, ff)], swsem.at[0], swsem.at[1], {"tp": partner}),
        rcopy(wu, wgu.at[:, pl.ds(3 * ff, ff)], swsem.at[2], swsem.at[3], {"tp": partner}),
        rcopy(wd, wdn.at[pl.ds(ff, ff)], swsem.at[4], swsem.at[5], {"tp": partner}),
    ]
    for swap in swaps:
        swap.start()

    wait_bytes(mo.at[pl.ds(0, ntp - 5)], psem.at[1])
    halves = []
    for core in range(2):
        total = mo[chip(0, core)].astype(F32)
        for distance in (1, -1, 2, -2, 4):
            total = total + mo[chip(distance, core)].astype(F32)
        halves.append(total)
    pieces = []
    for j in range(ny):
        pieces += [halves[0][:, 128 * j : 128 * j + 128], halves[1][:, 128 * j : 128 * j + 128]]
    mixer_out = jnp.concatenate(pieces, axis=1).astype(BF16).astype(F32)
    middle = (resid[...].astype(F32) + mixer_out).astype(BF16).astype(F32)
    square = jnp.mean(middle * middle, axis=-1, keepdims=True)
    normed = (middle * lax.rsqrt(square + EPS) * ngain_in[...]).astype(BF16)
    parts = normed.shape[1] // WIDE
    width = normed.shape[1] // NCH
    per = NCH // parts
    stacked = jnp.concatenate(
        [
            jnp.concatenate(
                [normed[:, p * WIDE + n * 128 : p * WIDE + (n + 1) * 128] for n in range(tiles)], axis=0
            )
            for p in range(parts)
        ],
        axis=1,
    )
    sent = dot(place, stacked, first)
    for p in range(parts):
        dm[p] = sent[:, p * 128 : (p + 1) * 128].reshape(nsp, 2 * tiles, 128).astype(BF16)

        @pl.loop(0, nsp - 1)
        def _(i):
            dst = peer(i, me, nsp)
            rcopy(dm.at[p, dst], dr.at[p, me], dsem.at[0, p], dsem.at[1, p], {"sp": dst}).start()

        dr[p, me] = dm[p, me]

    r_dev = {"tp": right_y}
    l_dev = {"tp": left_y}
    for p in range(parts):
        wait_bytes(dr.at[p, pl.ds(0, others)], dsem.at[1, p])
        rowsf[...] = dr[p].astype(F32).reshape(nsp * 2 * tiles, 128)
        for q in range(per):
            j = p * per + q
            for n in range(width // 128):
                for s in range(2):
                    tile = q * (width // 128) + n
                    picked = rowsf[pl.ds(2 * tile + s, nsp, stride=2 * tiles), :]
                    xs[0, j, s * nsp : (s + 1) * nsp, n * 128 : (n + 1) * 128] = picked.astype(BF16)
            rcopy(xs.at[0, j], xs.at[1, j], ag_send.at[0, 0], ag_recv.at[0, 1, j], r_dev).start()
            rcopy(xs.at[0, j], xs.at[5, j], ag_send.at[1, 0], ag_recv.at[1, 1, j], l_dev).start()

    for load in loads[1:]:
        load.wait()
    for swap in swaps:
        swap.wait()

    rows1 = 2 * nsp
    top = pl.ds(0, nsp)
    low = pl.ds(nsp, nsp)

    def add_chunk(rows, j):
        n = rows.shape[0]
        w = wgu[pl.ds(pl.multiple_of(j * width, width), width), :]
        acc[0:n] = jnp.where(j == 0, 0.0, acc[0:n]) + dot(rows, w)

    def activate(n):
        hidden[0:n] = (silu(acc[0:n, 0 : 2 * ff]) * acc[0:n, 2 * ff : 4 * ff]).astype(BF16)

    def down(n, j):
        return dot(hidden[0:n], wdn[:, pl.ds(pl.multiple_of(j * width, width), width)])

    def down_pair(k, j):
        z = down(2 * rows1, j)
        zs[k, j] = z[0:rows1]
        zs[4 + k, j] = z[rows1 : 2 * rows1]

    @pl.loop(0, NCH)
    def _(j):
        add_chunk(xs[0, j], j)

    activate(rows1)

    @pl.loop(0, NCH)
    def _(j):
        zs[0, j] = down(rows1, j)

    @pl.loop(0, 3 * NCH)
    def _(t):
        k = 1 + t // NCH
        j = t % NCH
        wait_bytes(xs.at[k, j], ag_recv.at[0, k, j])
        wait_bytes(xs.at[4 + k, j], ag_recv.at[1, k, j])

        @pl.when(k < 3)
        def _():
            rcopy(xs.at[k, j], xs.at[k + 1, j], ag_send.at[0, k], ag_recv.at[0, k + 1, j], r_dev).start()
            rcopy(xs.at[4 + k, j], xs.at[5 + k, j], ag_send.at[1, k], ag_recv.at[1, k + 1, j], l_dev).start()

        @pl.when(k == 3)
        def _():
            rcopy(
                xs.at[3, j, top], xs.at[4, j, top], ag_send.at[0, 3], ag_recv.at[0, 4, j], r_dev
            ).start()
            rcopy(
                xs.at[7, j, low], xs.at[4, j, low], ag_send.at[1, 3], ag_recv.at[1, 4, j], l_dev
            ).start()

        add_chunk(jnp.concatenate([xs[k, j], xs[4 + k, j]], axis=0), j)

        @pl.when(k > 1)
        def _():
            down_pair(k - 1, j)

        @pl.when(j == NCH - 1)
        def _():
            activate(2 * rows1)

    @pl.loop(0, NCH)
    def _(j):
        down_pair(3, j)
        sp_b[2, j, nsp:rows1] = zs[7, j, nsp:rows1].astype(BF16)
        sn_b[2, j, 0:nsp] = zs[3, j, 0:nsp].astype(BF16)
        rcopy(
            sp_b.at[2, j, low], rp_b.at[2, j, low], rs_send.at[0, 2], rs_recv.at[0, 2, j], r_dev
        ).start()
        rcopy(
            sn_b.at[2, j, top], rn_b.at[2, j, top], rs_send.at[1, 2], rs_recv.at[1, 2, j], l_dev
        ).start()
        wait_bytes(xs.at[4, j, top], ag_recv.at[0, 4, j])
        wait_bytes(xs.at[4, j, low], ag_recv.at[1, 4, j])
        add_chunk(xs[4, j], j)

    activate(rows1)

    @pl.loop(0, NCH)
    def _(j):
        z = down(rows1, j)
        sp_b[3, j, 0:nsp] = z[0:nsp].astype(BF16)
        sn_b[3, j, nsp:rows1] = z[nsp:rows1].astype(BF16)
        rcopy(
            sp_b.at[3, j, top], rp_b.at[3, j, top], rs_send.at[0, 3], rs_recv.at[0, 3, j], r_dev
        ).start()
        rcopy(
            sn_b.at[3, j, low], rn_b.at[3, j, low], rs_send.at[1, 3], rs_recv.at[1, 3, j], l_dev
        ).start()

    @pl.loop(0, NCH)
    def _(j):
        wait_bytes(rp_b.at[3, j, top], rs_recv.at[0, 3, j])
        wait_bytes(rn_b.at[3, j, low], rs_recv.at[1, 3, j])
        sp_b[2, j, 0:nsp] = (zs[7, j, 0:nsp] + rp_b[3, j, 0:nsp].astype(F32)).astype(BF16)
        sn_b[2, j, nsp:rows1] = (zs[3, j, nsp:rows1] + rn_b[3, j, nsp:rows1].astype(F32)).astype(BF16)
        rcopy(
            sp_b.at[2, j, top], rp_b.at[2, j, top], rs_send.at[0, 2], rs_recv.at[0, 2, j], r_dev
        ).start()
        rcopy(
            sn_b.at[2, j, low], rn_b.at[2, j, low], rs_send.at[1, 2], rs_recv.at[1, 2, j], l_dev
        ).start()

    @pl.loop(0, 2 * NCH)
    def _(t):
        k = 2 - t // NCH
        j = t % NCH
        wait_bytes(rp_b.at[k, j], rs_recv.at[0, k, j])
        wait_bytes(rn_b.at[k, j], rs_recv.at[1, k, j])
        sp_b[k - 1, j] = (zs[4 + k, j] + rp_b[k, j].astype(F32)).astype(BF16)
        sn_b[k - 1, j] = (zs[k, j] + rn_b[k, j].astype(F32)).astype(BF16)
        rcopy(
            sp_b.at[k - 1, j], rp_b.at[k - 1, j], rs_send.at[0, k - 1], rs_recv.at[0, k - 1, j], r_dev
        ).start()
        rcopy(
            sn_b.at[k - 1, j], rn_b.at[k - 1, j], rs_send.at[1, k - 1], rs_recv.at[1, k - 1, j], l_dev
        ).start()

    for p in range(parts):
        for q in range(per):
            j = p * per + q
            wait_bytes(rp_b.at[0, j], rs_recv.at[0, 0, j])
            wait_bytes(rn_b.at[0, j], rs_recv.at[1, 0, j])
            total = zs[0, j] + rp_b[0, j].astype(F32) + rn_b[0, j].astype(F32)
            for n in range(width // 128):
                for s in range(2):
                    tile = q * (width // 128) + n
                    rowsf[pl.ds(2 * tile + s, nsp, stride=2 * tiles), :] = total[
                        s * nsp : (s + 1) * nsp, n * 128 : (n + 1) * 128
                    ]
        bm[p] = rowsf[...].reshape(nsp, 2 * tiles, 128).astype(BF16)

        @pl.loop(0, nsp - 1)
        def _(i):
            dst = peer(i, me, nsp)
            rcopy(bm.at[p, dst], br.at[p, me], bsem.at[0, p], bsem.at[1, p], {"sp": dst}).start()

        br[p, me] = bm[p, me]

    for p in range(parts):
        wait_bytes(br.at[p, pl.ds(0, others)], bsem.at[1, p])
        back = br[p].astype(F32).reshape(nsp * 2 * tiles, 128).astype(BF16)
        mixed = dot(mix_hi, back) + dot(mix_lo, back)
        for n in range(tiles):
            cols = slice(p * WIDE + n * 128, p * WIDE + (n + 1) * 128)
            out[:, cols] = (middle[:, cols] + mixed[n * own : (n + 1) * own]).astype(BF16)

    wait_bytes(hl, hsem.at[0])
    wait_bytes(hr, hsem.at[2])
    wait_bytes(tot_r.at[pl.ds(0, others)], tsem.at[0])
    wait_bytes(st_r.at[pl.ds(0, others)], ssem.at[0])
    wait_bytes(sc_r.at[pl.ds(0, others)], osem.at[0])
    wait_bytes(blocks(4), wnear.at[0])

    @pl.when(x > 0)
    def _():
        wait_bytes(blocks(1), wfar.at[0])
        wait_bytes(blocks(nx - 1), wsem.at[0])

    wait_bytes(mo.at[pl.ds(0, ntp - 5)], psem.at[0])
    for copy in relays:
        copy.wait_send()
    for p in range(parts):
        wait_bytes(dr.at[p, pl.ds(0, others)], dsem.at[0, p])
        wait_bytes(br.at[p, pl.ds(0, others)], bsem.at[0, p])
    for way in range(2):
        for k in range(3):
            wait_bytes(xs.at[0], ag_send.at[way, k])
            wait_bytes(xs.at[0], rs_send.at[way, k])
        wait_bytes(xs.at[0, pl.ds(0, 2)], ag_send.at[way, 3])
        wait_bytes(xs.at[0, pl.ds(0, 2)], rs_send.at[way, 3])


def layer(nsp, ntp, resid, v, k, q, og, raw, hdl, extra, vf, kf, qf, gain, wout, ngain, routes, cw, wg, wu, wd):
    ny = ntp // 2
    tokens = v.shape[0]
    own = tokens // ntp
    width = resid.shape[1] // NCH
    ff = wg.shape[2]
    chan = wout.shape[0] // ny
    rows1 = 2 * nsp

    small = [
        resid,
        v,
        k,
        q,
        og,
        raw.transpose(0, 2, 1),
        hdl,
        extra.T,
        vf,
        kf,
        qf,
        gain.reshape(1, -1),
        ngain.reshape(1, -1),
        routes.T,
        cw.T,
    ]
    dma = pltpu.SemaphoreType.DMA
    hbm = pl.BlockSpec(memory_space=pl.ANY)
    pair = (nsp, 16, 128)
    parts = resid.shape[1] // WIDE
    msg = (parts, nsp, WIDE // 64, 128)
    ring = (4, NCH, rows1, width)
    scratch = [pltpu.VMEM(x.shape, x.dtype) for x in small] + [
        pltpu.VMEM((2, 8, tokens), F32),
        pltpu.VMEM((16, 512), BF16),
        pltpu.VMEM((16, 512), BF16),
        pltpu.VMEM((tokens + 32, 512), F32),
        pltpu.VMEM((1, 128), F32),
        pltpu.VMEM((nsp, 1, 128), F32),
        pltpu.VMEM((2, nsp, 128), F32),
        pltpu.VMEM(pair, BF16),
        pltpu.VMEM(pair, BF16),
        pltpu.VMEM(pair, F32),
        pltpu.VMEM(pair, BF16),
        pltpu.VMEM(pair, BF16),
        pltpu.VMEM((2, tokens, 256), BF16),
        pltpu.VMEM((chan, 128 * ny), BF16),
        pltpu.VMEM((ntp, own, 128 * ny), BF16),
        pltpu.VMEM((ntp, own, 128 * ny), BF16),
        pltpu.VMEM((2, 2, own, 128 * ny), BF16),
        pltpu.VMEM((2, 2, own, 128 * ny), BF16),
        pltpu.VMEM(msg, BF16),
        pltpu.VMEM(msg, BF16),
        pltpu.VMEM((nsp * WIDE // 64, 128), F32),
        pltpu.VMEM((8, NCH, rows1, width), BF16),
        pltpu.VMEM((wg.shape[1], 4 * ff), BF16),
        pltpu.VMEM((2 * ff, wd.shape[2]), BF16),
        pltpu.VMEM((2 * rows1, 4 * ff), F32),
        pltpu.VMEM((2 * rows1, 2 * ff), BF16),
        pltpu.VMEM((8, NCH, rows1, width), F32),
        pltpu.VMEM(ring, BF16),
        pltpu.VMEM(ring, BF16),
        pltpu.VMEM(ring, BF16),
        pltpu.VMEM(ring, BF16),
        pltpu.VMEM(msg, BF16),
        pltpu.VMEM(msg, BF16),
        dma((4,)),
        dma((4,)),
        dma((2,)),
        dma((2,)),
        dma((2,)),
        dma((2, 2)),
        dma((2,)),
        dma((2,)),
        dma((2,)),
        dma((6,)),
        dma((2,)),
        dma((2, 2, 2)),
        dma((2, parts)),
        dma((2, 4)),
        dma((2, 5, NCH)),
        dma((2, 4)),
        dma((2, 4, NCH)),
        dma((2, parts)),
        dma((NSMALL,)),
    ]
    return pl.pallas_call(
        functools.partial(body, nsp, ntp),
        out_shape=jax.ShapeDtypeStruct(resid.shape, BF16),
        in_specs=[hbm] * (NSMALL + 4),
        out_specs=pl.BlockSpec(memory_space=pltpu.VMEM),
        scratch_shapes=scratch,
        compiler_params=pltpu.CompilerParams(
            collective_id=0, has_side_effects=True, vmem_limit_bytes=56 * 1024 * 1024
        ),
        name="layer",
    )(*small, wout, wg[0], wu[0], wd[0])


def solution(mesh):
    both = ("sp", "tp")
    return jax.shard_map(
        functools.partial(layer, mesh.shape["sp"], mesh.shape["tp"]),
        mesh=mesh,
        in_specs=(
            P(both, None),
            P("sp", "tp"),
            P("sp", "tp"),
            P("sp", "tp"),
            P("sp", "tp"),
            P(None, "sp", "tp"),
            P(None, "tp"),
            P("sp", "tp"),
            P(None, "tp"),
            P(None, "tp"),
            P(None, "tp"),
            P("tp"),
            P(None, "tp"),
            P(),
            P("sp", None),
            P(both, None),
            P("sp", None, "tp"),
            P("sp", None, "tp"),
            P("sp", "tp", None),
        ),
        out_specs=P(both, None),
        check_vma=False,
    )
```

```python
import functools

import jax
import jax.numpy as jnp
from jax import lax
from jax.experimental import pallas as pl
from jax.experimental.pallas import tpu as pltpu
from jax.sharding import PartitionSpec as P

MESH = pl.DeviceIdType.MESH
HIGH = lax.Precision.HIGHEST
F32 = jnp.float32
BF16 = jnp.bfloat16
EPS = 1e-06
BLOCK = 128
NCH = 4
NX = 4
WIDE = 512
NSMALL = 15


def dot(a, b, contract=((1,), (0,)), precision=None):
    return lax.dot_general(
        a, b, (contract, ((), ())), preferred_element_type=F32, precision=precision
    )


def silu(v):
    return v / (1.0 + jnp.exp(-v))


def rcopy(src, dst, send, recv, dev):
    return pltpu.make_async_remote_copy(
        src_ref=src, dst_ref=dst, send_sem=send, recv_sem=recv, device_id=dev, device_id_type=MESH
    )


def wait_bytes(ref, sem):
    pltpu.make_async_copy(ref, ref, sem).wait()


def peer(i, me, n):
    step = n - 2 - i
    return (me + jnp.where(step % 2 == 0, step // 2 + 1, n - 1 - step // 2)) % n


def iota(shape, dim):
    return lax.broadcasted_iota(jnp.int32, shape, dim)


def body(
    nsp,
    ntp,
    *refs,
):
    small_hbm, (wout, wg, wu, wd), out = refs[:NSMALL], refs[NSMALL : NSMALL + 4], refs[NSMALL + 4]
    small = refs[NSMALL + 5 : 2 * NSMALL + 5]
    resid, v_in, k_in, q_in, og_in, raw_in, hdl_in, extra_in = small[:8]
    vf_in, kf_in, qf_in, gain_in, ngain_in, routes_in, cw_in = small[8:]
    (
    raw8,
    hl,
    hr,
    pad,
    tot_s,
    tot_r,
    decay,
    st_s,
    st_r,
    sc_f,
    sc_s,
    sc_r,
    heads,
    wc,
    po,
    mo,
    near,
    through,
    sm,
    sr,
    xsc,
    acc_own,
    dm,
    dr,
    rowsf,
    xs,
    wgu,
    wdn,
    acc,
    hidden,
    zs,
    sp_b,
    sn_b,
    rp_b,
    rn_b,
    bm,
    br,
    lsem,
    hsem,
    tsem,
    ssem,
    osem,
    hdsem,
    wsem,
    wnear,
    wfar,
    swsem,
    psem,
    nsem,
    csem,
    xsend,
    xrecv,
    dsem,
    ag_send,
    ag_recv,
    rs_send,
    rs_recv,
    bsem,
    isem,
    ) = refs[2 * NSMALL + 5 :]
    me = lax.axis_index("sp")
    tp = lax.axis_index("tp")
    ny = ntp // 2
    y = tp // 2
    c = tp % 2
    partner = y * 2 + (1 - c)
    right_y = ((y + 1) % ny) * 2 + c
    left_y = ((y + ny - 1) % ny) * 2 + c
    others = nsp - 1
    inputs = [
        pltpu.make_async_copy(src, dst, isem.at[n]) for n, (src, dst) in enumerate(zip(small_hbm, small))
    ]
    for n in (5, 6, 7, 1, 2, 3, 8, 9, 10, 4, 13, 14, 0, 11, 12):
        inputs[n].start()

    bar = pltpu.get_barrier_semaphore()

    @pl.loop(1, nsp)
    def _(i):
        pl.semaphore_signal(bar, inc=1, device_id={"sp": (me + i) % nsp}, device_id_type=MESH)

    @pl.loop(1, ntp)
    def _(i):
        pl.semaphore_signal(bar, inc=1, device_id={"tp": (tp + i) % ntp}, device_id_type=MESH)

    ff = wg.shape[1]
    chan = wout.shape[0] // ny
    nx = NX
    x = me % nx

    def w_rows(of):
        return wout.at[pl.ds(pl.multiple_of(of * chan, chan), chan)]

    def w_block(of):
        return wc.at[:, pl.ds(pl.multiple_of(of * 128, 128), 128)]

    loads = [
        pltpu.make_async_copy(w_rows(y), w_block(y), lsem.at[3]),
        pltpu.make_async_copy(wg, wgu.at[:, pl.ds(0, ff)], lsem.at[0]),
        pltpu.make_async_copy(wu, wgu.at[:, pl.ds(2 * ff, ff)], lsem.at[1]),
        pltpu.make_async_copy(wd, wdn.at[pl.ds(0, ff)], lsem.at[2]),
    ]
    for load in loads:
        load.start()

    tokens = v_in.shape[0]
    for n in (1, 2, 3):
        inputs[n].wait()

    pl.semaphore_wait(bar, nsp - 1 + ntp - 1)

    right = {"sp": (me + 1) % nsp}
    left = {"sp": (me + nsp - 1) % nsp}
    for ref, lo, width in ((v_in, 0, 256), (k_in, 256, 128), (q_in, 384, 128)):
        cols = pl.ds(lo, width)
        rcopy(ref.at[pl.ds(tokens - 16, 16)], hl.at[:, cols], hsem.at[0], hsem.at[1], right).start()
        rcopy(ref.at[pl.ds(0, 16)], hr.at[:, cols], hsem.at[2], hsem.at[3], left).start()

    far = 2 + x

    def w_send(distance, send, recv):
        dst = (y + ny - distance) % ny
        return rcopy(w_rows(dst), w_block(y), send, recv, {"tp": dst * 2 + c})

    @pl.when(x > 0)
    def _():
        w_send(far, wfar.at[0], wfar.at[1]).start()

    for distance in (1, -1, 2, -2):
        w_send(distance, wnear.at[0], wnear.at[1]).start()

    def w_relay():
        block = w_block((y + far) % ny)
        wait_bytes(block, wfar.at[1])
        for i in range(1, nx):
            to = me - x + (x + i) % nx
            rcopy(block, block, wsem.at[0], wsem.at[1], {"sp": to}).start()

    for n in (5, 6, 7):
        inputs[n].wait()
    raw8[0, 0:4] = raw_in[0].astype(F32)
    raw8[0, 4:8] = raw_in[1].astype(F32)
    raw8[1, 0:4] = extra_in[...]
    raw8[1, 4:8] = extra_in[...]
    sub = iota((8, 1), 0)
    rates = jnp.where(
        sub < 4, jnp.broadcast_to(hdl_in[0:1], (8, 4)), jnp.broadcast_to(hdl_in[1:2], (8, 4))
    )
    rates = jnp.sum(jnp.where(iota((8, 4), 0) % 4 == iota((8, 4), 1), rates, 0.0), axis=1, keepdims=True)
    step8 = raw8[0]
    step8 = jnp.maximum(step8, 0.0) + jnp.log1p(jnp.exp(-jnp.abs(step8)))
    log8 = raw8[1] - jnp.exp(rates) * step8
    lane = iota((1, 128), 1)
    row = iota((BLOCK, BLOCK), 0)
    col = iota((BLOCK, BLOCK), 1)
    upper = (row <= col).astype(F32)
    spread = ((iota((8, 512), 1) // 64) == iota((8, 512), 0)).astype(F32)
    cum, cum_t, tot_c, sw8, rd8 = [], [], [], [], []
    for b in range(2):
        logs = log8[:, b * BLOCK : (b + 1) * BLOCK]
        run = dot(logs, upper, precision=HIGH)
        total = run[:, BLOCK - 1 : BLOCK]
        both = jnp.where(sub < 4, run, run - logs)
        cum_t.append(both)
        cum.append(jnp.concatenate([both, jnp.zeros((120, BLOCK), F32)], axis=0).T)
        tot_c.append(jnp.broadcast_to(total, (8, 128)))
        sw8.append(jnp.exp(jnp.where(sub < 4, total - both, both)))
        rd8.append(jnp.exp(jnp.where(sub < 4, both, total - both)))
    tot_dev = jnp.exp(tot_c[0] + tot_c[1])
    tot_row = jnp.sum(jnp.where(sub == lane, tot_dev, 0.0), axis=0, keepdims=True)
    tot_s[...] = tot_row
    tot_r[me] = tot_row
    first = ((0,), (0,))
    step_x = dot(step8, spread, first, HIGH)
    sw_x = [dot(sw8[b], spread, first, HIGH) for b in range(2)]
    rd_x = [dot(rd8[b], spread, first, HIGH) for b in range(2)]

    def head_rows(b, first):
        e = jnp.exp(tot_c[b][first : first + 4])
        return jnp.concatenate([jnp.broadcast_to(e[h : h + 1], (64, 128)) for h in range(4)], axis=0)

    @pl.loop(0, nsp - 1)
    def _(i):
        rcopy(tot_s, tot_r.at[me], tsem.at[0], tsem.at[1], {"sp": peer(i, me, nsp)}).start()

    pad[16 : 16 + tokens, 0:256] = v_in[...].astype(F32)
    pad[16 : 16 + tokens, 256:384] = k_in[...].astype(F32)
    pad[16 : 16 + tokens, 384:512] = q_in[...].astype(F32)
    for n in (0, 4, *range(8, NSMALL)):
        inputs[n].wait()
    wait_bytes(hl, hsem.at[1])
    wait_bytes(hr, hsem.at[3])
    pad[0:16] = jnp.where(me > 0, hl[...].astype(F32), 0.0)
    pad[16 + tokens : 32 + tokens] = jnp.where(me < nsp - 1, hr[...].astype(F32), 0.0)
    filt = jnp.concatenate([vf_in[...], kf_in[...], qf_in[...]], axis=1).astype(F32)
    conv = filt[0:1] * pad[14 : 14 + tokens]
    for o in range(1, 5):
        conv = conv + filt[o : o + 1] * pad[14 + o : 14 + o + tokens]
    values = conv[:, 0:256].astype(BF16).astype(F32)
    keys = silu(conv[:, 256:384]).astype(BF16)
    queries = silu(conv[:, 384:512]).astype(BF16)
    scaled = (jnp.concatenate([values, values], axis=1) * step_x).astype(BF16)

    part = []
    for b in range(2):
        rows = slice(b * BLOCK, (b + 1) * BLOCK)
        weighted = (scaled[rows].astype(F32) * sw_x[b]).astype(BF16)
        part.append(dot(weighted, keys[rows], ((0,), (0,))))
    final_f = head_rows(1, 0) * part[0][0:256] + part[1][0:256]
    final_b = head_rows(0, 4) * part[1][256:512] + part[0][256:512]
    piece = 256 // nsp
    mine = jnp.concatenate(
        [final_f.reshape(nsp, piece, 128), final_b.reshape(nsp, piece, 128)], axis=1
    ).astype(BF16)
    st_s[...] = mine

    @pl.loop(0, nsp - 1)
    def _(i):
        dst = peer(i, me, nsp)
        rcopy(st_s.at[dst], st_r.at[me], ssem.at[0], ssem.at[1], {"sp": dst}).start()

    st_r[me] = st_s[me]

    inner = []
    lo_half = lane < 64
    for b in range(2):
        rows = slice(b * BLOCK, (b + 1) * BLOCK)
        score = dot(queries[rows], keys[rows], ((1,), (1,)))
        pairs = []
        for pair in range(2):
            halves = []
            for h in (2 * pair, 2 * pair + 1):
                f_gap = cum[b][:, h : h + 1] - cum_t[b][h : h + 1, :]
                b_gap = cum_t[b][4 + h : 5 + h, :] - cum[b][:, 4 + h : 5 + h]
                w = score * jnp.exp(jnp.where(col <= row, f_gap, b_gap))
                w_f = jnp.where(col <= row, w, 0.0)
                w_b = jnp.where(col >= row, w, 0.0)
                both = jnp.concatenate([w_f, w_b], axis=1).astype(BF16)
                lanes = slice(128 * pair, 128 * pair + 128)
                rhs = jnp.concatenate(
                    [scaled[rows, lanes], scaled[rows, 256 + 128 * pair : 384 + 128 * pair]], axis=0
                )
                halves.append(dot(both, rhs))
            pairs.append(jnp.where(lo_half, halves[0], halves[1]))
        inner.append(jnp.concatenate(pairs, axis=1))
    gate_act = silu(og_in[...].astype(F32))

    own = tokens // ntp
    mine_lane = iota((own, tokens), 1) == iota((own, tokens), 0) + tp * own
    e_lane = iota((own, 128), 1).astype(F32)
    hots = []
    for n in range(2):
        ids = jnp.where(mine_lane, routes_in[n : n + 1].astype(F32), 0.0)
        hots.append((jnp.sum(ids, axis=1, keepdims=True) == e_lane).astype(F32))
    strict = (iota((own, own), 1) < iota((own, own), 0)).astype(F32)
    ids = e_lane * 2.0 + dot(strict, hots[0] + hots[1], precision=HIGH)
    tiles = WIDE // 128
    r_id = iota((tiles * own, nsp * 2 * tiles), 1)
    t_id = iota((tiles * own, nsp * 2 * tiles), 0)
    r_slot = ((r_id // (2 * tiles)) * 2 + r_id % 2).astype(F32)
    same = ((r_id // 2) % tiles) == (t_id // own)
    w_lane = iota((tiles * own, own), 0) % own == iota((tiles * own, own), 1)
    mixing = jnp.zeros(r_id.shape, F32)
    place = jnp.zeros(r_id.shape, F32)
    slots = []
    for n in range(2):
        slot = jnp.sum(hots[n] * ids, axis=1, keepdims=True)
        slots.append(slot)
        hit = same & (r_slot == jnp.concatenate([slot] * tiles, axis=0))
        weight = jnp.sum(jnp.where(w_lane, cw_in[n : n + 1], 0.0), axis=1, keepdims=True)
        place = jnp.where(hit, 1.0, place)
        mixing = jnp.where(hit, weight, mixing)
    place = place.astype(BF16)
    mix_hi = mixing.astype(BF16)
    mix_lo = (mixing - mix_hi.astype(F32)).astype(BF16)

    @pl.when(x > 0)
    def _():
        w_relay()

    wait_bytes(tot_r.at[pl.ds(0, others)], tsem.at[1])
    head = me // (64 // piece)
    totals = jnp.concatenate([tot_r[d] for d in range(nsp)], axis=0)
    for n in range(2):
        of_head = jnp.sum(jnp.where(lane == head + 4 * n, totals, 0.0), axis=1, keepdims=True)
        decay[n] = jnp.broadcast_to(of_head, (nsp, 128))

    def scan(i, carry):
        d = nsp - 1 - i
        sc_f[i, 0:piece] = carry[0]
        sc_f[d, piece : 2 * piece] = carry[1]
        return (
            decay[0, pl.ds(i, 1), :] * carry[0] + st_r[i].astype(F32)[0:piece],
            decay[1, pl.ds(d, 1), :] * carry[1] + st_r[d].astype(F32)[piece : 2 * piece],
        )

    wait_bytes(st_r.at[pl.ds(0, others)], ssem.at[1])
    zero = jnp.zeros((piece, 128), F32)
    lax.fori_loop(0, nsp, scan, (zero, zero), unroll=8)
    sc_s[...] = sc_f[...].astype(BF16)

    @pl.loop(0, nsp - 1)
    def _(i):
        dst = peer(i, me, nsp)
        rcopy(sc_s.at[dst], sc_r.at[me], osem.at[0], osem.at[1], {"sp": dst}).start()

    sc_r[me] = sc_s[me]
    wait_bytes(sc_r.at[pl.ds(0, others)], osem.at[1])

    around = sc_r[...].astype(F32)
    enter = around[:, 0:piece].reshape(256, 128)
    leave = around[:, piece : 2 * piece].reshape(256, 128)
    enters = [enter, head_rows(0, 0) * enter + part[0][0:256]]
    leaves = [head_rows(1, 4) * leave + part[1][256:512], leave]
    group = jnp.where(iota((256, 256), 0) // 64 == iota((256, 256), 1) // 64, 1.0 / 64.0, 0.0).astype(BF16)
    swap_h = []
    for b in range(2):
        rows = slice(b * BLOCK, (b + 1) * BLOCK)
        state = jnp.concatenate([enters[b], leaves[b]], axis=0).astype(BF16)
        read = dot(queries[rows], state, ((1,), (1,))) * rd_x[b]
        gated = (inner[b] + read[:, 0:256] + read[:, 256:512]) * gate_act[rows]
        square = gated * gated
        square_hi = square.astype(BF16)
        mean = dot(square_hi, group) + dot((square - square_hi.astype(F32)).astype(BF16), group)
        normed = gated * lax.rsqrt(mean + EPS) * gain_in[...]
        heads[c, rows, :] = normed.astype(BF16)
        half = heads.at[c, pl.ds(b * BLOCK, BLOCK)]
        copy = rcopy(half, half, hdsem.at[0, b], hdsem.at[1, b], {"tp": partner})
        copy.start()
        swap_h.append(copy)

    def blocks(n):
        return wc.at[:, pl.ds(0, 128 * n)]

    loads[0].wait()
    wait_bytes(blocks(4), wnear.at[1])

    @pl.when(x == 0)
    def _():
        wait_bytes(blocks(nx - 1), wsem.at[1])

    @pl.when(x > 0)
    def _():
        wait_bytes(blocks(nx - 2), wsem.at[1])

    inner_c = chan // 2
    own_part = dot(heads[c], wc[pl.ds(pl.multiple_of(c * inner_c, inner_c), inner_c), :])
    for copy in swap_h:
        copy.wait()
    o_c = 1 - c
    full = own_part + dot(heads[o_c], wc[pl.ds(pl.multiple_of(o_c * inner_c, inner_c), inner_c), :])
    span = full.shape[1] // 2
    for h in range(2):
        po[h] = full[:, h * span : (h + 1) * span].reshape(ntp, own, span).astype(BF16)

    def chip(distance, core):
        return ((y + ny + distance) % ny) * 2 + core

    relays = [[], []]

    def send_far(h):
        for way in range(2):
            sign = 1 - 2 * way
            for core in range(2):
                copy = rcopy(
                    po.at[h, chip(3 * sign, core)],
                    near.at[h, way, core],
                    nsem.at[0, h, way, core],
                    nsem.at[1, h, way, core],
                    {"tp": chip(sign, c)},
                )
                copy.start()
                relays[h].append(copy)

    def send_direct(h):
        for distance in (4, 1, -1):
            for core in range(2):
                dst = chip(distance, core)
                rcopy(po.at[h, dst], mo.at[h, tp], psem.at[0, h], psem.at[1, h], {"tp": dst}).start()
        rcopy(po.at[h, partner], mo.at[h, tp], psem.at[0, h], psem.at[1, h], {"tp": partner}).start()
        mo[h, tp] = po[h, tp]

    def send_through(h):
        for way in range(2):
            for core in range(2):
                dst = chip(2 - 4 * way, core)
                relays[h][2 * way + core].wait_recv()
                through[h, way, core] = (
                    po[h, dst].astype(F32) + near[h, way, core].astype(F32)
                ).astype(BF16)
                rcopy(
                    through.at[h, way, core], mo.at[h, tp], psem.at[0, h], psem.at[1, h], {"tp": dst}
                ).start()

    send_far(0)
    send_direct(0)
    send_far(1)
    send_through(0)
    send_direct(1)
    send_through(1)

    swaps = [
        rcopy(wg, wgu.at[:, pl.ds(ff, ff)], swsem.at[0], swsem.at[1], {"tp": partner}),
        rcopy(wu, wgu.at[:, pl.ds(3 * ff, ff)], swsem.at[2], swsem.at[3], {"tp": partner}),
        rcopy(wd, wdn.at[pl.ds(ff, ff)], swsem.at[4], swsem.at[5], {"tp": partner}),
    ]
    for swap in swaps:
        swap.start()

    parts = resid.shape[1] // WIDE
    width = resid.shape[1] // NCH
    per = NCH // parts
    piled = parts // 2
    middles = []
    squares = jnp.zeros((own, 1), F32)
    for h in range(2):
        wait_bytes(mo.at[h, pl.ds(0, ntp - 5)], psem.at[1, h])
        halves = []
        for core in range(2):
            total = mo[h, chip(0, core)].astype(F32)
            for distance in (1, -1, 2, -2, 4):
                total = total + mo[h, chip(distance, core)].astype(F32)
            halves.append(total)
        pieces = []
        for j in range(span // 128):
            pieces += [halves[0][:, 128 * j : 128 * j + 128], halves[1][:, 128 * j : 128 * j + 128]]
        mixer_out = jnp.concatenate(pieces, axis=1).astype(BF16).astype(F32)
        cols = slice(h * 2 * span, (h + 1) * 2 * span)
        middle = (resid[:, cols].astype(F32) + mixer_out).astype(BF16).astype(F32)
        middles.append(middle)
        squares = squares + jnp.sum(middle * middle, axis=-1, keepdims=True)
        rows = (middle * ngain_in[:, cols]).astype(BF16)
        stacked = jnp.concatenate(
            [
                jnp.concatenate(
                    [rows[:, q * WIDE + n * 128 : q * WIDE + (n + 1) * 128] for n in range(tiles)], axis=0
                )
                for q in range(piled)
            ],
            axis=1,
        )
        sent = dot(place, stacked, first)
        for q in range(piled):
            p = h * piled + q
            dm[p] = sent[:, q * 128 : (q + 1) * 128].reshape(nsp, 2 * tiles, 128).astype(BF16)

            @pl.loop(0, nsp - 1)
            def _(i):
                dst = peer(i, me, nsp)
                rcopy(dm.at[p, dst], dr.at[p, me], dsem.at[0, p], dsem.at[1, p], {"sp": dst}).start()

            dr[p, me] = dm[p, me]

    inverse = lax.rsqrt(squares * (1.0 / resid.shape[1]) + EPS)
    scales = jnp.zeros((nsp, 128), F32)
    for n in range(2):
        wanted = (iota((own, nsp), 1) * 2 + n).astype(F32)
        named = ((slots[0] == wanted) | (slots[1] == wanted)).astype(F32)
        scales = scales + dot(named, jnp.where(lane == n, inverse, 0.0), first, HIGH)
    for e in range(nsp):
        sm[e] = scales[e : e + 1]

    @pl.loop(0, nsp - 1)
    def _(i):
        dst = peer(i, me, nsp)
        rcopy(sm.at[dst], sr.at[me], csem.at[0], csem.at[1], {"sp": dst}).start()

    sr[me] = sm[me]

    r_dev = {"tp": right_y}
    l_dev = {"tp": left_y}
    for p in range(parts):
        wait_bytes(dr.at[p, pl.ds(0, others)], dsem.at[1, p])
        rowsf[...] = dr[p].astype(F32).reshape(nsp * 2 * tiles, 128)
        for q in range(per):
            j = p * per + q
            for n in range(width // 128):
                for s in range(2):
                    tile = q * (width // 128) + n
                    picked = rowsf[pl.ds(2 * tile + s, nsp, stride=2 * tiles), :]
                    xs[0, j, s * nsp : (s + 1) * nsp, n * 128 : (n + 1) * 128] = picked.astype(BF16)
            rcopy(xs.at[0, j], xs.at[1, j], ag_send.at[0, 0], ag_recv.at[0, 1, j], r_dev).start()
            rcopy(xs.at[0, j], xs.at[5, j], ag_send.at[1, 0], ag_recv.at[1, 1, j], l_dev).start()

    for load in loads[1:]:
        load.wait()
    for swap in swaps:
        swap.wait()

    rows1 = 2 * nsp
    top = pl.ds(0, nsp)
    low = pl.ds(nsp, nsp)

    def add_chunk(rows, j, acc):
        n = rows.shape[0]
        w = wgu[pl.ds(pl.multiple_of(j * width, width), width), :]
        acc[0:n] = jnp.where(j == 0, 0.0, acc[0:n]) + dot(rows, w)

    def scale_of(k):
        hit = iota((rows1, 128), 0) == iota((rows1, 128), 1)
        return jnp.sum(jnp.where(hit, xsc[k], 0.0), axis=1, keepdims=True)

    def activate(n, acc, scale):
        gate = acc[0:n, 0 : 2 * ff] * scale
        hidden[0:n] = (silu(gate) * (acc[0:n, 2 * ff : 4 * ff] * scale)).astype(BF16)

    def send_scale(k, way):
        at = k if way == 0 or k == 0 else 4 + k
        to = k + 1 if way == 0 else 5 + k
        dev = r_dev if way == 0 else l_dev
        rcopy(xsc.at[at], xsc.at[to], xsend.at[way, k], xrecv.at[way, k + 1], dev).start()

    def down(n, j):
        return dot(hidden[0:n], wdn[:, pl.ds(pl.multiple_of(j * width, width), width)])

    def down_pair(k, j):
        z = down(2 * rows1, j)
        zs[k, j] = z[0:rows1]
        zs[4 + k, j] = z[rows1 : 2 * rows1]

    @pl.loop(0, NCH)
    def _(j):
        add_chunk(xs[0, j], j, acc_own)

    wait_bytes(sr.at[pl.ds(0, others)], csem.at[1])
    given = jnp.concatenate([sr[d] for d in range(nsp)], axis=0)
    ring_row = jnp.zeros((1, 128), F32)
    for n in range(2):
        spot = iota((nsp, 128), 1) == iota((nsp, 128), 0) + n * nsp
        ring_row = ring_row + jnp.sum(jnp.where(spot, given[:, n : n + 1], 0.0), axis=0, keepdims=True)
    xsc[0] = ring_row
    send_scale(0, 0)
    send_scale(0, 1)

    @pl.loop(0, 3 * NCH)
    def _(t):
        k = 1 + t // NCH
        j = t % NCH
        wait_bytes(xs.at[k, j], ag_recv.at[0, k, j])
        wait_bytes(xs.at[4 + k, j], ag_recv.at[1, k, j])

        @pl.when(k < 3)
        def _():
            rcopy(xs.at[k, j], xs.at[k + 1, j], ag_send.at[0, k], ag_recv.at[0, k + 1, j], r_dev).start()
            rcopy(xs.at[4 + k, j], xs.at[5 + k, j], ag_send.at[1, k], ag_recv.at[1, k + 1, j], l_dev).start()

        @pl.when(k == 3)
        def _():
            rcopy(
                xs.at[3, j, top], xs.at[4, j, top], ag_send.at[0, 3], ag_recv.at[0, 4, j], r_dev
            ).start()
            rcopy(
                xs.at[7, j, low], xs.at[4, j, low], ag_send.at[1, 3], ag_recv.at[1, 4, j], l_dev
            ).start()

        add_chunk(jnp.concatenate([xs[k, j], xs[4 + k, j]], axis=0), j, acc)

        @pl.when(k > 1)
        def _():
            down_pair(k - 1, j)

        @pl.when(j == NCH - 1)
        def _():
            wait_bytes(xsc.at[k], xrecv.at[0, k])
            wait_bytes(xsc.at[4 + k], xrecv.at[1, k])
            send_scale(k, 0)

            @pl.when(k < 3)
            def _():
                rcopy(
                    xsc.at[4 + k], xsc.at[5 + k], xsend.at[1, k], xrecv.at[1, k + 1], l_dev
                ).start()

            activate(2 * rows1, acc, jnp.concatenate([scale_of(k), scale_of(4 + k)], axis=0))

    @pl.loop(0, NCH)
    def _(j):
        down_pair(3, j)
        sp_b[2, j, nsp:rows1] = zs[7, j, nsp:rows1].astype(BF16)
        sn_b[2, j, 0:nsp] = zs[3, j, 0:nsp].astype(BF16)
        rcopy(
            sp_b.at[2, j, low], rp_b.at[2, j, low], rs_send.at[0, 2], rs_recv.at[0, 2, j], r_dev
        ).start()
        rcopy(
            sn_b.at[2, j, top], rn_b.at[2, j, top], rs_send.at[1, 2], rs_recv.at[1, 2, j], l_dev
        ).start()
        wait_bytes(xs.at[4, j, top], ag_recv.at[0, 4, j])
        wait_bytes(xs.at[4, j, low], ag_recv.at[1, 4, j])
        add_chunk(xs[4, j], j, acc)

    wait_bytes(xsc.at[4], xrecv.at[0, 4])
    activate(rows1, acc, scale_of(4))

    @pl.loop(0, NCH)
    def _(j):
        z = down(rows1, j)
        sp_b[3, j, 0:nsp] = z[0:nsp].astype(BF16)
        sn_b[3, j, nsp:rows1] = z[nsp:rows1].astype(BF16)
        rcopy(
            sp_b.at[3, j, top], rp_b.at[3, j, top], rs_send.at[0, 3], rs_recv.at[0, 3, j], r_dev
        ).start()
        rcopy(
            sn_b.at[3, j, low], rn_b.at[3, j, low], rs_send.at[1, 3], rs_recv.at[1, 3, j], l_dev
        ).start()

    activate(rows1, acc_own, scale_of(0))

    @pl.loop(0, NCH)
    def _(j):
        zs[0, j] = down(rows1, j)

    @pl.loop(0, NCH)
    def _(j):
        wait_bytes(rp_b.at[3, j, top], rs_recv.at[0, 3, j])
        wait_bytes(rn_b.at[3, j, low], rs_recv.at[1, 3, j])
        sp_b[2, j, 0:nsp] = (zs[7, j, 0:nsp] + rp_b[3, j, 0:nsp].astype(F32)).astype(BF16)
        sn_b[2, j, nsp:rows1] = (zs[3, j, nsp:rows1] + rn_b[3, j, nsp:rows1].astype(F32)).astype(BF16)
        rcopy(
            sp_b.at[2, j, top], rp_b.at[2, j, top], rs_send.at[0, 2], rs_recv.at[0, 2, j], r_dev
        ).start()
        rcopy(
            sn_b.at[2, j, low], rn_b.at[2, j, low], rs_send.at[1, 2], rs_recv.at[1, 2, j], l_dev
        ).start()

    @pl.loop(0, 2 * NCH)
    def _(t):
        k = 2 - t // NCH
        j = t % NCH
        wait_bytes(rp_b.at[k, j], rs_recv.at[0, k, j])
        wait_bytes(rn_b.at[k, j], rs_recv.at[1, k, j])
        sp_b[k - 1, j] = (zs[4 + k, j] + rp_b[k, j].astype(F32)).astype(BF16)
        sn_b[k - 1, j] = (zs[k, j] + rn_b[k, j].astype(F32)).astype(BF16)
        rcopy(
            sp_b.at[k - 1, j], rp_b.at[k - 1, j], rs_send.at[0, k - 1], rs_recv.at[0, k - 1, j], r_dev
        ).start()
        rcopy(
            sn_b.at[k - 1, j], rn_b.at[k - 1, j], rs_send.at[1, k - 1], rs_recv.at[1, k - 1, j], l_dev
        ).start()

    for p in range(parts):
        for q in range(per):
            j = p * per + q
            wait_bytes(rp_b.at[0, j], rs_recv.at[0, 0, j])
            wait_bytes(rn_b.at[0, j], rs_recv.at[1, 0, j])
            total = zs[0, j] + rp_b[0, j].astype(F32) + rn_b[0, j].astype(F32)
            for n in range(width // 128):
                for s in range(2):
                    tile = q * (width // 128) + n
                    rowsf[pl.ds(2 * tile + s, nsp, stride=2 * tiles), :] = total[
                        s * nsp : (s + 1) * nsp, n * 128 : (n + 1) * 128
                    ]
        bm[p] = rowsf[...].reshape(nsp, 2 * tiles, 128).astype(BF16)

        @pl.loop(0, nsp - 1)
        def _(i):
            dst = peer(i, me, nsp)
            rcopy(bm.at[p, dst], br.at[p, me], bsem.at[0, p], bsem.at[1, p], {"sp": dst}).start()

        br[p, me] = bm[p, me]

    for p in range(parts):
        wait_bytes(br.at[p, pl.ds(0, others)], bsem.at[1, p])
        back = br[p].astype(F32).reshape(nsp * 2 * tiles, 128).astype(BF16)
        mixed = dot(mix_hi, back) + dot(mix_lo, back)
        for n in range(tiles):
            cols = slice(p * WIDE + n * 128, p * WIDE + (n + 1) * 128)
            local = slice(cols.start % (2 * span), cols.start % (2 * span) + 128)
            base = middles[cols.start // (2 * span)][:, local]
            out[:, cols] = (base + mixed[n * own : (n + 1) * own]).astype(BF16)

    wait_bytes(hl, hsem.at[0])
    wait_bytes(hr, hsem.at[2])
    wait_bytes(tot_r.at[pl.ds(0, others)], tsem.at[0])
    wait_bytes(st_r.at[pl.ds(0, others)], ssem.at[0])
    wait_bytes(sc_r.at[pl.ds(0, others)], osem.at[0])
    wait_bytes(blocks(4), wnear.at[0])

    @pl.when(x > 0)
    def _():
        wait_bytes(blocks(1), wfar.at[0])
        wait_bytes(blocks(nx - 1), wsem.at[0])

    for h in range(2):
        wait_bytes(mo.at[h, pl.ds(0, ntp - 5)], psem.at[0, h])
        for copy in relays[h]:
            copy.wait_send()
    wait_bytes(sr.at[pl.ds(0, others)], csem.at[0])
    for k in range(4):
        wait_bytes(xsc.at[0], xsend.at[0, k])
    for k in range(3):
        wait_bytes(xsc.at[0], xsend.at[1, k])
    for p in range(parts):
        wait_bytes(dr.at[p, pl.ds(0, others)], dsem.at[0, p])
        wait_bytes(br.at[p, pl.ds(0, others)], bsem.at[0, p])
    for way in range(2):
        for k in range(3):
            wait_bytes(xs.at[0], ag_send.at[way, k])
            wait_bytes(xs.at[0], rs_send.at[way, k])
        wait_bytes(xs.at[0, pl.ds(0, 2)], ag_send.at[way, 3])
        wait_bytes(xs.at[0, pl.ds(0, 2)], rs_send.at[way, 3])


def layer(nsp, ntp, resid, v, k, q, og, raw, hdl, extra, vf, kf, qf, gain, wout, ngain, routes, cw, wg, wu, wd):
    ny = ntp // 2
    tokens = v.shape[0]
    own = tokens // ntp
    width = resid.shape[1] // NCH
    ff = wg.shape[2]
    chan = wout.shape[0] // ny
    rows1 = 2 * nsp

    small = [
        resid,
        v,
        k,
        q,
        og,
        raw.transpose(0, 2, 1),
        hdl,
        extra.T,
        vf,
        kf,
        qf,
        gain.reshape(1, -1),
        ngain.reshape(1, -1),
        routes.T,
        cw.T,
    ]
    dma = pltpu.SemaphoreType.DMA
    hbm = pl.BlockSpec(memory_space=pl.ANY)
    pair = (nsp, 16, 128)
    parts = resid.shape[1] // WIDE
    msg = (parts, nsp, WIDE // 64, 128)
    ring = (4, NCH, rows1, width)
    scratch = [pltpu.VMEM(x.shape, x.dtype) for x in small] + [
        pltpu.VMEM((2, 8, tokens), F32),
        pltpu.VMEM((16, 512), BF16),
        pltpu.VMEM((16, 512), BF16),
        pltpu.VMEM((tokens + 32, 512), F32),
        pltpu.VMEM((1, 128), F32),
        pltpu.VMEM((nsp, 1, 128), F32),
        pltpu.VMEM((2, nsp, 128), F32),
        pltpu.VMEM(pair, BF16),
        pltpu.VMEM(pair, BF16),
        pltpu.VMEM(pair, F32),
        pltpu.VMEM(pair, BF16),
        pltpu.VMEM(pair, BF16),
        pltpu.VMEM((2, tokens, 256), BF16),
        pltpu.VMEM((chan, 128 * ny), BF16),
        pltpu.VMEM((2, ntp, own, 64 * ny), BF16),
        pltpu.VMEM((2, ntp, own, 64 * ny), BF16),
        pltpu.VMEM((2, 2, 2, own, 64 * ny), BF16),
        pltpu.VMEM((2, 2, 2, own, 64 * ny), BF16),
        pltpu.VMEM((nsp, 1, 128), F32),
        pltpu.VMEM((nsp, 1, 128), F32),
        pltpu.VMEM((8, 1, 128), F32),
        pltpu.VMEM((rows1, 4 * ff), F32),
        pltpu.VMEM(msg, BF16),
        pltpu.VMEM(msg, BF16),
        pltpu.VMEM((nsp * WIDE // 64, 128), F32),
        pltpu.VMEM((8, NCH, rows1, width), BF16),
        pltpu.VMEM((wg.shape[1], 4 * ff), BF16),
        pltpu.VMEM((2 * ff, wd.shape[2]), BF16),
        pltpu.VMEM((2 * rows1, 4 * ff), F32),
        pltpu.VMEM((2 * rows1, 2 * ff), BF16),
        pltpu.VMEM((8, NCH, rows1, width), F32),
        pltpu.VMEM(ring, BF16),
        pltpu.VMEM(ring, BF16),
        pltpu.VMEM(ring, BF16),
        pltpu.VMEM(ring, BF16),
        pltpu.VMEM(msg, BF16),
        pltpu.VMEM(msg, BF16),
        dma((4,)),
        dma((4,)),
        dma((2,)),
        dma((2,)),
        dma((2,)),
        dma((2, 2)),
        dma((2,)),
        dma((2,)),
        dma((2,)),
        dma((6,)),
        dma((2, 2)),
        dma((2, 2, 2, 2)),
        dma((2,)),
        dma((2, 4)),
        dma((2, 5)),
        dma((2, parts)),
        dma((2, 4)),
        dma((2, 5, NCH)),
        dma((2, 4)),
        dma((2, 4, NCH)),
        dma((2, parts)),
        dma((NSMALL,)),
    ]
    return pl.pallas_call(
        functools.partial(body, nsp, ntp),
        out_shape=jax.ShapeDtypeStruct(resid.shape, BF16),
        in_specs=[hbm] * (NSMALL + 4),
        out_specs=pl.BlockSpec(memory_space=pltpu.VMEM),
        scratch_shapes=scratch,
        compiler_params=pltpu.CompilerParams(
            collective_id=0, has_side_effects=True, vmem_limit_bytes=56 * 1024 * 1024
        ),
        name="layer",
    )(*small, wout, wg[0], wu[0], wd[0])


def solution(mesh):
    both = ("sp", "tp")
    return jax.shard_map(
        functools.partial(layer, mesh.shape["sp"], mesh.shape["tp"]),
        mesh=mesh,
        in_specs=(
            P(both, None),
            P("sp", "tp"),
            P("sp", "tp"),
            P("sp", "tp"),
            P("sp", "tp"),
            P(None, "sp", "tp"),
            P(None, "tp"),
            P("sp", "tp"),
            P(None, "tp"),
            P(None, "tp"),
            P(None, "tp"),
            P("tp"),
            P(None, "tp"),
            P(),
            P("sp", None),
            P(both, None),
            P("sp", None, "tp"),
            P("sp", None, "tp"),
            P("sp", "tp", None),
        ),
        out_specs=P(both, None),
        check_vma=False,
    )
```

```python
import functools

import jax
import jax.numpy as jnp
from jax import lax
from jax.experimental import pallas as pl
from jax.experimental.pallas import tpu as pltpu
from jax.sharding import PartitionSpec as P

MESH = pl.DeviceIdType.MESH
HIGH = lax.Precision.HIGHEST
F32 = jnp.float32
BF16 = jnp.bfloat16
EPS = 1e-06
BLOCK = 128
NCH = 4
NX = 4
WIDE = 512
NSMALL = 15


def dot(a, b, contract=((1,), (0,)), precision=None):
    return lax.dot_general(
        a, b, (contract, ((), ())), preferred_element_type=F32, precision=precision
    )


def silu(v):
    return v / (1.0 + jnp.exp(-v))


def rcopy(src, dst, send, recv, dev):
    return pltpu.make_async_remote_copy(
        src_ref=src, dst_ref=dst, send_sem=send, recv_sem=recv, device_id=dev, device_id_type=MESH
    )


def wait_bytes(ref, sem):
    pltpu.make_async_copy(ref, ref, sem).wait()


def peer(i, me, n):
    step = n - 2 - i
    return (me + jnp.where(step % 2 == 0, step // 2 + 1, n - 1 - step // 2)) % n


def iota(shape, dim):
    return lax.broadcasted_iota(jnp.int32, shape, dim)


def body(
    nsp,
    ntp,
    *refs,
):
    small_hbm, (wout, wg, wu, wd), out = refs[:NSMALL], refs[NSMALL : NSMALL + 4], refs[NSMALL + 4]
    small = refs[NSMALL + 5 : 2 * NSMALL + 5]
    resid, v_in, k_in, q_in, og_in, raw_in, hdl_in, extra_in = small[:8]
    vf_in, kf_in, qf_in, gain_in, ngain_in, routes_in, cw_in = small[8:]
    (
    raw8,
    hl,
    hr,
    pad,
    tot_s,
    tot_r,
    decay,
    st_s,
    st_r,
    sc_f,
    sc_s,
    sc_r,
    heads,
    wc,
    po,
    mo,
    near,
    through,
    sm,
    sr,
    xsc,
    acc_own,
    dm,
    dr,
    rowsf,
    xs,
    wgu,
    wdn,
    acc,
    hidden,
    zs,
    sp_b,
    sn_b,
    rp_b,
    rn_b,
    bm,
    br,
    lsem,
    hsem,
    tsem,
    ssem,
    osem,
    hdsem,
    wsem,
    wnear,
    wfar,
    swsem,
    psem,
    nsem,
    csem,
    xsend,
    xrecv,
    dsem,
    ag_send,
    ag_recv,
    rs_send,
    rs_recv,
    bsem,
    isem,
    ) = refs[2 * NSMALL + 5 :]
    me = lax.axis_index("sp")
    tp = lax.axis_index("tp")
    ny = ntp // 2
    y = tp // 2
    c = tp % 2
    partner = y * 2 + (1 - c)
    right_y = ((y + 1) % ny) * 2 + c
    left_y = ((y + ny - 1) % ny) * 2 + c
    others = nsp - 1
    inputs = [
        pltpu.make_async_copy(src, dst, isem.at[n]) for n, (src, dst) in enumerate(zip(small_hbm, small))
    ]
    for n in (5, 6, 7, 1, 2, 3, 8, 9, 10, 4, 13, 14, 0, 11, 12):
        inputs[n].start()

    bar = pltpu.get_barrier_semaphore()

    @pl.loop(1, nsp)
    def _(i):
        pl.semaphore_signal(bar, inc=1, device_id={"sp": (me + i) % nsp}, device_id_type=MESH)

    @pl.loop(1, ntp)
    def _(i):
        pl.semaphore_signal(bar, inc=1, device_id={"tp": (tp + i) % ntp}, device_id_type=MESH)

    ff = wg.shape[1]
    chan = wout.shape[0] // ny
    nx = NX
    x = me % nx

    def w_rows(of):
        return wout.at[pl.ds(pl.multiple_of(of * chan, chan), chan)]

    def w_block(of):
        return wc.at[:, pl.ds(pl.multiple_of(of * 128, 128), 128)]

    loads = [
        pltpu.make_async_copy(w_rows(y), w_block(y), lsem.at[3]),
        pltpu.make_async_copy(wg, wgu.at[:, pl.ds(0, ff)], lsem.at[0]),
        pltpu.make_async_copy(wu, wgu.at[:, pl.ds(2 * ff, ff)], lsem.at[1]),
        pltpu.make_async_copy(wd, wdn.at[pl.ds(0, ff)], lsem.at[2]),
    ]
    for load in loads:
        load.start()

    tokens = v_in.shape[0]
    for n in (1, 2, 3):
        inputs[n].wait()

    pl.semaphore_wait(bar, nsp - 1 + ntp - 1)

    right = {"sp": (me + 1) % nsp}
    left = {"sp": (me + nsp - 1) % nsp}
    for ref, lo, width in ((v_in, 0, 256), (k_in, 256, 128), (q_in, 384, 128)):
        cols = pl.ds(lo, width)
        rcopy(ref.at[pl.ds(tokens - 16, 16)], hl.at[:, cols], hsem.at[0], hsem.at[1], right).start()
        rcopy(ref.at[pl.ds(0, 16)], hr.at[:, cols], hsem.at[2], hsem.at[3], left).start()

    far = 2 + x

    def w_send(distance, send, recv):
        dst = (y + ny - distance) % ny
        return rcopy(w_rows(dst), w_block(y), send, recv, {"tp": dst * 2 + c})

    @pl.when(x > 0)
    def _():
        w_send(far, wfar.at[0], wfar.at[1]).start()

    for distance in (1, -1, 2, -2):
        w_send(distance, wnear.at[0], wnear.at[1]).start()

    def w_relay():
        block = w_block((y + far) % ny)
        wait_bytes(block, wfar.at[1])
        for i in range(1, nx):
            to = me - x + (x + i) % nx
            rcopy(block, block, wsem.at[0], wsem.at[1], {"sp": to}).start()

    for n in (5, 6, 7):
        inputs[n].wait()
    raw8[0, 0:4] = raw_in[0].astype(F32)
    raw8[0, 4:8] = raw_in[1].astype(F32)
    raw8[1, 0:4] = extra_in[...]
    raw8[1, 4:8] = extra_in[...]
    sub = iota((8, 1), 0)
    rates = jnp.where(
        sub < 4, jnp.broadcast_to(hdl_in[0:1], (8, 4)), jnp.broadcast_to(hdl_in[1:2], (8, 4))
    )
    rates = jnp.sum(jnp.where(iota((8, 4), 0) % 4 == iota((8, 4), 1), rates, 0.0), axis=1, keepdims=True)
    step8 = raw8[0]
    step8 = jnp.maximum(step8, 0.0) + jnp.log1p(jnp.exp(-jnp.abs(step8)))
    log8 = raw8[1] - jnp.exp(rates) * step8
    lane = iota((1, 128), 1)
    row = iota((BLOCK, BLOCK), 0)
    col = iota((BLOCK, BLOCK), 1)
    upper = (row <= col).astype(F32)
    spread = ((iota((8, 512), 1) // 64) == iota((8, 512), 0)).astype(F32)
    cum, cum_t, tot_c, sw8, rd8 = [], [], [], [], []
    for b in range(2):
        logs = log8[:, b * BLOCK : (b + 1) * BLOCK]
        run = dot(logs, upper, precision=HIGH)
        total = run[:, BLOCK - 1 : BLOCK]
        both = jnp.where(sub < 4, run, run - logs)
        cum_t.append(both)
        cum.append(jnp.concatenate([both, jnp.zeros((120, BLOCK), F32)], axis=0).T)
        tot_c.append(jnp.broadcast_to(total, (8, 128)))
        sw8.append(jnp.exp(jnp.where(sub < 4, total - both, both)))
        rd8.append(jnp.exp(jnp.where(sub < 4, both, total - both)))
    tot_dev = jnp.exp(tot_c[0] + tot_c[1])
    tot_row = jnp.sum(jnp.where(sub == lane, tot_dev, 0.0), axis=0, keepdims=True)
    tot_s[...] = tot_row
    tot_r[me] = tot_row
    first = ((0,), (0,))
    step_x = dot(step8, spread, first, HIGH)
    sw_x = [dot(sw8[b], spread, first, HIGH) for b in range(2)]
    rd_x = [dot(rd8[b], spread, first, HIGH) for b in range(2)]

    def head_rows(b, first):
        e = jnp.exp(tot_c[b][first : first + 4])
        return jnp.concatenate([jnp.broadcast_to(e[h : h + 1], (64, 128)) for h in range(4)], axis=0)

    @pl.loop(0, nsp - 1)
    def _(i):
        rcopy(tot_s, tot_r.at[me], tsem.at[0], tsem.at[1], {"sp": peer(i, me, nsp)}).start()

    pad[16 : 16 + tokens, 0:256] = v_in[...].astype(F32)
    pad[16 : 16 + tokens, 256:384] = k_in[...].astype(F32)
    pad[16 : 16 + tokens, 384:512] = q_in[...].astype(F32)
    for n in (0, 4, *range(8, NSMALL)):
        inputs[n].wait()
    wait_bytes(hl, hsem.at[1])
    wait_bytes(hr, hsem.at[3])
    pad[0:16] = jnp.where(me > 0, hl[...].astype(F32), 0.0)
    pad[16 + tokens : 32 + tokens] = jnp.where(me < nsp - 1, hr[...].astype(F32), 0.0)
    filt = jnp.concatenate([vf_in[...], kf_in[...], qf_in[...]], axis=1).astype(F32)
    conv = filt[0:1] * pad[14 : 14 + tokens]
    for o in range(1, 5):
        conv = conv + filt[o : o + 1] * pad[14 + o : 14 + o + tokens]
    values = conv[:, 0:256].astype(BF16).astype(F32)
    keys = silu(conv[:, 256:384]).astype(BF16)
    queries = silu(conv[:, 384:512]).astype(BF16)
    scaled = (jnp.concatenate([values, values], axis=1) * step_x).astype(BF16)

    part = []
    for b in range(2):
        rows = slice(b * BLOCK, (b + 1) * BLOCK)
        weighted = (scaled[rows].astype(F32) * sw_x[b]).astype(BF16)
        part.append(dot(weighted, keys[rows], ((0,), (0,))))
    final_f = head_rows(1, 0) * part[0][0:256] + part[1][0:256]
    final_b = head_rows(0, 4) * part[1][256:512] + part[0][256:512]
    piece = 256 // nsp
    mine = jnp.concatenate(
        [final_f.reshape(nsp, piece, 128), final_b.reshape(nsp, piece, 128)], axis=1
    ).astype(BF16)
    st_s[...] = mine

    @pl.loop(0, nsp - 1)
    def _(i):
        dst = peer(i, me, nsp)
        rcopy(st_s.at[dst], st_r.at[me], ssem.at[0], ssem.at[1], {"sp": dst}).start()

    st_r[me] = st_s[me]

    inner = []
    lo_half = lane < 64
    for b in range(2):
        rows = slice(b * BLOCK, (b + 1) * BLOCK)
        score = dot(queries[rows], keys[rows], ((1,), (1,)))
        pairs = []
        for pair in range(2):
            halves = []
            for h in (2 * pair, 2 * pair + 1):
                f_gap = cum[b][:, h : h + 1] - cum_t[b][h : h + 1, :]
                b_gap = cum_t[b][4 + h : 5 + h, :] - cum[b][:, 4 + h : 5 + h]
                w = score * jnp.exp(jnp.where(col <= row, f_gap, b_gap))
                w_f = jnp.where(col <= row, w, 0.0)
                w_b = jnp.where(col >= row, w, 0.0)
                both = jnp.concatenate([w_f, w_b], axis=1).astype(BF16)
                lanes = slice(128 * pair, 128 * pair + 128)
                rhs = jnp.concatenate(
                    [scaled[rows, lanes], scaled[rows, 256 + 128 * pair : 384 + 128 * pair]], axis=0
                )
                halves.append(dot(both, rhs))
            pairs.append(jnp.where(lo_half, halves[0], halves[1]))
        inner.append(jnp.concatenate(pairs, axis=1))
    gate_act = silu(og_in[...].astype(F32))

    own = tokens // ntp
    mine_lane = iota((own, tokens), 1) == iota((own, tokens), 0) + tp * own
    e_lane = iota((own, 128), 1).astype(F32)
    hots = []
    for n in range(2):
        ids = jnp.where(mine_lane, routes_in[n : n + 1].astype(F32), 0.0)
        hots.append((jnp.sum(ids, axis=1, keepdims=True) == e_lane).astype(F32))
    strict = (iota((own, own), 1) < iota((own, own), 0)).astype(F32)
    ids = e_lane * 2.0 + dot(strict, hots[0] + hots[1], precision=HIGH)
    tiles = WIDE // 128
    r_id = iota((tiles * own, nsp * 2 * tiles), 1)
    t_id = iota((tiles * own, nsp * 2 * tiles), 0)
    r_slot = ((r_id // (2 * tiles)) * 2 + r_id % 2).astype(F32)
    same = ((r_id // 2) % tiles) == (t_id // own)
    w_lane = iota((tiles * own, own), 0) % own == iota((tiles * own, own), 1)
    mixing = jnp.zeros(r_id.shape, F32)
    place = jnp.zeros(r_id.shape, F32)
    slots = []
    for n in range(2):
        slot = jnp.sum(hots[n] * ids, axis=1, keepdims=True)
        slots.append(slot)
        hit = same & (r_slot == jnp.concatenate([slot] * tiles, axis=0))
        weight = jnp.sum(jnp.where(w_lane, cw_in[n : n + 1], 0.0), axis=1, keepdims=True)
        place = jnp.where(hit, 1.0, place)
        mixing = jnp.where(hit, weight, mixing)
    place = place.astype(BF16)
    mix_hi = mixing.astype(BF16)
    mix_lo = (mixing - mix_hi.astype(F32)).astype(BF16)

    @pl.when(x > 0)
    def _():
        w_relay()

    wait_bytes(tot_r.at[pl.ds(0, others)], tsem.at[1])
    head = me // (64 // piece)
    totals = jnp.concatenate([tot_r[d] for d in range(nsp)], axis=0)
    for n in range(2):
        of_head = jnp.sum(jnp.where(lane == head + 4 * n, totals, 0.0), axis=1, keepdims=True)
        decay[n] = jnp.broadcast_to(of_head, (nsp, 128))

    def scan(i, carry):
        d = nsp - 1 - i
        sc_f[i, 0:piece] = carry[0]
        sc_f[d, piece : 2 * piece] = carry[1]
        return (
            decay[0, pl.ds(i, 1), :] * carry[0] + st_r[i].astype(F32)[0:piece],
            decay[1, pl.ds(d, 1), :] * carry[1] + st_r[d].astype(F32)[piece : 2 * piece],
        )

    wait_bytes(st_r.at[pl.ds(0, others)], ssem.at[1])
    zero = jnp.zeros((piece, 128), F32)
    lax.fori_loop(0, nsp, scan, (zero, zero), unroll=8)
    sc_s[...] = sc_f[...].astype(BF16)

    @pl.loop(0, nsp - 1)
    def _(i):
        dst = peer(i, me, nsp)
        rcopy(sc_s.at[dst], sc_r.at[me], osem.at[0], osem.at[1], {"sp": dst}).start()

    sc_r[me] = sc_s[me]
    wait_bytes(sc_r.at[pl.ds(0, others)], osem.at[1])

    around = sc_r[...].astype(F32)
    enter = around[:, 0:piece].reshape(256, 128)
    leave = around[:, piece : 2 * piece].reshape(256, 128)
    enters = [enter, head_rows(0, 0) * enter + part[0][0:256]]
    leaves = [head_rows(1, 4) * leave + part[1][256:512], leave]
    group = jnp.where(iota((256, 256), 0) // 64 == iota((256, 256), 1) // 64, 1.0 / 64.0, 0.0).astype(BF16)
    swap_h = []
    for b in range(2):
        rows = slice(b * BLOCK, (b + 1) * BLOCK)
        state = jnp.concatenate([enters[b], leaves[b]], axis=0).astype(BF16)
        read = dot(queries[rows], state, ((1,), (1,))) * rd_x[b]
        gated = (inner[b] + read[:, 0:256] + read[:, 256:512]) * gate_act[rows]
        square = gated * gated
        square_hi = square.astype(BF16)
        mean = dot(square_hi, group) + dot((square - square_hi.astype(F32)).astype(BF16), group)
        normed = gated * lax.rsqrt(mean + EPS) * gain_in[...]
        heads[c, rows, :] = normed.astype(BF16)
        half = heads.at[c, pl.ds(b * BLOCK, BLOCK)]
        copy = rcopy(half, half, hdsem.at[0, b], hdsem.at[1, b], {"tp": partner})
        copy.start()
        swap_h.append(copy)

    def blocks(n):
        return wc.at[:, pl.ds(0, 128 * n)]

    loads[0].wait()
    wait_bytes(blocks(4), wnear.at[1])

    @pl.when(x == 0)
    def _():
        wait_bytes(blocks(nx - 1), wsem.at[1])

    @pl.when(x > 0)
    def _():
        wait_bytes(blocks(nx - 2), wsem.at[1])

    inner_c = chan // 2
    own_part = dot(heads[c], wc[pl.ds(pl.multiple_of(c * inner_c, inner_c), inner_c), :])
    for copy in swap_h:
        copy.wait()
    o_c = 1 - c
    full = own_part + dot(heads[o_c], wc[pl.ds(pl.multiple_of(o_c * inner_c, inner_c), inner_c), :])
    span = full.shape[1] // 2
    for h in range(2):
        po[h] = full[:, h * span : (h + 1) * span].reshape(ntp, own, span).astype(BF16)

    def chip(distance, core):
        return ((y + ny + distance) % ny) * 2 + core

    relays = [[], []]

    def send_far(h):
        for way in range(2):
            sign = 1 - 2 * way
            for core in range(2):
                copy = rcopy(
                    po.at[h, chip(3 * sign, core)],
                    near.at[h, way, core],
                    nsem.at[0, h, way, core],
                    nsem.at[1, h, way, core],
                    {"tp": chip(sign, c)},
                )
                copy.start()
                relays[h].append(copy)

    def send_direct(h):
        for distance in (4, 1, -1):
            for core in range(2):
                dst = chip(distance, core)
                rcopy(po.at[h, dst], mo.at[h, tp], psem.at[0, h], psem.at[1, h], {"tp": dst}).start()
        rcopy(po.at[h, partner], mo.at[h, tp], psem.at[0, h], psem.at[1, h], {"tp": partner}).start()
        mo[h, tp] = po[h, tp]

    def send_through(h):
        for way in range(2):
            for core in range(2):
                dst = chip(2 - 4 * way, core)
                relays[h][2 * way + core].wait_recv()
                through[h, way, core] = (
                    po[h, dst].astype(F32) + near[h, way, core].astype(F32)
                ).astype(BF16)
                rcopy(
                    through.at[h, way, core], mo.at[h, tp], psem.at[0, h], psem.at[1, h], {"tp": dst}
                ).start()

    send_far(0)
    send_direct(0)
    send_far(1)
    send_through(0)
    send_direct(1)
    send_through(1)

    swaps = [
        rcopy(wg, wgu.at[:, pl.ds(ff, ff)], swsem.at[0], swsem.at[1], {"tp": partner}),
        rcopy(wu, wgu.at[:, pl.ds(3 * ff, ff)], swsem.at[2], swsem.at[3], {"tp": partner}),
        rcopy(wd, wdn.at[pl.ds(ff, ff)], swsem.at[4], swsem.at[5], {"tp": partner}),
    ]
    for swap in swaps:
        swap.start()

    parts = resid.shape[1] // WIDE
    width = resid.shape[1] // NCH
    per = NCH // parts
    piled = parts // 2
    middles = []
    squares = jnp.zeros((own, 1), F32)
    for h in range(2):
        wait_bytes(mo.at[h, pl.ds(0, ntp - 5)], psem.at[1, h])
        halves = []
        for core in range(2):
            total = mo[h, chip(0, core)].astype(F32)
            for distance in (1, -1, 2, -2, 4):
                total = total + mo[h, chip(distance, core)].astype(F32)
            halves.append(total)
        pieces = []
        for j in range(span // 128):
            pieces += [halves[0][:, 128 * j : 128 * j + 128], halves[1][:, 128 * j : 128 * j + 128]]
        mixer_out = jnp.concatenate(pieces, axis=1).astype(BF16).astype(F32)
        cols = slice(h * 2 * span, (h + 1) * 2 * span)
        middle = (resid[:, cols].astype(F32) + mixer_out).astype(BF16).astype(F32)
        middles.append(middle)
        squares = squares + jnp.sum(middle * middle, axis=-1, keepdims=True)
        rows = (middle * ngain_in[:, cols]).astype(BF16)
        stacked = jnp.concatenate(
            [
                jnp.concatenate(
                    [rows[:, q * WIDE + n * 128 : q * WIDE + (n + 1) * 128] for n in range(tiles)], axis=0
                )
                for q in range(piled)
            ],
            axis=1,
        )
        sent = dot(place, stacked, first)
        for q in range(piled):
            p = h * piled + q
            dm[p] = sent[:, q * 128 : (q + 1) * 128].reshape(nsp, 2 * tiles, 128).astype(BF16)

            @pl.loop(0, nsp - 1)
            def _(i):
                dst = peer(i, me, nsp)
                rcopy(dm.at[p, dst], dr.at[p, me], dsem.at[0, p], dsem.at[1, p], {"sp": dst}).start()

            dr[p, me] = dm[p, me]

    inverse = lax.rsqrt(squares * (1.0 / resid.shape[1]) + EPS)
    scales = jnp.zeros((nsp, 128), F32)
    for n in range(2):
        wanted = (iota((own, nsp), 1) * 2 + n).astype(F32)
        named = ((slots[0] == wanted) | (slots[1] == wanted)).astype(F32)
        scales = scales + dot(named, jnp.where(lane == n, inverse, 0.0), first, HIGH)
    for e in range(nsp):
        sm[e] = scales[e : e + 1]

    @pl.loop(0, nsp - 1)
    def _(i):
        dst = peer(i, me, nsp)
        rcopy(sm.at[dst], sr.at[me], csem.at[0], csem.at[1], {"sp": dst}).start()

    sr[me] = sm[me]

    r_dev = {"tp": right_y}
    l_dev = {"tp": left_y}
    for p in range(parts):
        wait_bytes(dr.at[p, pl.ds(0, others)], dsem.at[1, p])
        rowsf[0 : nsp * 2 * tiles] = dr[p].astype(F32).reshape(nsp * 2 * tiles, 128)
        for q in range(per):
            j = p * per + q
            for n in range(width // 128):
                for s in range(2):
                    tile = q * (width // 128) + n
                    picked = rowsf[pl.ds(2 * tile + s, nsp, stride=2 * tiles), :]
                    xs[0, j, s * nsp : (s + 1) * nsp, n * 128 : (n + 1) * 128] = picked.astype(BF16)
            rcopy(xs.at[0, j], xs.at[1, j], ag_send.at[0, 0], ag_recv.at[0, 1, j], r_dev).start()
            rcopy(xs.at[0, j], xs.at[5, j], ag_send.at[1, 0], ag_recv.at[1, 1, j], l_dev).start()

    for load in loads[1:]:
        load.wait()
    for swap in swaps:
        swap.wait()

    rows1 = 2 * nsp
    top = pl.ds(0, nsp)
    low = pl.ds(nsp, nsp)

    def add_chunk(rows, j, acc):
        n = rows.shape[0]
        w = wgu[pl.ds(pl.multiple_of(j * width, width), width), :]
        acc[0:n] = jnp.where(j == 0, 0.0, acc[0:n]) + dot(rows, w)

    def scale_of(k):
        hit = iota((rows1, 128), 0) == iota((rows1, 128), 1)
        return jnp.sum(jnp.where(hit, xsc[k], 0.0), axis=1, keepdims=True)

    def activate(n, acc, scale):
        gate = acc[0:n, 0 : 2 * ff] * scale
        hidden[0:n] = (silu(gate) * (acc[0:n, 2 * ff : 4 * ff] * scale)).astype(BF16)

    def send_scale(k, way):
        at = k if way == 0 or k == 0 else 4 + k
        to = k + 1 if way == 0 else 5 + k
        dev = r_dev if way == 0 else l_dev
        rcopy(xsc.at[at], xsc.at[to], xsend.at[way, k], xrecv.at[way, k + 1], dev).start()

    def down(n, j):
        return dot(hidden[0:n], wdn[:, pl.ds(pl.multiple_of(j * width, width), width)])

    def down_pair(k, j):
        z = down(2 * rows1, j)
        zs[k, j] = z[0:rows1]
        zs[4 + k, j] = z[rows1 : 2 * rows1]

    @pl.loop(0, NCH)
    def _(j):
        add_chunk(xs[0, j], j, acc_own)

    wait_bytes(sr.at[pl.ds(0, others)], csem.at[1])
    given = jnp.concatenate([sr[d] for d in range(nsp)], axis=0)
    ring_row = jnp.zeros((1, 128), F32)
    for n in range(2):
        spot = iota((nsp, 128), 1) == iota((nsp, 128), 0) + n * nsp
        ring_row = ring_row + jnp.sum(jnp.where(spot, given[:, n : n + 1], 0.0), axis=0, keepdims=True)
    xsc[0] = ring_row
    send_scale(0, 0)
    send_scale(0, 1)

    @pl.loop(0, 3 * NCH)
    def _(t):
        k = 1 + t // NCH
        j = t % NCH
        wait_bytes(xs.at[k, j], ag_recv.at[0, k, j])
        wait_bytes(xs.at[4 + k, j], ag_recv.at[1, k, j])

        @pl.when(k < 3)
        def _():
            rcopy(xs.at[k, j], xs.at[k + 1, j], ag_send.at[0, k], ag_recv.at[0, k + 1, j], r_dev).start()
            rcopy(xs.at[4 + k, j], xs.at[5 + k, j], ag_send.at[1, k], ag_recv.at[1, k + 1, j], l_dev).start()

        @pl.when(k == 3)
        def _():
            rcopy(
                xs.at[3, j, top], xs.at[4, j, top], ag_send.at[0, 3], ag_recv.at[0, 4, j], r_dev
            ).start()
            rcopy(
                xs.at[7, j, low], xs.at[4, j, low], ag_send.at[1, 3], ag_recv.at[1, 4, j], l_dev
            ).start()

        add_chunk(jnp.concatenate([xs[k, j], xs[4 + k, j]], axis=0), j, acc)

        @pl.when(k > 1)
        def _():
            down_pair(k - 1, j)

        @pl.when(j == NCH - 1)
        def _():
            wait_bytes(xsc.at[k], xrecv.at[0, k])
            wait_bytes(xsc.at[4 + k], xrecv.at[1, k])
            send_scale(k, 0)

            @pl.when(k < 3)
            def _():
                rcopy(
                    xsc.at[4 + k], xsc.at[5 + k], xsend.at[1, k], xrecv.at[1, k + 1], l_dev
                ).start()

            activate(2 * rows1, acc, jnp.concatenate([scale_of(k), scale_of(4 + k)], axis=0))

    @pl.loop(0, NCH)
    def _(j):
        down_pair(3, j)
        sp_b[2, j, nsp:rows1] = zs[7, j, nsp:rows1].astype(BF16)
        sn_b[2, j, 0:nsp] = zs[3, j, 0:nsp].astype(BF16)
        rcopy(
            sp_b.at[2, j, low], rp_b.at[2, j, low], rs_send.at[0, 2], rs_recv.at[0, 2, j], r_dev
        ).start()
        rcopy(
            sn_b.at[2, j, top], rn_b.at[2, j, top], rs_send.at[1, 2], rs_recv.at[1, 2, j], l_dev
        ).start()
        wait_bytes(xs.at[4, j, top], ag_recv.at[0, 4, j])
        wait_bytes(xs.at[4, j, low], ag_recv.at[1, 4, j])
        add_chunk(xs[4, j], j, acc)

    wait_bytes(xsc.at[4], xrecv.at[0, 4])
    activate(rows1, acc, scale_of(4))

    @pl.loop(0, NCH)
    def _(j):
        z = down(rows1, j)
        sp_b[3, j, 0:nsp] = z[0:nsp].astype(BF16)
        sn_b[3, j, nsp:rows1] = z[nsp:rows1].astype(BF16)
        rcopy(
            sp_b.at[3, j, top], rp_b.at[3, j, top], rs_send.at[0, 3], rs_recv.at[0, 3, j], r_dev
        ).start()
        rcopy(
            sn_b.at[3, j, low], rn_b.at[3, j, low], rs_send.at[1, 3], rs_recv.at[1, 3, j], l_dev
        ).start()

    activate(rows1, acc_own, scale_of(0))

    @pl.loop(0, NCH)
    def _(j):
        zs[0, j] = down(rows1, j)

    @pl.loop(0, NCH)
    def _(j):
        wait_bytes(rp_b.at[3, j, top], rs_recv.at[0, 3, j])
        wait_bytes(rn_b.at[3, j, low], rs_recv.at[1, 3, j])
        sp_b[2, j, 0:nsp] = (zs[7, j, 0:nsp] + rp_b[3, j, 0:nsp].astype(F32)).astype(BF16)
        sn_b[2, j, nsp:rows1] = (zs[3, j, nsp:rows1] + rn_b[3, j, nsp:rows1].astype(F32)).astype(BF16)
        rcopy(
            sp_b.at[2, j, top], rp_b.at[2, j, top], rs_send.at[0, 2], rs_recv.at[0, 2, j], r_dev
        ).start()
        rcopy(
            sn_b.at[2, j, low], rn_b.at[2, j, low], rs_send.at[1, 2], rs_recv.at[1, 2, j], l_dev
        ).start()

    @pl.loop(0, 2 * NCH)
    def _(t):
        k = 2 - t // NCH
        j = t % NCH
        wait_bytes(rp_b.at[k, j], rs_recv.at[0, k, j])
        wait_bytes(rn_b.at[k, j], rs_recv.at[1, k, j])
        sp_b[k - 1, j] = (zs[4 + k, j] + rp_b[k, j].astype(F32)).astype(BF16)
        sn_b[k - 1, j] = (zs[k, j] + rn_b[k, j].astype(F32)).astype(BF16)
        rcopy(
            sp_b.at[k - 1, j], rp_b.at[k - 1, j], rs_send.at[0, k - 1], rs_recv.at[0, k - 1, j], r_dev
        ).start()
        rcopy(
            sn_b.at[k - 1, j], rn_b.at[k - 1, j], rs_send.at[1, k - 1], rs_recv.at[1, k - 1, j], l_dev
        ).start()

    for p in range(parts):
        for q in range(per):
            j = p * per + q
            wait_bytes(rp_b.at[0, j], rs_recv.at[0, 0, j])
            wait_bytes(rn_b.at[0, j], rs_recv.at[1, 0, j])
            total = zs[0, j] + rp_b[0, j].astype(F32) + rn_b[0, j].astype(F32)
            for n in range(width // 128):
                for s in range(2):
                    tile = q * (width // 128) + n
                    rowsf[pl.ds(2 * tile + s, nsp, stride=2 * tiles), :] = total[
                        s * nsp : (s + 1) * nsp, n * 128 : (n + 1) * 128
                    ]
        bm[p] = rowsf[0 : nsp * 2 * tiles].reshape(nsp, 2 * tiles, 128).astype(BF16)

        @pl.loop(0, nsp - 1)
        def _(i):
            dst = peer(i, me, nsp)
            rcopy(bm.at[p, dst], br.at[p, me], bsem.at[0, p], bsem.at[1, p], {"sp": dst}).start()

        br[p, me] = bm[p, me]

    for p in range(parts):
        wait_bytes(br.at[p, pl.ds(0, others)], bsem.at[1, p])
        back = br[p].astype(F32).reshape(nsp * 2 * tiles, 128).astype(BF16)
        mixed = dot(mix_hi, back) + dot(mix_lo, back)
        for n in range(tiles):
            cols = slice(p * WIDE + n * 128, p * WIDE + (n + 1) * 128)
            local = slice(cols.start % (2 * span), cols.start % (2 * span) + 128)
            base = middles[cols.start // (2 * span)][:, local]
            out[:, cols] = (base + mixed[n * own : (n + 1) * own]).astype(BF16)

    wait_bytes(hl, hsem.at[0])
    wait_bytes(hr, hsem.at[2])
    wait_bytes(tot_r.at[pl.ds(0, others)], tsem.at[0])
    wait_bytes(st_r.at[pl.ds(0, others)], ssem.at[0])
    wait_bytes(sc_r.at[pl.ds(0, others)], osem.at[0])
    wait_bytes(blocks(4), wnear.at[0])

    @pl.when(x > 0)
    def _():
        wait_bytes(blocks(1), wfar.at[0])
        wait_bytes(blocks(nx - 1), wsem.at[0])

    for h in range(2):
        wait_bytes(mo.at[h, pl.ds(0, ntp - 5)], psem.at[0, h])
        for copy in relays[h]:
            copy.wait_send()
    wait_bytes(sr.at[pl.ds(0, others)], csem.at[0])
    for k in range(4):
        wait_bytes(xsc.at[0], xsend.at[0, k])
    for k in range(3):
        wait_bytes(xsc.at[0], xsend.at[1, k])
    for p in range(parts):
        wait_bytes(dr.at[p, pl.ds(0, others)], dsem.at[0, p])
        wait_bytes(br.at[p, pl.ds(0, others)], bsem.at[0, p])
    for way in range(2):
        for k in range(3):
            wait_bytes(xs.at[0], ag_send.at[way, k])
            wait_bytes(xs.at[0], rs_send.at[way, k])
        wait_bytes(xs.at[0, pl.ds(0, 2)], ag_send.at[way, 3])
        wait_bytes(xs.at[0, pl.ds(0, 2)], rs_send.at[way, 3])


def layer(nsp, ntp, resid, v, k, q, og, raw, hdl, extra, vf, kf, qf, gain, wout, ngain, routes, cw, wg, wu, wd):
    ny = ntp // 2
    tokens = v.shape[0]
    own = tokens // ntp
    width = resid.shape[1] // NCH
    ff = wg.shape[2]
    chan = wout.shape[0] // ny
    rows1 = 2 * nsp

    small = [
        resid,
        v,
        k,
        q,
        og,
        raw.transpose(0, 2, 1),
        hdl,
        extra.T,
        vf,
        kf,
        qf,
        gain.reshape(1, -1),
        ngain.reshape(1, -1),
        routes.T,
        cw.T,
    ]
    dma = pltpu.SemaphoreType.DMA
    hbm = pl.BlockSpec(memory_space=pl.ANY)
    pair = (nsp, 16, 128)
    parts = resid.shape[1] // WIDE
    msg = (parts, nsp, WIDE // 64, 128)
    ring = (4, NCH, rows1, width)
    scratch = [pltpu.VMEM(x.shape, x.dtype) for x in small] + [
        pltpu.VMEM((2, 8, tokens), F32),
        pltpu.VMEM((16, 512), BF16),
        pltpu.VMEM((16, 512), BF16),
        pltpu.VMEM((tokens + 32, 512), F32),
        pltpu.VMEM((1, 128), F32),
        pltpu.VMEM((nsp, 1, 128), F32),
        pltpu.VMEM((2, nsp, 128), F32),
        pltpu.VMEM(pair, BF16),
        pltpu.VMEM(pair, BF16),
        pltpu.VMEM(pair, F32),
        pltpu.VMEM(pair, BF16),
        pltpu.VMEM(pair, BF16),
        pltpu.VMEM((2, tokens, 256), BF16),
        pltpu.VMEM((chan, 128 * ny), BF16),
        pltpu.VMEM((2, ntp, own, 64 * ny), BF16),
        pltpu.VMEM((2, ntp, own, 64 * ny), BF16),
        pltpu.VMEM((2, 2, 2, own, 64 * ny), BF16),
        pltpu.VMEM((2, 2, 2, own, 64 * ny), BF16),
        pltpu.VMEM((nsp, 1, 128), F32),
        pltpu.VMEM((nsp, 1, 128), F32),
        pltpu.VMEM((8, 1, 128), F32),
        pltpu.VMEM((rows1, 4 * ff), F32),
        pltpu.VMEM(msg, BF16),
        pltpu.VMEM(msg, BF16),
        pltpu.VMEM((nsp * WIDE // 64 + 8, 128), F32),
        pltpu.VMEM((8, NCH, rows1, width), BF16),
        pltpu.VMEM((wg.shape[1], 4 * ff), BF16),
        pltpu.VMEM((2 * ff, wd.shape[2]), BF16),
        pltpu.VMEM((2 * rows1, 4 * ff), F32),
        pltpu.VMEM((2 * rows1, 2 * ff), BF16),
        pltpu.VMEM((8, NCH, rows1, width), F32),
        pltpu.VMEM(ring, BF16),
        pltpu.VMEM(ring, BF16),
        pltpu.VMEM(ring, BF16),
        pltpu.VMEM(ring, BF16),
        pltpu.VMEM(msg, BF16),
        pltpu.VMEM(msg, BF16),
        dma((4,)),
        dma((4,)),
        dma((2,)),
        dma((2,)),
        dma((2,)),
        dma((2, 2)),
        dma((2,)),
        dma((2,)),
        dma((2,)),
        dma((6,)),
        dma((2, 2)),
        dma((2, 2, 2, 2)),
        dma((2,)),
        dma((2, 4)),
        dma((2, 5)),
        dma((2, parts)),
        dma((2, 4)),
        dma((2, 5, NCH)),
        dma((2, 4)),
        dma((2, 4, NCH)),
        dma((2, parts)),
        dma((NSMALL,)),
    ]
    return pl.pallas_call(
        functools.partial(body, nsp, ntp),
        out_shape=jax.ShapeDtypeStruct(resid.shape, BF16),
        in_specs=[hbm] * (NSMALL + 4),
        out_specs=pl.BlockSpec(memory_space=pltpu.VMEM),
        scratch_shapes=scratch,
        compiler_params=pltpu.CompilerParams(
            collective_id=0, has_side_effects=True, vmem_limit_bytes=56 * 1024 * 1024
        ),
        name="layer",
    )(*small, wout, wg[0], wu[0], wd[0])


def solution(mesh):
    both = ("sp", "tp")
    return jax.shard_map(
        functools.partial(layer, mesh.shape["sp"], mesh.shape["tp"]),
        mesh=mesh,
        in_specs=(
            P(both, None),
            P("sp", "tp"),
            P("sp", "tp"),
            P("sp", "tp"),
            P("sp", "tp"),
            P(None, "sp", "tp"),
            P(None, "tp"),
            P("sp", "tp"),
            P(None, "tp"),
            P(None, "tp"),
            P(None, "tp"),
            P("tp"),
            P(None, "tp"),
            P(),
            P("sp", None),
            P(both, None),
            P("sp", None, "tp"),
            P("sp", None, "tp"),
            P("sp", "tp", None),
        ),
        out_specs=P(both, None),
        check_vma=False,
    )
```
